256 devices in a mesh: rep: 2 (over z_hi), fs: 16 (over z_lo, y), tp: 8 (over x, core).
Axes of the slice: x: 4, y: 4, z: 8 (z_hi: 2, z_lo: 4; z = z_hi * 4 + z_lo), core: 2. Of those that a mesh axis runs over, the one named last changes fastest.
Arguments:
- stream: bfloat16 [16384, 2048], P(('rep', 'fs'), 'tp'), may hold values from -6 to 6
- recurrent_norm_gain: float32 [2048], replicated, may hold values from 0.1 to 1.9
- feedforward_norm_gain: float32 [2048], replicated, may hold values from 0.1 to 1.9
- recurrent_input_weight: bfloat16 [2048, 2048], P('fs', 'tp'), may hold values from -0.125 to 0.125
- output_gate_weight: bfloat16 [2048, 2048], P('fs', 'tp'), may hold values from -0.125 to 0.125
- causal_filter_weight: bfloat16 [4, 2048], P(None, 'tp'), may hold values from -3 to 3
- decay_gate_matrix: bfloat16 [32, 64, 64], P('tp'), may hold values from -0.75 to 0.75
- input_gate_matrix: bfloat16 [32, 64, 64], P('tp'), may hold values from -0.75 to 0.75
- channel_decay_param: float32 [2048], P('tp'), may hold values from 3 to 10
- token_decay_offset: float32 [16384, 2048], P(('rep', 'fs'), 'tp'), may hold values from -0.7 to 0, as said below
- recurrent_output_weight: bfloat16 [2048, 2048], P('tp', 'fs'), may hold values from -0.125 to 0.125
- up_projection_weight: bfloat16 [2048, 6144], P('fs', 'tp'), may hold values from -0.125 to 0.125
- down_projection_weight: bfloat16 [6144, 2048], P('tp', 'fs'), may hold values from -0.078125 to 0.078125
Outputs:
- updated: bfloat16 [16384, 2048], P(('rep', 'fs'), 'tp')
The draws below stay inside these ranges and needn't reach their ends.
Inputs may be any that keep to these rules, and one draw needn't show every extreme that they name: `token_decay_offset`: zero except at a few positions, where a whole row is negative.
All inputs are finite; a program needn't handle non-finite values.
Results may differ from the reference program's by a relative error of at most 0.015.
Values may be sent and summed in bfloat16 or wider, within the bound.
A program may use at most 64 MiB of HBM per device.

```python
import jax
import jax.numpy as jnp
from jax import lax

D = 2048
FF = 6144
BLOCK = 64
CONV = 4
SEQ_LEN = 128
TOKENS = 16384
BLOCKS = 32
N_TP = 8


def draw_channel_decay_param(key, part):
    kind_key = jax.random.fold_in(key, 11)
    slow_key = jax.random.fold_in(key, 12)
    fast_key = jax.random.fold_in(key, 13)
    fast = jax.random.uniform(kind_key, (D,), jnp.float32) < 0.5
    slow_rate = jnp.exp(jax.random.uniform(slow_key, (D,), jnp.float32, jnp.log(0.3), jnp.log(3.0))) / SEQ_LEN
    fast_rate = jnp.exp(jax.random.uniform(fast_key, (D,), jnp.float32, jnp.log(0.1), jnp.log(0.3)))
    rate = jnp.where(fast, fast_rate, slow_rate)
    return (-jnp.log(jnp.expm1(rate / 8.0))).astype(jnp.float32)


def draw_token_decay_offset(key, part):
    where_key = jax.random.fold_in(key, 21)
    depth_key = jax.random.fold_in(key, 22)
    hits = jax.random.uniform(where_key, (TOKENS, 1), jnp.float32) < 3.0 / SEQ_LEN
    depth = jax.random.uniform(depth_key, (TOKENS, D), jnp.float32, 0.22, 0.69)
    return jnp.where(hits, -depth, 0.0).astype(jnp.float32)


def block_scale(own_key, shape, cuts, least, high):
    loudness = 1.0
    for position, blocks in cuts:
        heights = jax.random.uniform(jax.random.fold_in(jax.random.fold_in(own_key, 6), position), (blocks,), jnp.float32, least / len(cuts), high / len(cuts))
        loudness = loudness * jnp.repeat(jnp.exp(heights), shape[position] // blocks).reshape((-1,) + (1,) * (len(shape) - 1 - position))
    return loudness


def noise(rng, shape, width, most, shards=(), kind=jnp.bfloat16):
    array = width * jax.random.normal(rng, shape, jnp.float32)
    if shards:
        array = array * block_scale(rng, shape, shards, -0.22, 0.18)
    return jnp.clip(array, -most, most).astype(kind)


def setup_inputs(seed: int = 0) -> dict:
    seeds = jax.random.split(jax.random.key(seed), 14)
    return {
        "stream": noise(seeds[0], (TOKENS, D), 1.0, 6.0, ((0, 32), (1, 8))),
        "recurrent_norm_gain": jnp.clip(1.0 + 0.18 * jax.random.normal(seeds[1], (D,), jnp.float32), 0.1, 1.9),
        "feedforward_norm_gain": jnp.clip(1.0 + 0.18 * jax.random.normal(seeds[2], (D,), jnp.float32), 0.1, 1.9),
        "recurrent_input_weight": noise(seeds[3], (D, D), D ** -0.5, 0.125, ((0, 16), (1, 8))),
        "output_gate_weight": noise(seeds[4], (D, D), D ** -0.5, 0.125, ((0, 16), (1, 8))),
        "causal_filter_weight": noise(seeds[5], (CONV, D), CONV ** -0.5, 3.0, ((1, 8),)),
        "decay_gate_matrix": noise(seeds[6], (BLOCKS, BLOCK, BLOCK), BLOCK ** -0.5, 0.75, ((0, 8),)),
        "input_gate_matrix": noise(seeds[7], (BLOCKS, BLOCK, BLOCK), BLOCK ** -0.5, 0.75, ((0, 8),)),
        "channel_decay_param": draw_channel_decay_param(jax.random.fold_in(seeds[13], 71), 0),
        "token_decay_offset": draw_token_decay_offset(jax.random.fold_in(seeds[13], 71), 0),
        "recurrent_output_weight": noise(seeds[10], (D, D), D ** -0.5, 0.125, ((0, 8), (1, 16))),
        "up_projection_weight": noise(seeds[11], (D, FF), D ** -0.5, 0.125, ((0, 16), (1, 8))),
        "down_projection_weight": noise(seeds[12], (FF, D), FF ** -0.5, 0.078125, ((0, 8), (1, 16))),
    }


EPSILON = 1e-06
DECAY_MULTIPLIER = 8.0

def norm_rows(values, gain):
    widened = values.astype(jnp.float32)
    inverse = lax.rsqrt(lax.optimization_barrier(jnp.mean(widened * widened, axis=-1, keepdims=True)) + EPSILON)
    return (widened * inverse * gain).astype(jnp.bfloat16)

def short_filter(values, causal_filter_weight):
    positions, channels = values.shape
    sequences = positions // SEQ_LEN
    reach = causal_filter_weight.shape[0]
    widened = lax.optimization_barrier(values).astype(jnp.float32).reshape(sequences, SEQ_LEN, channels)
    padded = jnp.pad(widened, ((0, 0), (reach - 1, 0), (0, 0)))
    taps = causal_filter_weight.astype(jnp.float32)
    total = taps[0] * padded[:, 0:SEQ_LEN]
    for offset in range(1, reach):
        total = total + taps[offset] * padded[:, offset:offset + SEQ_LEN]
    return total.reshape(positions, channels).astype(jnp.bfloat16)

def combine(earlier, later):
    return (earlier[0] * later[0], later[0] * earlier[1] + later[1])

def recurrent_states(filtered_input, output_gate_rows, decay_gate_matrix, input_gate_matrix, channel_decay_param, token_decay_offset):
    positions, channels = filtered_input.shape
    blocks, block_size, _ = decay_gate_matrix.shape
    widened = lax.optimization_barrier(filtered_input).astype(jnp.float32)
    grouped = widened.reshape(positions, blocks, block_size)
    recurrent_step = jax.nn.sigmoid(jnp.einsum('tnc,ncd->tnd', grouped, decay_gate_matrix.astype(jnp.float32)).reshape(positions, channels))
    inputs = jax.nn.sigmoid(jnp.einsum('tnc,ncd->tnd', grouped, input_gate_matrix.astype(jnp.float32)).reshape(positions, channels))
    decay_logarithm = -DECAY_MULTIPLIER * recurrent_step * jax.nn.softplus(-channel_decay_param) + token_decay_offset
    drive = jnp.sqrt(-jnp.expm1(2.0 * decay_logarithm)) * inputs * widened
    shaped = (positions // SEQ_LEN, SEQ_LEN, channels)
    _, states = lax.associative_scan(combine, (jnp.exp(decay_logarithm).reshape(shaped), drive.reshape(shaped)), axis=1)
    gate_wide = lax.optimization_barrier(output_gate_rows).astype(jnp.float32)
    return (states.reshape(positions, channels) * jax.nn.gelu(gate_wide, approximate=False)).astype(jnp.bfloat16)

def reference(stream, recurrent_norm_gain, feedforward_norm_gain, recurrent_input_weight, output_gate_weight, causal_filter_weight, decay_gate_matrix, input_gate_matrix, channel_decay_param, token_decay_offset, recurrent_output_weight, up_projection_weight, down_projection_weight):
    normed = norm_rows(stream, recurrent_norm_gain)
    span = D // N_TP
    grouped_block_rows = span // BLOCK
    mixer_update = jnp.zeros(stream.shape, jnp.float32)
    for channel_group in range(N_TP):
        lower_bound = channel_group * span
        upper_bound = lower_bound + span
        values = jnp.dot(normed, recurrent_input_weight[:, lower_bound:upper_bound], preferred_element_type=jnp.float32).astype(jnp.bfloat16)
        gate_values = jnp.dot(normed, output_gate_weight[:, lower_bound:upper_bound], preferred_element_type=jnp.float32).astype(jnp.bfloat16)
        filtered_input = short_filter(values, causal_filter_weight[:, lower_bound:upper_bound])
        mixed_rows = recurrent_states(filtered_input, gate_values, decay_gate_matrix[channel_group * grouped_block_rows:(channel_group + 1) * grouped_block_rows], input_gate_matrix[channel_group * grouped_block_rows:(channel_group + 1) * grouped_block_rows], channel_decay_param[lower_bound:upper_bound], token_decay_offset[:, lower_bound:upper_bound])
        partial_value = jnp.dot(mixed_rows, recurrent_output_weight[lower_bound:upper_bound], preferred_element_type=jnp.float32).astype(jnp.bfloat16)
        mixer_update = mixer_update + lax.optimization_barrier(partial_value).astype(jnp.float32)
    middle = (stream.astype(jnp.float32) + mixer_update).astype(jnp.bfloat16)
    normed_mid = norm_rows(middle, feedforward_norm_gain)
    hidden_span = FF // N_TP
    channel_update = jnp.zeros(stream.shape, jnp.float32)
    for channel_group in range(N_TP):
        lower_bound = channel_group * hidden_span
        upper_bound = lower_bound + hidden_span
        raised = jnp.dot(normed_mid, up_projection_weight[:, lower_bound:upper_bound], preferred_element_type=jnp.float32)
        activity = jnp.square(jax.nn.relu(raised)).astype(jnp.bfloat16)
        partial_value = jnp.dot(activity, down_projection_weight[lower_bound:upper_bound], preferred_element_type=jnp.float32).astype(jnp.bfloat16)
        channel_update = channel_update + lax.optimization_barrier(partial_value).astype(jnp.float32)
    return (middle.astype(jnp.float32) + channel_update).astype(jnp.bfloat16)
```

```python
import jax
import jax.numpy as jnp
from jax import lax
from jax.experimental import pallas as pl
from jax.experimental.pallas import tpu as pltpu
from jax.sharding import Mesh
from jax.sharding import PartitionSpec as P

MESH = pl.DeviceIdType.MESH
SEQ_LEN = 128
FS = ("fs_0", "fs_1")
REP_FS = ("rep", "fs_0", "fs_1")
AXES = ("rep", "fs_0", "fs_1", "tp")

EPSILON = 1e-06
DECAY_MULTIPLIER = 8.0
F32 = jnp.float32
BF16 = jnp.bfloat16

ROWS, WIDTH, PARTS, GROUP = 512, 256, 4, 8
PART = ROWS // PARTS
HALF = PART // 2

KINDS = (
    "oy+", "oy-", "oz+", "oz-",
    "ry+", "ry-", "rz+", "rz-",
    "a1z+", "a1z-", "a3z+", "a3z-", "b1y+", "b1y-", "b3y+", "b3y-",
    "a2z+", "a2z-", "b2y+", "b2y-",
    "last",
)


def wrap(value, n):
    return lax.rem(value + n, n)


class Place:
    def __init__(self):
        self.rep, self.z, self.y, self.tp = (lax.axis_index(a) for a in AXES)
        self.whole_z = self.rep * 4 + self.z
        self.x, self.core = self.tp // 2, lax.rem(self.tp, 2)
        self.other = 1 - self.core

    def device(self, x=0, y=0, z=0, flip=False):
        z_there = wrap(self.whole_z + z, 8)
        core = self.other if flip else self.core
        return (z_there // 4, lax.rem(z_there, 4), wrap(self.y + y, 4), wrap(self.x + x, 4) * 2 + core)

    def shard(self, z=0, y=0):
        return wrap(self.z + z, 4) * 4 + wrap(self.y + y, 4)

    def slot(self, x=0, flip=False):
        return wrap(self.x + x, 4) * 2 + (self.other if flip else self.core)


class WeightGather:
    def __init__(self, place, index, own_ref, held, local_sem, send_sem, recv_sems):
        self.p, self.i, self.own, self.held = place, index, own_ref, held
        self.local = pltpu.make_async_copy(own_ref, held.at[place.shard()], local_sem.at[index])
        self.send_sem, self.recv_sems = send_sem.at[index], recv_sems
        self.sent = {}

    def go(self, kind, shard, part, recv_kind=None):
        where = {"y+": dict(y=1), "y-": dict(y=-1), "z+": dict(z=1), "z-": dict(z=-1)}[kind[-2:]]
        view = self.held.at[(self.p.shard(**shard), *part)]
        copy = pltpu.make_async_remote_copy(
            src_ref=view,
            dst_ref=view,
            send_sem=self.send_sem,
            recv_sem=self.recv_sems.at[self.i, KINDS.index(recv_kind or kind)],
            device_id=self.p.device(**where),
            device_id_type=MESH,
        )
        copy.start()
        self.sent[kind] = copy

    def got(self, *kinds):
        for kind in kinds:
            self.sent[kind].wait_recv()

    def start(self):
        self.local.wait()
        for kind in ("oy+", "oy-", "oz+", "oz-"):
            self.go(kind, {}, ())

    def first(self):
        every = slice(None)
        self.got("oy+")
        self.go("ry+", dict(y=-1), (every, 0))
        self.go("a1z+", dict(y=-1), (0,))
        self.go("a1z-", dict(y=-1), (0,))
        self.got("oz+")
        self.go("rz+", dict(z=-1), (every, 0))
        self.go("b1y+", dict(z=-1), (1,))
        self.go("b1y-", dict(z=-1), (1,))
        self.got("oy-")
        self.go("ry-", dict(y=1), (every, 1))
        self.go("a3z+", dict(y=1), (0,))
        self.go("a3z-", dict(y=1), (0,))
        self.got("oz-")
        self.go("rz-", dict(z=1), (every, 1))
        self.go("b3y+", dict(z=1), (1,))
        self.go("b3y-", dict(z=1), (1,))

    def second(self):
        self.got("ry+", "ry-")
        self.go("a2z+", dict(y=2), (0,))
        self.go("a2z-", dict(y=2), (0,))
        self.got("rz+", "rz-")
        self.go("b2y+", dict(z=2), (1,))
        self.go("b2y-", dict(z=2), (1,))
        for n, y in ((1, -1), (3, 1)):
            self.got(f"a{n}z+")
            self.go(f"f{n}z+", dict(z=-1, y=y), (0, 0), "last")
            self.got(f"a{n}z-")
            self.go(f"f{n}z-", dict(z=1, y=y), (0, 1), "last")
        for n, z in ((1, -1), (3, 1)):
            self.got(f"b{n}y+")
            self.go(f"g{n}y+", dict(z=z, y=-1), (1, 0), "last")
            self.got(f"b{n}y-")
            self.go(f"g{n}y-", dict(z=z, y=1), (1, 1), "last")

    def third(self):
        self.got("a2z+")
        self.go("f2z+", dict(z=-1, y=2), (0, 0), "last")
        self.got("a2z-")
        self.go("f2z-", dict(z=1, y=2), (0, 1), "last")
        self.got("b2y+")
        self.go("g2y+", dict(z=2, y=-1), (1, 0), "last")
        self.got("b2y-")
        self.go("g2y-", dict(z=2, y=1), (1, 1), "last")

    def bytes_of(self, shards, sem):
        view = self.held.at[pl.ds(0, shards)]
        pltpu.make_async_copy(view, view, sem).wait()

    def finish(self):
        self.bytes_of(3, self.recv_sems.at[self.i, KINDS.index("last")])

    def drain(self):
        self.bytes_of(15, self.send_sem)


class TokenGather:
    def __init__(self, place, index, held, start, rows, send_sems, recv_sems):
        self.p, self.held, self.start, self.rows = place, held, start, rows
        self.send_sem, self.recv_sems = send_sems.at[index], recv_sems.at[index]
        self.sent = {}

    def go(self, name, sem, slot, device, start=0, rows=None):
        view = self.held.at[slot, pl.ds(self.start + start, rows or self.rows)]
        copy = pltpu.make_async_remote_copy(
            src_ref=view,
            dst_ref=view,
            send_sem=self.send_sem,
            recv_sem=self.recv_sems.at[sem],
            device_id=device,
            device_id_type=MESH,
        )
        copy.start()
        self.sent[name] = copy

    def slots_of(self, slots, sem):
        view = self.held.at[pl.ds(0, slots), pl.ds(self.start, self.rows)]
        pltpu.make_async_copy(view, view, sem).wait()

    def begin(self):
        p = self.p
        self.go("o+", 0, p.slot(), p.device(x=1))
        self.go("o-", 1, p.slot(), p.device(x=-1))
        self.go("p0", 3, p.slot(), p.device(flip=True))

    def near(self):
        p, half = self.p, self.rows // 2
        self.sent["o+"].wait_recv()
        self.go("f+", 2, p.slot(x=-1), p.device(x=1), 0, half)
        self.go("p1", 3, p.slot(x=-1), p.device(flip=True))
        self.sent["o-"].wait_recv()
        self.go("f-", 2, p.slot(x=1), p.device(x=-1), half, half)
        self.go("p3", 3, p.slot(x=1), p.device(flip=True))

    def far(self):
        p = self.p
        self.slots_of(1, self.recv_sems.at[2])
        self.go("p2", 3, p.slot(x=2), p.device(flip=True))

    def finish(self):
        self.slots_of(4, self.recv_sems.at[3])

    def drain(self):
        self.slots_of(7, self.send_sem)


class TokenSum:
    def __init__(self, place, index, part, terms, from_core, chip, near, last, send_sems, recv_sems):
        self.p, self.part, self.rows = place, part, pl.ds(part * PART, PART)
        self.terms, self.from_core, self.chip, self.near, self.last = terms, from_core, chip, near, last
        self.send_sem, self.recv_sems = send_sems.at[index], recv_sems.at[index]
        self.sent = {}

    def go(self, name, sem, src, dst, device):
        copy = pltpu.make_async_remote_copy(
            src_ref=src,
            dst_ref=dst,
            send_sem=self.send_sem,
            recv_sem=self.recv_sems.at[sem],
            device_id=device,
            device_id_type=MESH,
        )
        copy.start()
        self.sent[name] = copy

    def half(self, h):
        return pl.ds(self.part * PART + h * HALF, HALF)

    def begin(self):
        p = self.p
        self.go("d", 0, self.terms.at[:, p.other, self.rows], self.from_core.at[:, self.rows], p.device(flip=True))

    def chip_sum(self, x):
        p = self.p
        there = wrap(p.x + x, 4)
        return self.terms[there, p.core, self.rows].astype(F32) + self.from_core[there, self.rows].astype(F32)

    def cores(self):
        p, chip = self.p, self.chip
        self.sent["d"].wait_recv()
        right, left, far = wrap(p.x + 1, 4), wrap(p.x - 1, 4), wrap(p.x + 2, 4)
        chip[far, self.rows] = self.chip_sum(2).astype(BF16)
        self.go("h+", 1, chip.at[far, self.half(0)], self.near.at[0, self.half(0)], p.device(x=1))
        self.go("h-", 2, chip.at[far, self.half(1)], self.near.at[1, self.half(1)], p.device(x=-1))
        chip[right, self.rows] = self.chip_sum(1).astype(BF16)
        self.go("e+", 3, chip.at[right, self.half(1)], self.last.at[0, self.half(1)], p.device(x=1))
        chip[left, self.rows] = self.chip_sum(-1).astype(BF16)
        self.go("e-", 3, chip.at[left, self.half(0)], self.last.at[1, self.half(0)], p.device(x=-1))

    def ring(self):
        p, chip = self.p, self.chip
        for name, x, h, side in (("h+", 1, 0, 0), ("h-", -1, 1, 1)):
            there = wrap(p.x + x, 4)
            rows = self.half(h)
            self.sent[name].wait_recv()
            total = chip[there, rows].astype(F32) + self.near[side, rows].astype(F32)
            self.near[side, rows] = total.astype(BF16)
            self.go("e2" + name, 3, self.near.at[side, rows], self.last.at[side, rows], p.device(x=x))

    def finish(self, base):
        both = self.last.at[:, self.rows]
        pltpu.make_async_copy(both, both, self.recv_sems.at[3]).wait()
        total = self.chip_sum(0) + (self.last[0, self.rows].astype(F32) + self.last[1, self.rows].astype(F32))
        return (base.astype(F32) + total).astype(BF16)

    def drain(self):
        view = self.terms.at[:, 0, self.rows]
        part = self.chip.at[pl.ds(0, 3), self.rows]
        pltpu.make_async_copy(view, view, self.send_sem).wait()
        pltpu.make_async_copy(part, part, self.send_sem).wait()


def norm_rows(held, rows, gain_ref, normed):
    total = jnp.zeros((PART, 1), F32)
    for k in range(GROUP):
        piece = held[k, rows].astype(F32)
        total = total + jnp.sum(piece * piece, axis=-1, keepdims=True)
    inverse = lax.rsqrt(total * (1.0 / (GROUP * WIDTH)) + EPSILON)
    for k in range(GROUP):
        columns = slice(k * WIDTH, (k + 1) * WIDTH)
        piece = held[k, rows].astype(F32) * inverse * gain_ref[:, columns]
        normed[rows, columns] = piece.astype(BF16)


def block_diagonal(matrix_ref, out_ref, offset):
    blocks, size, _ = matrix_ref.shape
    row = lax.broadcasted_iota(jnp.int32, (size, blocks * size), 0)
    column = lax.broadcasted_iota(jnp.int32, (size, blocks * size), 1)
    for b in range(blocks):
        select = (column == row + b * size).astype(F32).astype(BF16)
        spread = jnp.dot(matrix_ref[b], select, preferred_element_type=F32)
        out_ref[b * size : (b + 1) * size, offset : offset + blocks * size] = spread.astype(BF16)


def shifted(values, by, row, fill):
    return jnp.where(row >= by, pltpu.roll(values, by, 0), fill)


def mixer_rows(values, gates, offsets, taps, maps, rate):
    channels = values.shape[1]
    row = lax.broadcasted_iota(jnp.int32, values.shape, 0)
    wide = values.astype(F32)
    reach = taps.shape[0]
    total = taps[0:1] * shifted(wide, reach - 1, row, 0.0)
    for k in range(1, reach):
        by = reach - 1 - k
        total = total + taps[k : k + 1] * (shifted(wide, by, row, 0.0) if by else wide)
    conved = total.astype(BF16)
    both = jax.nn.sigmoid(jnp.dot(conved, maps, preferred_element_type=F32))
    decay = rate * both[:, :channels] + offsets
    factor = jnp.exp(decay)
    twice = 2.0 * decay
    small = -twice * (1.0 + twice * (0.5 + twice * (1.0 / 6.0 + twice * (1.0 / 24.0))))
    lost = jnp.where(twice > -0.03, small, 1.0 - factor * factor)
    state = jnp.sqrt(lost) * both[:, channels:] * conved.astype(F32)
    by = 1
    while by < SEQ_LEN:
        state = factor * shifted(state, by, row, 0.0) + state
        if 2 * by < SEQ_LEN:
            factor = factor * shifted(factor, by, row, 1.0)
        by *= 2
    gate = gates.astype(F32)
    gelu = 0.5 * gate * (1.0 + lax.erf(gate * (0.5**0.5)))
    return (state * gelu).astype(BF16)


def kernel(
    stream_ref, gain1_ref, gain2_ref, input_ref, gate_ref, taps_ref, decay_ref, inmap_ref, param_ref, offset_hbm,
    output_ref, up_ref, down_ref,
    out_ref,
    w_input, w_gate, w_output, w_up, w_down,
    held1, held2, normed, values, gates, offsets, mixed, activity, maps,
    terms1, core1, chip1, near1, last1, terms2, core2, chip2, near2, last2,
    local_sem, wsend, wrecv, tsend, trecv,
):
    p = Place()
    weights = [
        WeightGather(p, i, own, held, local_sem, wsend, wrecv)
        for i, (own, held) in enumerate(
            (
                (input_ref, w_input),
                (gate_ref, w_gate),
                (output_ref, w_output),
                (up_ref, w_up),
                (down_ref, w_down),
            )
        )
    ]
    own_stream = pltpu.make_async_copy(stream_ref, held1.at[p.tp], local_sem.at[5])
    own_offsets = pltpu.make_async_copy(offset_hbm, offsets, local_sem.at[6])
    for w in weights[:2]:
        w.local.start()
    own_stream.start()
    for w in weights[2:]:
        w.local.start()
    own_offsets.start()

    barrier = pltpu.get_barrier_semaphore()
    greeted = [dict(x=1), dict(x=-1), dict(y=1), dict(y=-1), dict(z=1), dict(z=-1), dict(flip=True)]
    for where in greeted:
        pl.semaphore_signal(barrier, inc=1, device_id=p.device(**where), device_id_type=MESH)
    pl.semaphore_wait(barrier, len(greeted))

    gather1 = TokenGather(p, 0, held1, 0, ROWS, tsend, trecv)
    gather2 = [TokenGather(p, 1 + c, held2, c * PART, PART, tsend, trecv) for c in range(PARTS)]
    sum1 = [
        TokenSum(p, 1 + PARTS + c, c, terms1, core1, chip1, near1, last1, tsend, trecv) for c in range(PARTS)
    ]
    sum2 = [
        TokenSum(p, 1 + 2 * PARTS + c, c, terms2, core2, chip2, near2, last2, tsend, trecv) for c in range(PARTS)
    ]
    w_in, w_g, w_out, w_u, w_d = weights

    w_in.start()
    w_g.start()
    own_stream.wait()
    gather1.begin()
    w_out.start()
    block_diagonal(decay_ref, maps, 0)
    block_diagonal(inmap_ref, maps, WIDTH)
    parameter = -param_ref[...]
    rate = -DECAY_MULTIPLIER * (jnp.maximum(parameter, 0.0) + jnp.log1p(jnp.exp(-jnp.abs(parameter))))
    w_in.first()
    w_g.first()
    gather1.near()
    w_in.second()
    w_g.second()
    w_out.first()
    w_u.start()
    gather1.far()
    w_in.third()
    w_g.third()
    w_out.second()
    gather1.finish()

    @pl.loop(0, PARTS)
    def _(c):
        norm_rows(held1, pl.ds(pl.multiple_of(c * PART, PART), PART), gain1_ref, normed)

    w_in.finish()
    w_g.finish()

    tall = ROWS // 2

    @pl.loop(0, 2)
    def _(m):
        rows = pl.ds(pl.multiple_of(m * tall, tall), tall)
        columns = normed[rows, :]
        full = w_input[...].reshape(GROUP * WIDTH, WIDTH)
        values[rows, :] = jnp.dot(columns, full, preferred_element_type=F32).astype(BF16)
        full = w_gate[...].reshape(GROUP * WIDTH, WIDTH)
        gates[rows, :] = jnp.dot(columns, full, preferred_element_type=F32).astype(BF16)

    w_out.third()
    w_u.first()
    own_offsets.wait()
    taps = taps_ref[...].astype(F32)

    def columns_of(held, j, depth):
        pair = held[pl.ds(2 * j, 2)].reshape(2, depth, 128)
        return jnp.concatenate([pair[0], pair[1]], axis=1)

    def mix(c):
        rows = pl.ds(c * PART, PART)
        mixed[rows, :] = mixer_rows(values[rows, :], gates[rows, :], offsets[rows, :], taps, maps[...], rate)

    def project(c, source, held, depth, terms):
        rows = pl.ds(c * PART, PART)

        @pl.loop(0, GROUP)
        def _(j):
            total = jnp.dot(source[rows, :], columns_of(held, j, depth), preferred_element_type=F32)
            terms[j // 2, lax.rem(j, 2), rows] = total.astype(BF16)

    def middle_of(c):
        rows = pl.ds(c * PART, PART)
        held2[p.tp, rows] = sum1[c].finish(held1[p.tp, rows])
        gather2[c].begin()

    def raise_rows(c):
        rows = pl.ds(c * PART, PART)
        norm_rows(held2, rows, gain2_ref, normed)

    mix(0)
    w_out.finish()
    project(0, mixed, w_output, WIDTH, terms1)
    sum1[0].begin()
    w_d.start()
    w_u.second()
    mix(1)
    project(1, mixed, w_output, WIDTH, terms1)
    sum1[1].begin()
    sum1[0].cores()
    mix(2)
    project(2, mixed, w_output, WIDTH, terms1)
    sum1[2].begin()
    sum1[1].cores()
    sum1[0].ring()
    w_u.third()
    mix(3)
    project(3, mixed, w_output, WIDTH, terms1)
    sum1[3].begin()
    sum1[2].cores()
    sum1[1].ring()
    middle_of(0)
    w_d.first()
    sum1[3].cores()
    sum1[2].ring()
    middle_of(1)
    gather2[0].near()
    sum1[3].ring()
    middle_of(2)
    gather2[1].near()
    gather2[0].far()
    w_d.second()
    middle_of(3)
    gather2[2].near()
    gather2[1].far()
    gather2[0].finish()
    raise_rows(0)
    gather2[3].near()
    gather2[2].far()
    gather2[1].finish()
    raise_rows(1)
    gather2[3].far()
    gather2[2].finish()
    raise_rows(2)
    gather2[3].finish()
    raise_rows(3)
    w_d.third()
    w_u.finish()

    hidden = w_up.shape[-1]

    def lift(c):
        rows = pl.ds(c * PART, PART)
        columns = normed[rows, :]
        for n in range(hidden // WIDTH):
            some = slice(n * WIDTH, (n + 1) * WIDTH)
            full = w_up[:, :, :, :, some].reshape(GROUP * WIDTH, WIDTH)
            raised = jnp.maximum(jnp.dot(columns, full, preferred_element_type=F32), 0.0)
            activity[rows, some] = (raised * raised).astype(BF16)

    for c in range(PARTS):
        lift(c)
    w_d.finish()

    def last_of(c):
        rows = pl.ds(c * PART, PART)
        out_ref[rows, :] = sum2[c].finish(held2[p.tp, rows])

    for c in range(PARTS + 3):
        if c < PARTS:
            project(c, activity, w_down, hidden, terms2)
            sum2[c].begin()
        if 0 <= c - 1 < PARTS:
            sum2[c - 1].cores()
        if 0 <= c - 2 < PARTS:
            sum2[c - 2].ring()
        if 0 <= c - 3 < PARTS:
            last_of(c - 3)

    for w in weights:
        w.drain()
    for event in (gather1, *gather2, *sum1, *sum2):
        event.drain()


def quarters(weight):
    rows, columns = weight.shape
    return weight.reshape(2, 2, rows // 4, columns)


def shards(
    stream,
    recurrent_norm_gain,
    feedforward_norm_gain,
    recurrent_input_weight,
    output_gate_weight,
    causal_filter_weight,
    decay_gate_matrix,
    input_gate_matrix,
    channel_decay_param,
    token_decay_offset,
    recurrent_output_weight,
    up_projection_weight,
    down_projection_weight,
):
    cut = [
        quarters(w)
        for w in (
            recurrent_input_weight,
            output_gate_weight,
            recurrent_output_weight,
            up_projection_weight,
            down_projection_weight,
        )
    ]
    hidden = up_projection_weight.shape[1]
    far, near = pl.BlockSpec(memory_space=pltpu.HBM), pl.BlockSpec(memory_space=pltpu.VMEM)
    sums = [
        pltpu.VMEM((4, 2, ROWS, WIDTH), BF16),
        pltpu.VMEM((4, ROWS, WIDTH), BF16),
        pltpu.VMEM((4, ROWS, WIDTH), BF16),
        pltpu.VMEM((2, ROWS, WIDTH), BF16),
        pltpu.VMEM((2, ROWS, WIDTH), BF16),
    ]
    events = 1 + 3 * PARTS
    return pl.pallas_call(
        kernel,
        out_shape=jax.ShapeDtypeStruct(stream.shape, stream.dtype),
        in_specs=[far, near, near, far, far, near, near, near, near, far, far, far, far],
        out_specs=near,
        scratch_shapes=[
            *[pltpu.VMEM((16, *w.shape), BF16) for w in cut],
            pltpu.VMEM((GROUP, ROWS, WIDTH), BF16),
            pltpu.VMEM((GROUP, ROWS, WIDTH), BF16),
            pltpu.VMEM((ROWS, GROUP * WIDTH), BF16),
            pltpu.VMEM((ROWS, WIDTH), BF16),
            pltpu.VMEM((ROWS, WIDTH), BF16),
            pltpu.VMEM((ROWS, WIDTH), F32),
            pltpu.VMEM((ROWS, WIDTH), BF16),
            pltpu.VMEM((ROWS, hidden), BF16),
            pltpu.VMEM((WIDTH, 2 * WIDTH), BF16),
            *sums,
            *sums,
            pltpu.SemaphoreType.DMA((7,)),
            pltpu.SemaphoreType.DMA((5,)),
            pltpu.SemaphoreType.DMA((5, len(KINDS))),
            pltpu.SemaphoreType.DMA((events,)),
            pltpu.SemaphoreType.DMA((events, 4)),
        ],
        compiler_params=pltpu.CompilerParams(
            collective_id=0, has_side_effects=True, vmem_limit_bytes=60 * 1024 * 1024
        ),
    )(
        stream,
        recurrent_norm_gain.reshape(1, -1),
        feedforward_norm_gain.reshape(1, -1),
        cut[0],
        cut[1],
        causal_filter_weight,
        decay_gate_matrix,
        input_gate_matrix,
        channel_decay_param.reshape(1, -1),
        token_decay_offset,
        cut[2],
        cut[3],
        cut[4],
    )


def solution(mesh):
    split = Mesh(
        mesh.devices.reshape(mesh.shape["rep"], 4, 4, mesh.shape["tp"]),
        AXES,
    )
    placed = (
        P(REP_FS, "tp"),
        P(),
        P(),
        P(FS, "tp"),
        P(FS, "tp"),
        P(None, "tp"),
        P("tp", None, None),
        P("tp", None, None),
        P("tp"),
        P(REP_FS, "tp"),
        P("tp", FS),
        P(FS, "tp"),
        P("tp", FS),
    )
    return jax.shard_map(
        shards, mesh=split, in_specs=placed, out_specs=P(REP_FS, "tp"), check_vma=False
    )
```

```python
import functools

import jax
import jax.numpy as jnp
from jax import lax
from jax.experimental import pallas as pl
from jax.experimental.pallas import tpu as pltpu
from jax.sharding import Mesh
from jax.sharding import PartitionSpec as P

MESH = pl.DeviceIdType.MESH
SEQ_LEN = 128
FS = ("fs_0", "fs_1")
REP_FS = ("rep", "fs_0", "fs_1")
AXES = ("rep", "fs_0", "fs_1", "tp")

EPSILON = 1e-06
DECAY_MULTIPLIER = 8.0
F32 = jnp.float32
BF16 = jnp.bfloat16

ROWS, WIDTH, PARTS, GROUP = 512, 256, 4, 8
PART = ROWS // PARTS
HALF = PART // 2

EVERY = slice(None)
STEPS = {
    "S": ((), (("oy+", 0, 0, ()), ("oy-", 0, 0, ()), ("oz+", 0, 0, ()), ("oz-", 0, 0, ()))),
    "a": (("oy+",), (("ry+", 0, -1, (EVERY, 0)), ("a1z+", 0, -1, (0,)), ("a1z-", 0, -1, (0,)))),
    "b": (("oz+",), (("rz+", -1, 0, (EVERY, 0)), ("b1y+", -1, 0, (1,)), ("b1y-", -1, 0, (1,)))),
    "c": (("oy-",), (("ry-", 0, 1, (EVERY, 1)), ("a3z+", 0, 1, (0,)), ("a3z-", 0, 1, (0,)))),
    "d": (("oz-",), (("rz-", 1, 0, (EVERY, 1)), ("b3y+", 1, 0, (1,)), ("b3y-", 1, 0, (1,)))),
    "e": (("ry+", "ry-"), (("a2z+", 0, 2, (0,)), ("a2z-", 0, 2, (0,)))),
    "f": (("rz+", "rz-"), (("b2y+", 2, 0, (1,)), ("b2y-", 2, 0, (1,)))),
    "g": (("a1z+",), (("f1z+", -1, -1, (0, 0)),)),
    "h": (("a1z-",), (("f1z-", 1, -1, (0, 1)),)),
    "i": (("a3z+",), (("f3z+", -1, 1, (0, 0)),)),
    "j": (("a3z-",), (("f3z-", 1, 1, (0, 1)),)),
    "k": (("b1y+",), (("g1y+", -1, -1, (1, 0)),)),
    "l": (("b1y-",), (("g1y-", -1, 1, (1, 1)),)),
    "m": (("b3y+",), (("g3y+", 1, -1, (1, 0)),)),
    "n": (("b3y-",), (("g3y-", 1, 1, (1, 1)),)),
    "o": (("a2z+",), (("f2z+", -1, 2, (0, 0)),)),
    "p": (("a2z-",), (("f2z-", 1, 2, (0, 1)),)),
    "q": (("b2y+",), (("g2y+", 2, -1, (1, 0)),)),
    "r": (("b2y-",), (("g2y-", 2, 1, (1, 1)),)),
}
SENT = [message[0] for _, sends in STEPS.values() for message in sends]
LAST = [name for name in SENT if name[0] in "fg"]
KINDS = [name for name in SENT if name not in LAST] + ["last"]


def wrap(value, n):
    return lax.rem(value + n, n)


class Place:
    def __init__(self):
        self.rep, self.z, self.y, self.tp = (lax.axis_index(a) for a in AXES)
        self.whole_z = self.rep * 4 + self.z
        self.x, self.core = self.tp // 2, lax.rem(self.tp, 2)
        self.other = 1 - self.core

    def device(self, x=0, y=0, z=0, flip=False):
        z_there = wrap(self.whole_z + z, 8)
        core = self.other if flip else self.core
        return (z_there // 4, lax.rem(z_there, 4), wrap(self.y + y, 4), wrap(self.x + x, 4) * 2 + core)

    def shard(self, z=0, y=0):
        return wrap(self.z + z, 4) * 4 + wrap(self.y + y, 4)

    def slot(self, x=0, flip=False):
        return wrap(self.x + x, 4) * 2 + (self.other if flip else self.core)


class WeightGather:
    def __init__(self, place, index, own_ref, held, local_sem, send_sem, recv_sems):
        self.p, self.i, self.own, self.held = place, index, own_ref, held
        self.local = pltpu.make_async_copy(own_ref, held.at[place.shard()], local_sem.at[index])
        self.send_sem, self.recv_sems = send_sem.at[index], recv_sems
        self.sent = {}

    def go(self, kind, z, y, part):
        where = {"y+": dict(y=1), "y-": dict(y=-1), "z+": dict(z=1), "z-": dict(z=-1)}[kind[-2:]]
        view = self.held.at[(self.p.shard(z, y), *part)]
        copy = pltpu.make_async_remote_copy(
            src_ref=view,
            dst_ref=view,
            send_sem=self.send_sem,
            recv_sem=self.recv_sems.at[self.i, KINDS.index("last" if kind in LAST else kind)],
            device_id=self.p.device(**where),
            device_id_type=MESH,
        )
        copy.start()
        self.sent[kind] = copy

    def step(self, name):
        if name == "S":
            self.local.wait()
        waits, sends = STEPS[name]
        for kind in waits:
            self.sent[kind].wait_recv()
        for message in sends:
            self.go(*message)

    def bytes_of(self, shards, sem):
        view = self.held.at[pl.ds(0, shards)]
        pltpu.make_async_copy(view, view, sem).wait()

    def finish(self):
        self.bytes_of(3, self.recv_sems.at[self.i, KINDS.index("last")])

    def drain(self):
        self.bytes_of(15, self.send_sem)


class TokenGather:
    def __init__(self, place, index, held, start, rows, send_sems, recv_sems):
        self.p, self.held, self.start, self.rows = place, held, start, rows
        self.send_sem, self.recv_sems = send_sems.at[index], recv_sems.at[index]
        self.sent = {}

    def go(self, name, sem, slot, device, start=0, rows=None):
        view = self.held.at[slot, pl.ds(self.start + start, rows or self.rows)]
        copy = pltpu.make_async_remote_copy(
            src_ref=view,
            dst_ref=view,
            send_sem=self.send_sem,
            recv_sem=self.recv_sems.at[sem],
            device_id=device,
            device_id_type=MESH,
        )
        copy.start()
        self.sent[name] = copy

    def slots_of(self, slots, sem):
        view = self.held.at[pl.ds(0, slots), pl.ds(self.start, self.rows)]
        pltpu.make_async_copy(view, view, sem).wait()

    def begin(self):
        p = self.p
        self.go("o+", 0, p.slot(), p.device(x=1))
        self.go("o-", 1, p.slot(), p.device(x=-1))
        self.go("p0", 3, p.slot(), p.device(flip=True))

    def near(self, sign):
        p, half = self.p, self.rows // 2
        if sign == "+":
            self.sent["o+"].wait_recv()
            self.go("f+", 2, p.slot(x=-1), p.device(x=1), 0, half)
            self.go("p1", 3, p.slot(x=-1), p.device(flip=True))
        else:
            self.sent["o-"].wait_recv()
            self.go("f-", 2, p.slot(x=1), p.device(x=-1), half, half)
            self.go("p3", 3, p.slot(x=1), p.device(flip=True))

    def far(self):
        p = self.p
        self.slots_of(1, self.recv_sems.at[2])
        self.go("p2", 3, p.slot(x=2), p.device(flip=True))

    def finish(self):
        self.slots_of(4, self.recv_sems.at[3])

    def drain(self):
        self.slots_of(7, self.send_sem)


class TokenSum:
    def __init__(self, place, index, part, terms, from_core, chip, near, last, send_sems, recv_sems):
        self.p, self.part, self.rows = place, part, pl.ds(part * PART, PART)
        self.terms, self.from_core, self.chip, self.near, self.last = terms, from_core, chip, near, last
        self.send_sem, self.recv_sems = send_sems.at[index], recv_sems.at[index]
        self.sent = {}

    def go(self, name, sem, src, dst, device):
        copy = pltpu.make_async_remote_copy(
            src_ref=src,
            dst_ref=dst,
            send_sem=self.send_sem,
            recv_sem=self.recv_sems.at[sem],
            device_id=device,
            device_id_type=MESH,
        )
        copy.start()
        self.sent[name] = copy

    def half(self, h):
        return pl.ds(self.part * PART + h * HALF, HALF)

    def begin(self):
        p = self.p
        self.go("d", 0, self.terms.at[:, p.other, self.rows], self.from_core.at[:, self.rows], p.device(flip=True))

    def chip_sum(self, x):
        p = self.p
        there = wrap(p.x + x, 4)
        return self.terms[there, p.core, self.rows].astype(F32) + self.from_core[there, self.rows].astype(F32)

    def cores(self):
        p, chip = self.p, self.chip
        self.sent["d"].wait_recv()
        right, left, far = wrap(p.x + 1, 4), wrap(p.x - 1, 4), wrap(p.x + 2, 4)
        chip[far, self.rows] = self.chip_sum(2).astype(BF16)
        self.go("h+", 1, chip.at[far, self.half(0)], self.near.at[0, self.half(0)], p.device(x=1))
        self.go("h-", 2, chip.at[far, self.half(1)], self.near.at[1, self.half(1)], p.device(x=-1))
        chip[right, self.rows] = self.chip_sum(1).astype(BF16)
        self.go("e+", 3, chip.at[right, self.half(1)], self.last.at[0, self.half(1)], p.device(x=1))
        chip[left, self.rows] = self.chip_sum(-1).astype(BF16)
        self.go("e-", 3, chip.at[left, self.half(0)], self.last.at[1, self.half(0)], p.device(x=-1))

    def ring(self, sign):
        p = self.p
        name, x, side = ("h+", 1, 0) if sign == "+" else ("h-", -1, 1)
        rows = self.half(side)
        self.sent[name].wait_recv()
        total = self.chip[wrap(p.x + x, 4), rows].astype(F32) + self.near[side, rows].astype(F32)
        self.near[side, rows] = total.astype(BF16)
        self.go("e2" + sign, 3, self.near.at[side, rows], self.last.at[side, rows], p.device(x=x))

    def finish(self, base):
        both = self.last.at[:, self.rows]
        pltpu.make_async_copy(both, both, self.recv_sems.at[3]).wait()
        total = self.chip_sum(0) + (self.last[0, self.rows].astype(F32) + self.last[1, self.rows].astype(F32))
        return (base.astype(F32) + total).astype(BF16)

    def drain(self):
        view = self.terms.at[:, 0, self.rows]
        part = self.chip.at[pl.ds(0, 3), self.rows]
        pltpu.make_async_copy(view, view, self.send_sem).wait()
        pltpu.make_async_copy(part, part, self.send_sem).wait()


def norm_rows(held, rows, gain_ref, normed):
    total = jnp.zeros((PART, 1), F32)
    for k in range(GROUP):
        piece = held[k, rows].astype(F32)
        total = total + jnp.sum(piece * piece, axis=-1, keepdims=True)
    inverse = lax.rsqrt(total * (1.0 / (GROUP * WIDTH)) + EPSILON)
    for k in range(GROUP):
        columns = slice(k * WIDTH, (k + 1) * WIDTH)
        piece = held[k, rows].astype(F32) * inverse * gain_ref[:, columns]
        normed[rows, columns] = piece.astype(BF16)


def block_diagonal(matrix_ref, out_ref, offset):
    blocks, size, _ = matrix_ref.shape
    row = lax.broadcasted_iota(jnp.int32, (size, blocks * size), 0)
    column = lax.broadcasted_iota(jnp.int32, (size, blocks * size), 1)
    for b in range(blocks):
        select = (column == row + b * size).astype(F32).astype(BF16)
        spread = jnp.dot(matrix_ref[b], select, preferred_element_type=F32)
        out_ref[b * size : (b + 1) * size, offset : offset + blocks * size] = spread.astype(BF16)


def shifted(values, by, row, fill):
    return jnp.where(row >= by, pltpu.roll(values, by, 0), fill)


def mixer_rows(values, gates, offsets, taps, maps, rate):
    channels = values.shape[1]
    row = lax.broadcasted_iota(jnp.int32, values.shape, 0)
    wide = values.astype(F32)
    reach = taps.shape[0]
    total = taps[0:1] * shifted(wide, reach - 1, row, 0.0)
    for k in range(1, reach):
        by = reach - 1 - k
        total = total + taps[k : k + 1] * (shifted(wide, by, row, 0.0) if by else wide)
    conved = total.astype(BF16)
    both = jax.nn.sigmoid(jnp.dot(conved, maps, preferred_element_type=F32))
    decay = rate * both[:, :channels] + offsets
    factor = jnp.exp(decay)
    twice = 2.0 * decay
    small = -twice * (1.0 + twice * (0.5 + twice * (1.0 / 6.0 + twice * (1.0 / 24.0))))
    lost = jnp.where(twice > -0.03, small, 1.0 - factor * factor)
    state = jnp.sqrt(lost) * both[:, channels:] * conved.astype(F32)
    by = 1
    while by < SEQ_LEN:
        state = factor * shifted(state, by, row, 0.0) + state
        if 2 * by < SEQ_LEN:
            factor = factor * shifted(factor, by, row, 1.0)
        by *= 2
    gate = gates.astype(F32)
    gelu = 0.5 * gate * (1.0 + lax.erf(gate * (0.5**0.5)))
    return (state * gelu).astype(BF16)


ORDER = (
    "GS 0S 1S 2S", "X 0a 0b 0c", "0d 1a 1b 1c", "1d 2a 2b 2c", "2d 0g 0h 0l", "G+ G- 0e 0j",
    "0k 0f 0i 0m", "0n 1g 1h 1l", "1e 1j 1k 1f", "1i 1m 1n 2g", "2h 2l 2e 2j", "2k GB 2f 2i",
    "2m 2n 0o 0p", "0q 0r GF N0", "3S N1 N2 1o", "1p 1q 1r N3", "2o 2p 2q 2r", "0F 4S 3a 3b",
    "1F I0 2F I1", "3c 3d M0 M1", "M2 M3 P0 P1", "P2 P3 4a 4b", "K0 K1 K2 3h", "3l K3 3g 4d",
    "4c R0+ R0- 3k", "R1+ R1- 3e 3f", "R2+ R2- 3i 3j", "3m 3n R3+ R3-", "4g 4h 4l L0", "L1 4k L2 L3",
    "4f 4n 4m A0+", "A0- 4e 4i 4j", "A1+ A1- A2+ A2-", "3o 3p 3q 3r", "A3+ A3- B0 B1", "B2 Q0 Q1 B3",
    "4o 4p 4q 4r", "Q2 Q3 3F U0", "U1 U2 4F U3", "V0 V1 V2 V3", "k0 k1 k2 k3", "r0+ r0- r1+ r1-",
    "r2+ r2- r3+ r3-", "l0 l1 l2 l3",
)


def kernel(
    stream_ref, gain1_hbm, gain2_hbm, input_ref, gate_ref, taps_hbm, decay_hbm, inmap_hbm, param_hbm, offset_hbm,
    output_ref, up_ref, down_ref,
    out_hbm,
    w_input, w_gate, w_output, w_up, w_down,
    held1, held2, normed, values, gates, offsets, mixed, activity, maps,
    terms1, core1, chip1, near1, last1, terms2, core2, chip2, near2, last2,
    gain1, gain2, taps_ref, decay_ref, inmap_ref, param_ref, rate_ref, out_ref,
    local_sem, out_sem, wsend, wrecv, tsend, trecv,
):
    p = Place()
    barrier = pltpu.get_barrier_semaphore()
    greeted = [dict(x=1), dict(x=-1), dict(y=1), dict(y=-1), dict(z=1), dict(z=-1), dict(flip=True)]
    for where in greeted:
        pl.semaphore_signal(barrier, inc=1, device_id=p.device(**where), device_id_type=MESH)
    weights = [
        WeightGather(p, i, own, held, local_sem, wsend, wrecv)
        for i, (own, held) in enumerate(
            (
                (input_ref, w_input),
                (gate_ref, w_gate),
                (output_ref, w_output),
                (up_ref, w_up),
                (down_ref, w_down),
            )
        )
    ]
    own_stream = pltpu.make_async_copy(stream_ref, held1.at[p.tp], local_sem.at[5])
    small = [
        pltpu.make_async_copy(source, target, local_sem.at[6 + k])
        for k, (source, target) in enumerate(
            (
                (decay_hbm, decay_ref),
                (inmap_hbm, inmap_ref),
                (param_hbm, param_ref),
                (gain1_hbm, gain1),
                (gain2_hbm, gain2),
                (taps_hbm, taps_ref),
                (offset_hbm, offsets),
            )
        )
    ]
    for copy in (weights[0].local, own_stream, *(w.local for w in weights[1:]), *small):
        copy.start()
    pl.semaphore_wait(barrier, len(greeted))

    gather1 = TokenGather(p, 0, held1, 0, ROWS, tsend, trecv)
    gather2 = [TokenGather(p, 1 + c, held2, c * PART, PART, tsend, trecv) for c in range(PARTS)]
    sum1 = [
        TokenSum(p, 1 + PARTS + c, c, terms1, core1, chip1, near1, last1, tsend, trecv) for c in range(PARTS)
    ]
    sum2 = [
        TokenSum(p, 1 + 2 * PARTS + c, c, terms2, core2, chip2, near2, last2, tsend, trecv) for c in range(PARTS)
    ]
    hidden = w_up.shape[-1]
    writes = [
        pltpu.make_async_copy(out_ref.at[pl.ds(c * PART, PART)], out_hbm.at[pl.ds(c * PART, PART)], out_sem.at[c])
        for c in range(PARTS)
    ]

    def rows_of(c):
        return pl.ds(c * PART, PART)

    def prepare():
        for copy in small:
            copy.wait()
        block_diagonal(decay_ref, maps, 0)
        block_diagonal(inmap_ref, maps, WIDTH)
        parameter = -param_ref[...]
        softplus = jnp.maximum(parameter, 0.0) + jnp.log1p(jnp.exp(-jnp.abs(parameter)))
        rate_ref[...] = -DECAY_MULTIPLIER * softplus

    def begin():
        own_stream.wait()
        gather1.begin()

    def columns_of(held, j, depth):
        pair = held[2 * j : 2 * j + 2].reshape(2, depth, 128)
        return jnp.concatenate([pair[0], pair[1]], axis=1)

    def inward(m):
        rows = pl.ds(m * (ROWS // 2), ROWS // 2)
        columns = normed[rows, :]
        for held, target in ((w_input, values), (w_gate, gates)):
            full = held[...].reshape(GROUP * WIDTH, WIDTH)
            target[rows, :] = jnp.dot(columns, full, preferred_element_type=F32).astype(BF16)

    def mix(c):
        rows = rows_of(c)
        taps = taps_ref[...].astype(F32)
        mixed[rows, :] = mixer_rows(values[rows, :], gates[rows, :], offsets[rows, :], taps, maps[...], rate_ref[...])

    def project(c, source, held, depth, terms, total):
        rows = rows_of(c)
        for j in range(GROUP):
            product = jnp.dot(source[rows, :], columns_of(held, j, depth), preferred_element_type=F32)
            terms[j // 2, j % 2, rows] = product.astype(BF16)
        total.begin()

    def middle_of(c):
        rows = rows_of(c)
        held2[p.tp, rows] = sum1[c].finish(held1[p.tp, rows])
        gather2[c].begin()

    def raise_rows(c):
        gather2[c].finish()
        norm_rows(held2, rows_of(c), gain2, normed)

    def lift(c):
        rows = rows_of(c)
        columns = normed[rows, :]
        for n in range(hidden // WIDTH):
            some = slice(n * WIDTH, (n + 1) * WIDTH)
            full = w_up[:, :, :, :, some].reshape(GROUP * WIDTH, WIDTH)
            raised = jnp.maximum(jnp.dot(columns, full, preferred_element_type=F32), 0.0)
            activity[rows, some] = (raised * raised).astype(BF16)

    def last_of(c):
        rows = rows_of(c)
        out_ref[rows, :] = sum2[c].finish(held2[p.tp, rows])
        writes[c].start()

    actions = {
        "X": prepare,
        "GS": begin,
        "G+": lambda: gather1.near("+"),
        "G-": lambda: gather1.near("-"),
        "GB": gather1.far,
        "GF": gather1.finish,
        "I0": lambda: inward(0),
        "I1": lambda: inward(1),
    }
    for i, w in enumerate(weights):
        for name in STEPS:
            actions[f"{i}{name}"] = functools.partial(w.step, name)
        actions[f"{i}F"] = w.finish
    for c in range(PARTS):
        actions[f"N{c}"] = functools.partial(norm_rows, held1, rows_of(c), gain1, normed)
        actions[f"M{c}"] = functools.partial(mix, c)
        actions[f"P{c}"] = functools.partial(project, c, mixed, w_output, WIDTH, terms1, sum1[c])
        actions[f"K{c}"] = sum1[c].cores
        actions[f"L{c}"] = functools.partial(middle_of, c)
        actions[f"B{c}"] = gather2[c].far
        actions[f"Q{c}"] = functools.partial(raise_rows, c)
        actions[f"U{c}"] = functools.partial(lift, c)
        actions[f"V{c}"] = functools.partial(project, c, activity, w_down, hidden, terms2, sum2[c])
        actions[f"k{c}"] = sum2[c].cores
        actions[f"l{c}"] = functools.partial(last_of, c)
        for sign in "+-":
            actions[f"R{c}{sign}"] = functools.partial(sum1[c].ring, sign)
            actions[f"A{c}{sign}"] = functools.partial(gather2[c].near, sign)
            actions[f"r{c}{sign}"] = functools.partial(sum2[c].ring, sign)
    order = " ".join(ORDER).split()
    assert sorted(order) == sorted(actions)
    for name in order:
        actions[name]()

    for w in weights:
        w.drain()
    for event in (gather1, *gather2, *sum1, *sum2):
        event.drain()
    for write in writes:
        write.wait()


def quarters(weight):
    rows, columns = weight.shape
    return weight.reshape(2, 2, rows // 4, columns)


def shards(
    stream,
    recurrent_norm_gain,
    feedforward_norm_gain,
    recurrent_input_weight,
    output_gate_weight,
    causal_filter_weight,
    decay_gate_matrix,
    input_gate_matrix,
    channel_decay_param,
    token_decay_offset,
    recurrent_output_weight,
    up_projection_weight,
    down_projection_weight,
):
    cut = [
        quarters(w)
        for w in (
            recurrent_input_weight,
            output_gate_weight,
            recurrent_output_weight,
            up_projection_weight,
            down_projection_weight,
        )
    ]
    hidden = up_projection_weight.shape[1]
    far = pl.BlockSpec(memory_space=pltpu.HBM)
    sums = [
        pltpu.VMEM((4, 2, ROWS, WIDTH), BF16),
        pltpu.VMEM((4, ROWS, WIDTH), BF16),
        pltpu.VMEM((4, ROWS, WIDTH), BF16),
        pltpu.VMEM((2, ROWS, WIDTH), BF16),
        pltpu.VMEM((2, ROWS, WIDTH), BF16),
    ]
    events = 1 + 3 * PARTS
    return pl.pallas_call(
        kernel,
        out_shape=jax.ShapeDtypeStruct(stream.shape, stream.dtype),
        in_specs=[far] * 13,
        out_specs=far,
        scratch_shapes=[
            *[pltpu.VMEM((16, *w.shape), BF16) for w in cut],
            pltpu.VMEM((GROUP, ROWS, WIDTH), BF16),
            pltpu.VMEM((GROUP, ROWS, WIDTH), BF16),
            pltpu.VMEM((ROWS, GROUP * WIDTH), BF16),
            pltpu.VMEM((ROWS, WIDTH), BF16),
            pltpu.VMEM((ROWS, WIDTH), BF16),
            pltpu.VMEM((ROWS, WIDTH), F32),
            pltpu.VMEM((ROWS, WIDTH), BF16),
            pltpu.VMEM((ROWS, hidden), BF16),
            pltpu.VMEM((WIDTH, 2 * WIDTH), BF16),
            *sums,
            *sums,
            pltpu.VMEM((1, GROUP * WIDTH), F32),
            pltpu.VMEM((1, GROUP * WIDTH), F32),
            pltpu.VMEM(causal_filter_weight.shape, BF16),
            pltpu.VMEM(decay_gate_matrix.shape, BF16),
            pltpu.VMEM(input_gate_matrix.shape, BF16),
            pltpu.VMEM((1, WIDTH), F32),
            pltpu.VMEM((1, WIDTH), F32),
            pltpu.VMEM((ROWS, WIDTH), BF16),
            pltpu.SemaphoreType.DMA((13,)),
            pltpu.SemaphoreType.DMA((PARTS,)),
            pltpu.SemaphoreType.DMA((5,)),
            pltpu.SemaphoreType.DMA((5, len(KINDS))),
            pltpu.SemaphoreType.DMA((events,)),
            pltpu.SemaphoreType.DMA((events, 4)),
        ],
        compiler_params=pltpu.CompilerParams(
            collective_id=0, has_side_effects=True, vmem_limit_bytes=60 * 1024 * 1024
        ),
    )(
        stream,
        recurrent_norm_gain.reshape(1, -1),
        feedforward_norm_gain.reshape(1, -1),
        cut[0],
        cut[1],
        causal_filter_weight,
        decay_gate_matrix,
        input_gate_matrix,
        channel_decay_param.reshape(1, -1),
        token_decay_offset,
        cut[2],
        cut[3],
        cut[4],
    )


def solution(mesh):
    split = Mesh(
        mesh.devices.reshape(mesh.shape["rep"], 4, 4, mesh.shape["tp"]),
        AXES,
    )
    placed = (
        P(REP_FS, "tp"),
        P(),
        P(),
        P(FS, "tp"),
        P(FS, "tp"),
        P(None, "tp"),
        P("tp", None, None),
        P("tp", None, None),
        P("tp"),
        P(REP_FS, "tp"),
        P("tp", FS),
        P(FS, "tp"),
        P("tp", FS),
    )
    return jax.shard_map(
        shards, mesh=split, in_specs=placed, out_specs=P(REP_FS, "tp"), check_vma=False
    )
```

```python
import functools

import jax
import jax.numpy as jnp
from jax import lax
from jax.experimental import pallas as pl
from jax.experimental.pallas import tpu as pltpu
from jax.sharding import Mesh
from jax.sharding import PartitionSpec as P

MESH = pl.DeviceIdType.MESH
SEQ_LEN = 128
FS = ("fs_0", "fs_1")
REP_FS = ("rep", "fs_0", "fs_1")
AXES = ("rep", "fs_0", "fs_1", "tp")

EPSILON = 1e-06
DECAY_MULTIPLIER = 8.0
F32 = jnp.float32
BF16 = jnp.bfloat16

ROWS, WIDTH, PARTS, GROUP = 512, 256, 4, 8
PART = ROWS // PARTS
HALF = PART // 2
TALL = ROWS // 2
VMEM_LIMIT = 60 * 1024 * 1024
TURNS = (0, -1, 1, 2, 2)

EVERY = slice(None)
STEPS = {
    "S": ((), (("oy+", 0, 0, ()), ("oy-", 0, 0, ()), ("oz+", 0, 0, ()), ("oz-", 0, 0, ()))),
    "a": (
        ("o",),
        (
            ("ry+", 0, -1, (EVERY, 0)), ("rz+", -1, 0, (EVERY, 0)), ("ry-", 0, 1, (EVERY, 1)), ("rz-", 1, 0, (EVERY, 1)),
            ("a1z+", 0, -1, (0,)), ("a1z-", 0, -1, (0,)), ("b1y+", -1, 0, (1,)), ("b1y-", -1, 0, (1,)),
            ("a3z+", 0, 1, (0,)), ("a3z-", 0, 1, (0,)), ("b3y+", 1, 0, (1,)), ("b3y-", 1, 0, (1,)),
        ),
    ),
    "e": (
        ("r",),
        (("a2z+", 0, 2, (0,)), ("a2z-", 0, 2, (0,)), ("b2y+", 2, 0, (1,)), ("b2y-", 2, 0, (1,))),
    ),
    "g": (
        ("1",),
        (("f1z+", -1, -1, (0, 0)), ("f1z-", 1, -1, (0, 1)), ("g1y+", -1, -1, (1, 0)), ("g1y-", -1, 1, (1, 1))),
    ),
    "h": (
        ("3",),
        (("f3z+", -1, 1, (0, 0)), ("f3z-", 1, 1, (0, 1)), ("g3y+", 1, -1, (1, 0)), ("g3y-", 1, 1, (1, 1))),
    ),
    "i": (
        ("2",),
        (("f2z+", -1, 2, (0, 0)), ("f2z-", 1, 2, (0, 1)), ("g2y+", 2, -1, (1, 0)), ("g2y-", 2, 1, (1, 1))),
    ),
}
GROUPS = {
    "o": 16, "r": 8, "1": 8, "3": 8, "2": 8, "down": 2, "up": 2, "beside": 4, "opposite": 4,
}
NAMES = list(GROUPS)


def group_of(name):
    if name[0] in "or":
        return name[0]
    if name[0] in "ab":
        return name[1]
    if name[1] == "2":
        return "opposite"
    return "beside" if name[0] == "f" else {"1": "down", "3": "up"}[name[1]]


def wrap(value, n):
    return lax.rem(value + n, n)


class Place:
    def __init__(self):
        self.rep, self.z, self.y, self.tp = (lax.axis_index(a) for a in AXES)
        self.whole_z = self.rep * 4 + self.z
        self.x, self.core = self.tp // 2, lax.rem(self.tp, 2)
        self.other = 1 - self.core

    def device(self, x=0, y=0, z=0, flip=False):
        z_there = wrap(self.whole_z + z, 8)
        core = self.other if flip else self.core
        return (z_there // 4, lax.rem(z_there, 4), wrap(self.y + y, 4), wrap(self.x + x, 4) * 2 + core)

    def shard(self, z=0, y=0):
        return wrap(self.z + z, 4) * 4 + wrap(self.y + y, 4)

    def slot(self, x=0, flip=False):
        return wrap(self.x + x, 4) * 2 + (self.other if flip else self.core)


class WeightGather:
    def __init__(self, place, index, own_ref, held, local_sem, send_sem, recv_sems):
        self.p, self.i, self.own, self.held = place, index, own_ref, held
        self.local = pltpu.make_async_copy(own_ref, held.at[place.shard()], local_sem.at[index])
        self.send_sem, self.recv_sems = send_sem.at[index], recv_sems

    def go(self, kind, z, y, part):
        where = {"y+": dict(y=1), "y-": dict(y=-1), "z+": dict(z=1), "z-": dict(z=-1)}[kind[-2:]]
        view = self.held.at[(self.p.shard(z, y), *part)]
        copy = pltpu.make_async_remote_copy(
            src_ref=view,
            dst_ref=view,
            send_sem=self.send_sem,
            recv_sem=self.recv_sems.at[self.i, NAMES.index(group_of(kind))],
            device_id=self.p.device(**where),
            device_id_type=MESH,
        )
        copy.start()

    def step(self, name):
        if name == "S":
            self.local.wait()
        waits, sends = STEPS[name]
        self.arrived(*waits)
        for message in sends:
            self.go(*message)

    def arrived(self, *groups):
        for name in groups:
            quarters = GROUPS[name]
            view = self.held.at[pl.ds(0, quarters // 4)] if quarters >= 4 else self.held.at[0, 0]
            pltpu.make_async_copy(view, view, self.recv_sems.at[self.i, NAMES.index(name)]).wait()

    def drain(self):
        view = self.held.at[pl.ds(0, 15)]
        pltpu.make_async_copy(view, view, self.send_sem).wait()


class TokenGather:
    def __init__(self, place, index, held, start, rows, send_sems, recv_sems):
        self.p, self.held, self.start, self.rows = place, held, start, rows
        self.send_sem, self.recv_sems = send_sems.at[index], recv_sems.at[index]
        self.sent = {}

    def go(self, name, sem, slot, device, start=0, rows=None):
        view = self.held.at[slot, pl.ds(self.start + start, rows or self.rows)]
        copy = pltpu.make_async_remote_copy(
            src_ref=view,
            dst_ref=view,
            send_sem=self.send_sem,
            recv_sem=self.recv_sems.at[sem],
            device_id=device,
            device_id_type=MESH,
        )
        copy.start()
        self.sent[name] = copy

    def slots_of(self, slots, sem):
        view = self.held.at[pl.ds(0, slots), pl.ds(self.start, self.rows)]
        pltpu.make_async_copy(view, view, sem).wait()

    def begin(self):
        p = self.p
        self.go("o+", 0, p.slot(), p.device(x=1))
        self.go("o-", 0, p.slot(), p.device(x=-1))
        self.go("p0", 2, p.slot(), p.device(flip=True))

    def near(self):
        p, half = self.p, self.rows // 2
        self.slots_of(2, self.recv_sems.at[0])
        self.go("f+", 1, p.slot(x=-1), p.device(x=1), 0, half)
        self.go("f-", 1, p.slot(x=1), p.device(x=-1), half, half)
        self.go("p1", 2, p.slot(x=-1), p.device(flip=True))
        self.go("p3", 2, p.slot(x=1), p.device(flip=True))

    def far(self):
        p = self.p
        self.slots_of(1, self.recv_sems.at[1])
        self.go("p2", 2, p.slot(x=2), p.device(flip=True))

    def finish(self):
        self.slots_of(4, self.recv_sems.at[2])

    def drain(self):
        self.slots_of(7, self.send_sem)


class TokenSum:
    def __init__(self, place, index, part, terms, from_core, chip, near, last, send_sems, recv_sems):
        self.p, self.part, self.rows = place, part, pl.ds(part * PART, PART)
        self.terms, self.from_core, self.chip, self.near, self.last = terms, from_core, chip, near, last
        self.send_sem, self.recv_sems = send_sems.at[index], recv_sems.at[index]
        self.sent = {}

    def go(self, name, sem, src, dst, device):
        copy = pltpu.make_async_remote_copy(
            src_ref=src,
            dst_ref=dst,
            send_sem=self.send_sem,
            recv_sem=self.recv_sems.at[sem],
            device_id=device,
            device_id_type=MESH,
        )
        copy.start()
        self.sent[name] = copy

    def half(self, h):
        return pl.ds(self.part * PART + h * HALF, HALF)

    def begin(self):
        p = self.p
        self.go("d", 0, self.terms.at[:, p.other, self.rows], self.from_core.at[:, self.rows], p.device(flip=True))

    def chip_sum(self, x):
        p = self.p
        there = wrap(p.x + x, 4)
        return self.terms[there, p.core, self.rows].astype(F32) + self.from_core[there, self.rows].astype(F32)

    def cores(self):
        p, chip = self.p, self.chip
        self.sent["d"].wait_recv()
        right, left, far = wrap(p.x + 1, 4), wrap(p.x - 1, 4), wrap(p.x + 2, 4)
        chip[far, self.rows] = self.chip_sum(2).astype(BF16)
        self.go("h+", 1, chip.at[far, self.half(0)], self.near.at[0, self.half(0)], p.device(x=1))
        self.go("h-", 1, chip.at[far, self.half(1)], self.near.at[1, self.half(1)], p.device(x=-1))
        chip[right, self.rows] = self.chip_sum(1).astype(BF16)
        self.go("e+", 2, chip.at[right, self.half(1)], self.last.at[0, self.half(1)], p.device(x=1))
        chip[left, self.rows] = self.chip_sum(-1).astype(BF16)
        self.go("e-", 2, chip.at[left, self.half(0)], self.last.at[1, self.half(0)], p.device(x=-1))

    def ring(self):
        p = self.p
        both = self.near.at[0, self.rows]
        pltpu.make_async_copy(both, both, self.recv_sems.at[1]).wait()
        for x, side in ((1, 0), (-1, 1)):
            rows = self.half(side)
            total = self.chip[wrap(p.x + x, 4), rows].astype(F32) + self.near[side, rows].astype(F32)
            self.near[side, rows] = total.astype(BF16)
            self.go("e2", 2, self.near.at[side, rows], self.last.at[side, rows], p.device(x=x))

    def finish(self, base):
        both = self.last.at[:, self.rows]
        pltpu.make_async_copy(both, both, self.recv_sems.at[2]).wait()
        total = self.chip_sum(0) + (self.last[0, self.rows].astype(F32) + self.last[1, self.rows].astype(F32))
        return (base.astype(F32) + total).astype(BF16)

    def drain(self):
        view = self.terms.at[:, 0, self.rows]
        part = self.chip.at[pl.ds(0, 3), self.rows]
        pltpu.make_async_copy(view, view, self.send_sem).wait()
        pltpu.make_async_copy(part, part, self.send_sem).wait()


class ColumnSum:
    def __init__(self, place, index, part, terms, from_core, chip, near, last, send_sems, recv_sems):
        self.p, self.start, self.rows = place, part * TALL, pl.ds(part * TALL, TALL)
        self.terms, self.from_core, self.chip, self.near, self.last = terms, from_core, chip, near, last
        self.send_sem, self.recv_sems = send_sems.at[index], recv_sems.at[index]

    def go(self, sem, src, dst, device):
        pltpu.make_async_remote_copy(
            src_ref=src,
            dst_ref=dst,
            send_sem=self.send_sem,
            recv_sem=self.recv_sems.at[sem],
            device_id=device,
            device_id_type=MESH,
        ).start()

    def arrived(self, view, sem):
        pltpu.make_async_copy(view, view, self.recv_sems.at[sem]).wait()

    def half(self, h):
        return pl.ds(self.start + h * (TALL // 2), TALL // 2)

    def chip_sum(self, there, rows):
        return self.terms[there, self.p.core, rows].astype(F32) + self.from_core[there, rows].astype(F32)

    def begin(self, k, core=None):
        there = wrap(self.p.z + k, 4)

        def send():
            terms = self.terms.at[there, self.p.other, self.rows]
            self.go(k, terms, self.from_core.at[there, self.rows], self.p.device(flip=True))

        if core is None:
            send()
        else:
            pl.when(core != self.p.core)(send)

    def away(self, k, core):
        there = wrap(self.p.z + k, 4)
        away = wrap(there - self.p.x, 4)
        return there, away if core is None else jnp.where(core == self.p.core, away, 4)

    def cores(self, k, core=None):
        p, chip = self.p, self.chip
        there, away = self.away(k, core)
        arrived = functools.partial(self.arrived, self.from_core.at[0, self.rows], k)
        if core is None:
            arrived()
        else:
            pl.when(core == p.core)(arrived)

        def add(rows):
            chip[there, rows] = self.chip_sum(there, rows).astype(BF16)

        @pl.when(away == 2)
        def _():
            add(self.rows)
            self.go(4, chip.at[there, self.half(0)], self.near.at[0, self.half(0)], p.device(x=1))
            self.go(5, chip.at[there, self.half(1)], self.near.at[1, self.half(1)], p.device(x=-1))

        for distance, x, side in ((1, 1, 0), (3, -1, 1)):

            @pl.when(away == distance)
            def _(x=x, side=side):
                rows = self.half(1 - side)
                add(rows)
                self.go(6, chip.at[there, rows], self.last.at[side, rows], p.device(x=x))
                add(self.half(side))

    def ring(self, k, core=None):
        p = self.p
        there, away = self.away(k, core)
        for distance, x, side in ((1, 1, 0), (3, -1, 1)):

            @pl.when(away == distance)
            def _(x=x, side=side):
                rows = self.half(side)
                view = self.near.at[side, rows]
                self.arrived(view, 4 + side)
                total = self.chip[there, rows].astype(F32) + self.near[side, rows].astype(F32)
                self.near[side, rows] = total.astype(BF16)
                self.go(6, view, self.last.at[side, rows], p.device(x=x))

    def finish(self, base):
        self.arrived(self.last.at[:, self.rows], 6)
        total = self.chip_sum(self.p.x, self.rows)
        total = total + (self.last[0, self.rows].astype(F32) + self.last[1, self.rows].astype(F32))
        return (base.astype(F32) + total).astype(BF16)

    def drain(self):
        view = self.chip.at[:, self.rows]
        part = self.chip.at[pl.ds(0, 3), self.rows]
        pltpu.make_async_copy(view, view, self.send_sem).wait()
        pltpu.make_async_copy(part, part, self.send_sem).wait()


def norm_rows(held, rows, gain_ref, normed):
    total = jnp.zeros((PART, 1), F32)
    for k in range(GROUP):
        piece = held[k, rows].astype(F32)
        total = total + jnp.sum(piece * piece, axis=-1, keepdims=True)
    inverse = lax.rsqrt(total * (1.0 / (GROUP * WIDTH)) + EPSILON)
    for k in range(GROUP):
        columns = slice(k * WIDTH, (k + 1) * WIDTH)
        piece = held[k, rows].astype(F32) * inverse * gain_ref[:, columns]
        normed[rows, columns] = piece.astype(BF16)


def block_diagonal(matrix_ref, out_ref, offset):
    blocks, size, _ = matrix_ref.shape
    row = lax.broadcasted_iota(jnp.int32, (size, blocks * size), 0)
    column = lax.broadcasted_iota(jnp.int32, (size, blocks * size), 1)
    for b in range(blocks):
        select = (column == row + b * size).astype(F32).astype(BF16)
        spread = jnp.dot(matrix_ref[b], select, preferred_element_type=F32)
        out_ref[b * size : (b + 1) * size, offset : offset + blocks * size] = spread.astype(BF16)


def shifted(values, by, row, fill):
    return jnp.where(row >= by, pltpu.roll(values, by, 0), fill)


def mixer_rows(values, offsets, taps, maps, rate):
    channels = values.shape[1]
    row = lax.broadcasted_iota(jnp.int32, values.shape, 0)
    wide = values.astype(F32)
    reach = taps.shape[0]
    total = taps[0:1] * shifted(wide, reach - 1, row, 0.0)
    for k in range(1, reach):
        by = reach - 1 - k
        total = total + taps[k : k + 1] * (shifted(wide, by, row, 0.0) if by else wide)
    conved = total.astype(BF16)
    both = jax.nn.sigmoid(jnp.dot(conved, maps, preferred_element_type=F32))
    decay = rate * both[:, :channels] + offsets
    factor = jnp.exp(decay)
    twice = 2.0 * decay
    small = -twice * (1.0 + twice * (0.5 + twice * (1.0 / 6.0 + twice * (1.0 / 24.0))))
    lost = jnp.where(twice > -0.03, small, 1.0 - factor * factor)
    state = jnp.sqrt(lost) * both[:, channels:] * conved.astype(F32)
    by = 1
    while by < SEQ_LEN:
        state = factor * shifted(state, by, row, 0.0) + state
        if 2 * by < SEQ_LEN:
            factor = factor * shifted(factor, by, row, 1.0)
        by *= 2
    return state


def gated(state, gates):
    gate = gates.astype(F32)
    gelu = 0.5 * gate * (1.0 + lax.erf(gate * (0.5**0.5)))
    return (state * gelu).astype(BF16)


ORDER = (
    "0S 1S GS X", "2S 0a GA0 1a", "2a 0e GA1 0h", "GB0 GF0 1h 2e", "0g GB1 1e GF1", "0i 3S N0 N3",
    "N2 2g 1g N1", "2h 1i 2i 0F", "4S I0 5S I1", "3a M0 M2 1F", "M3 J1 J0 2F", "P0 M1 4a P1",
    "P2 K0 P3 K1", "5a 3g K2 3e", "K3 4e R0 5g", "R1 5e R2 5h", "4h 3i R3 6S", "4i L0 7S 8S",
    "3h L1 L2 4g", "6a 5i L3 A1", "A0 7a A2 8a", "6e A3 B2 3F", "7e B1 4F 6g", "B0 B3 7g Q1",
    "Q0 8e Q2 8g", "5F U02 6h Q3", "7h U10 U11 U00", "8h 6i U01 U12", "7i V0 8i V1", "V2 k00 V3 V4",
    "k10 k20 k11 k21", "k31 k30 k40 k01", "k41 r10 r00 r20", "r11 r01 r41 r40", "r31 r30 r21 l0", "l1",
)


def kernel(
    stream_ref, gain1_hbm, gain2_hbm, input_ref, gate_ref, taps_hbm, decay_hbm, inmap_hbm, param_hbm, offset_hbm,
    output_ref, up_ref, down_ref,
    out_hbm,
    w_input, w_gate, w_output, w_up0, w_up1, w_up2, w_down0, w_down1, w_down2,
    held1, held2, normed, values, gates, offsets, state, activity, maps,
    terms1, core1, chip1, near1, last1, terms2, core2, chip2, near2, last2,
    gain1, gain2, taps_ref, decay_ref, inmap_ref, param_ref, rate_ref, out_ref,
    local_sem, out_sem, wsend, wrecv, tsend, trecv, csend, crecv,
):
    w_up, w_down = (w_up0, w_up1, w_up2), (w_down0, w_down1, w_down2)
    p = Place()
    barrier = pltpu.get_barrier_semaphore()
    greeted = [dict(x=1), dict(x=-1), dict(y=1), dict(y=-1), dict(z=1), dict(z=-1), dict(flip=True)]
    for where in greeted:
        pl.semaphore_signal(barrier, inc=1, device_id=p.device(**where), device_id_type=MESH)
    blocks = range(len(w_up))
    weights = [
        WeightGather(p, i, own, held, local_sem, wsend, wrecv)
        for i, (own, held) in enumerate(
            (
                (input_ref, w_input),
                (gate_ref, w_gate),
                (output_ref, w_output),
                *((up_ref.at[:, :, :, n * WIDTH : (n + 1) * WIDTH], w_up[n]) for n in blocks),
                *((down_ref.at[n], w_down[n]) for n in blocks),
            )
        )
    ]
    own_stream = pltpu.make_async_copy(stream_ref, held1.at[p.tp], local_sem.at[9])
    small = [
        pltpu.make_async_copy(source, target, local_sem.at[10 + k])
        for k, (source, target) in enumerate(
            (
                (decay_hbm, decay_ref),
                (inmap_hbm, inmap_ref),
                (param_hbm, param_ref),
                (gain1_hbm, gain1),
                (gain2_hbm, gain2),
                (taps_hbm, taps_ref),
                (offset_hbm, offsets),
            )
        )
    ]
    for copy in (weights[0].local, own_stream, *(w.local for w in weights[1:]), *small):
        copy.start()
    pl.semaphore_wait(barrier, len(greeted))

    gather1 = [TokenGather(p, c, held1, c * TALL, TALL, tsend, trecv) for c in range(2)]
    gather2 = [TokenGather(p, 2 + c, held2, c * PART, PART, tsend, trecv) for c in range(PARTS)]
    sum1 = [
        TokenSum(p, 2 + PARTS + c, c, terms1, core1, chip1, near1, last1, tsend, trecv) for c in range(PARTS)
    ]
    sum2 = [ColumnSum(p, c, c, terms2, core2, chip2, near2, last2, csend, crecv) for c in range(2)]
    writes = [
        pltpu.make_async_copy(out_ref.at[pl.ds(c * TALL, TALL)], out_hbm.at[pl.ds(c * TALL, TALL)], out_sem.at[c])
        for c in range(2)
    ]

    def rows_of(c):
        return pl.ds(c * PART, PART)

    def prepare():
        for copy in small:
            copy.wait()
        block_diagonal(decay_ref, maps, 0)
        block_diagonal(inmap_ref, maps, WIDTH)
        parameter = -param_ref[...]
        softplus = jnp.maximum(parameter, 0.0) + jnp.log1p(jnp.exp(-jnp.abs(parameter)))
        rate_ref[...] = -DECAY_MULTIPLIER * softplus

    def begin():
        own_stream.wait()
        for gather in gather1:
            gather.begin()

    def columns_of(held, j, depth):
        pair = held[2 * j : 2 * j + 2].reshape(2, depth, 128)
        return jnp.concatenate([pair[0], pair[1]], axis=1)

    def in_halves(rows, held):
        deep = GROUP * WIDTH // 2
        low, high = (held[8 * h : 8 * h + 8].reshape(deep, WIDTH) for h in range(2))
        low = jnp.dot(normed[rows, :deep], low, preferred_element_type=F32)
        return low + jnp.dot(normed[rows, deep:], high, preferred_element_type=F32)

    def inward(m, held, target):
        rows = pl.ds(m * TALL, TALL)
        target[rows, :] = in_halves(rows, held).astype(BF16)

    def mix(c):
        rows = rows_of(c)
        taps = taps_ref[...].astype(F32)
        state[rows, :] = mixer_rows(values[rows, :], offsets[rows, :], taps, maps[...], rate_ref[...])

    def project(c):
        rows = rows_of(c)
        mixed = gated(state[rows, :], gates[rows, :])
        for j in range(GROUP):
            product = jnp.dot(mixed, columns_of(w_output, j, WIDTH), preferred_element_type=F32)
            terms1[j // 2, j % 2, rows] = product.astype(BF16)
        sum1[c].begin()

    def last_core(turn):
        near = p.y // 2
        return {3: near, 4: 1 - near}.get(turn)

    def lower(turn):
        z, core = TURNS[turn], last_core(turn)
        there = wrap(p.z + z, 4)
        for w in weights[-len(blocks) :]:
            w.arrived(*(() if turn == 0 else (NAMES[turn - 5],)))
        for c in range(2):
            rows = pl.ds(c * TALL, TALL)
            for k in (0, 1) if core is None else (core,):
                product = 0.0
                for n in blocks:
                    pair = w_down[n][pl.ds(there * 4 + 2 * k, 2)].reshape(2, WIDTH, 128)
                    columns = jnp.concatenate([pair[0], pair[1]], axis=1)
                    some = activity[rows, n * WIDTH : (n + 1) * WIDTH]
                    product = product + jnp.dot(some, columns, preferred_element_type=F32)
                terms2[there, k, rows] = product.astype(BF16)
            sum2[c].begin(z % 4, core)

    def middle_of(c):
        rows = rows_of(c)
        held2[p.tp, rows] = sum1[c].finish(held1[p.tp, rows])
        gather2[c].begin()

    def raise_rows(c):
        gather2[c].finish()
        norm_rows(held2, rows_of(c), gain2, normed)

    def lift(c, n):
        rows = pl.ds(c * TALL, TALL)
        raised = jnp.maximum(in_halves(rows, w_up[n]), 0.0)
        activity[rows, n * WIDTH : (n + 1) * WIDTH] = (raised * raised).astype(BF16)

    def last_of(c):
        rows = pl.ds(c * TALL, TALL)
        out_ref[rows, :] = sum2[c].finish(held2[p.tp, rows])
        writes[c].start()

    actions = {
        "X": prepare,
        "GS": begin,
    }
    for i, w in enumerate(weights):
        for name in STEPS:
            actions[f"{i}{name}"] = functools.partial(w.step, name)
        if i < 3 + len(blocks):
            actions[f"{i}F"] = functools.partial(w.arrived, *NAMES[-4:])
    for c in range(PARTS):
        actions[f"N{c}"] = functools.partial(norm_rows, held1, rows_of(c), gain1, normed)
        actions[f"M{c}"] = functools.partial(mix, c)
        actions[f"P{c}"] = functools.partial(project, c)
        actions[f"K{c}"] = sum1[c].cores
        actions[f"L{c}"] = functools.partial(middle_of, c)
        actions[f"B{c}"] = gather2[c].far
        actions[f"Q{c}"] = functools.partial(raise_rows, c)
        actions[f"R{c}"] = sum1[c].ring
        actions[f"A{c}"] = gather2[c].near
    for turn, z in enumerate(TURNS):
        actions[f"V{turn}"] = functools.partial(lower, turn)
        for c in range(2):
            actions[f"k{turn}{c}"] = functools.partial(sum2[c].cores, z % 4, last_core(turn))
            actions[f"r{turn}{c}"] = functools.partial(sum2[c].ring, z % 4, last_core(turn))
    for c in range(2):
        actions[f"GA{c}"] = gather1[c].near
        actions[f"GB{c}"] = gather1[c].far
        actions[f"GF{c}"] = gather1[c].finish
        actions[f"I{c}"] = functools.partial(inward, c, w_input, values)
        actions[f"J{c}"] = functools.partial(inward, c, w_gate, gates)
        for n in blocks:
            actions[f"U{c}{n}"] = functools.partial(lift, c, n)
        actions[f"l{c}"] = functools.partial(last_of, c)
    order = " ".join(ORDER).split()
    assert sorted(order) == sorted(actions)
    for name in order:
        actions[name]()

    for w in weights:
        w.drain()
    for event in (*gather1, *gather2, *sum1, *sum2):
        event.drain()
    for write in writes:
        write.wait()


def quarters(weight):
    rows, columns = weight.shape
    return weight.reshape(2, 2, rows // 4, columns)


def shards(
    stream,
    recurrent_norm_gain,
    feedforward_norm_gain,
    recurrent_input_weight,
    output_gate_weight,
    causal_filter_weight,
    decay_gate_matrix,
    input_gate_matrix,
    channel_decay_param,
    token_decay_offset,
    recurrent_output_weight,
    up_projection_weight,
    down_projection_weight,
):
    mixer = [quarters(w) for w in (recurrent_input_weight, output_gate_weight, recurrent_output_weight)]
    up, hidden = quarters(up_projection_weight), up_projection_weight.shape[1]
    blocks = hidden // WIDTH
    down = down_projection_weight.reshape(blocks, 2, 2, WIDTH // 4, -1)
    far = pl.BlockSpec(memory_space=pltpu.HBM)
    sums = [
        pltpu.VMEM((4, 2, ROWS, WIDTH), BF16),
        pltpu.VMEM((4, ROWS, WIDTH), BF16),
        pltpu.VMEM((4, ROWS, WIDTH), BF16),
        pltpu.VMEM((2, ROWS, WIDTH), BF16),
        pltpu.VMEM((2, ROWS, WIDTH), BF16),
    ]
    events = 2 + 2 * PARTS
    return pl.pallas_call(
        kernel,
        out_shape=jax.ShapeDtypeStruct(stream.shape, stream.dtype),
        in_specs=[far] * 13,
        out_specs=far,
        scratch_shapes=[
            *[pltpu.VMEM((16, *w.shape), BF16) for w in mixer],
            *[pltpu.VMEM((16, *up.shape[:-1], WIDTH), BF16)] * blocks,
            *[pltpu.VMEM((16, *down.shape[1:]), BF16)] * blocks,
            pltpu.VMEM((GROUP, ROWS, WIDTH), BF16),
            pltpu.VMEM((GROUP, ROWS, WIDTH), BF16),
            pltpu.VMEM((ROWS, GROUP * WIDTH), BF16),
            pltpu.VMEM((ROWS, WIDTH), BF16),
            pltpu.VMEM((ROWS, WIDTH), BF16),
            pltpu.VMEM((ROWS, WIDTH), F32),
            pltpu.VMEM((ROWS, WIDTH), F32),
            pltpu.VMEM((ROWS, hidden), BF16),
            pltpu.VMEM((WIDTH, 2 * WIDTH), BF16),
            *sums,
            *sums,
            pltpu.VMEM((1, GROUP * WIDTH), F32),
            pltpu.VMEM((1, GROUP * WIDTH), F32),
            pltpu.VMEM(causal_filter_weight.shape, BF16),
            pltpu.VMEM(decay_gate_matrix.shape, BF16),
            pltpu.VMEM(input_gate_matrix.shape, BF16),
            pltpu.VMEM((1, WIDTH), F32),
            pltpu.VMEM((1, WIDTH), F32),
            pltpu.VMEM((ROWS, WIDTH), BF16),
            pltpu.SemaphoreType.DMA((17,)),
            pltpu.SemaphoreType.DMA((2,)),
            pltpu.SemaphoreType.DMA((3 + 2 * blocks,)),
            pltpu.SemaphoreType.DMA((3 + 2 * blocks, len(GROUPS))),
            pltpu.SemaphoreType.DMA((events,)),
            pltpu.SemaphoreType.DMA((events, 3)),
            pltpu.SemaphoreType.DMA((2,)),
            pltpu.SemaphoreType.DMA((2, 7)),
        ],
        compiler_params=pltpu.CompilerParams(
            collective_id=0, has_side_effects=True, vmem_limit_bytes=VMEM_LIMIT
        ),
    )(
        stream,
        recurrent_norm_gain.reshape(1, -1),
        feedforward_norm_gain.reshape(1, -1),
        mixer[0],
        mixer[1],
        causal_filter_weight,
        decay_gate_matrix,
        input_gate_matrix,
        channel_decay_param.reshape(1, -1),
        token_decay_offset,
        mixer[2],
        up,
        down,
    )


def solution(mesh):
    split = Mesh(
        mesh.devices.reshape(mesh.shape["rep"], 4, 4, mesh.shape["tp"]),
        AXES,
    )
    placed = (
        P(REP_FS, "tp"),
        P(),
        P(),
        P(FS, "tp"),
        P(FS, "tp"),
        P(None, "tp"),
        P("tp", None, None),
        P("tp", None, None),
        P("tp"),
        P(REP_FS, "tp"),
        P("tp", FS),
        P(FS, "tp"),
        P("tp", FS),
    )
    return jax.shard_map(
        shards, mesh=split, in_specs=placed, out_specs=P(REP_FS, "tp"), check_vma=False
    )
```

```python
import functools

import jax
import jax.numpy as jnp
from jax import lax
from jax.experimental import pallas as pl
from jax.experimental.pallas import tpu as pltpu
from jax.sharding import Mesh
from jax.sharding import PartitionSpec as P

MESH = pl.DeviceIdType.MESH
SEQ_LEN = 128
FS = ("fs_0", "fs_1")
REP_FS = ("rep", "fs_0", "fs_1")
AXES = ("rep", "fs_0", "fs_1", "tp")

EPSILON = 1e-06
DECAY_MULTIPLIER = 8.0
F32 = jnp.float32
BF16 = jnp.bfloat16

ROWS, WIDTH, PARTS, GROUP = 512, 256, 4, 8
PART = ROWS // PARTS
HALF = PART // 2
TALL = ROWS // 2
VMEM_LIMIT = 60 * 1024 * 1024
TURNS = (0, -1, 1, 2, 2)

EVERY = slice(None)
STEPS = {
    "S": ((), (("oy+", 0, 0, ()), ("oy-", 0, 0, ()), ("oz+", 0, 0, ()), ("oz-", 0, 0, ()))),
    "a": (
        ("own",),
        (
            ("ry+", 0, -1, (EVERY, 0)), ("ry-", 0, 1, (EVERY, 1)),
            ("a1z+", 0, -1, (0,)), ("a1z-", 0, -1, (0,)), ("b1y+", -1, 0, (1,)), ("b1y-", -1, 0, (1,)),
            ("a3z+", 0, 1, (0,)), ("a3z-", 0, 1, (0,)), ("b3y+", 1, 0, (1,)), ("b3y-", 1, 0, (1,)),
        ),
    ),
    "b": ((), (("rz+", -1, 0, (EVERY, 0)), ("rz-", 1, 0, (EVERY, 1)))),
    "e": (("ry",), (("a2z+", 0, 2, (0,)), ("a2z-", 0, 2, (0,)))),
    "f": (("rz",), (("b2y+", 2, 0, (1,)), ("b2y-", 2, 0, (1,)))),
    "g": (
        ("by",),
        (("g1y+", -1, -1, (1, 0)), ("g1y-", -1, 1, (1, 1)), ("g3y+", 1, -1, (1, 0)), ("g3y-", 1, 1, (1, 1))),
    ),
    "h": (
        ("az",),
        (("f1z+", -1, -1, (0, 0)), ("f1z-", 1, -1, (0, 1)), ("f3z+", -1, 1, (0, 0)), ("f3z-", 1, 1, (0, 1))),
    ),
    "i": (("a2",), (("f2z+", -1, 2, (0, 0)), ("f2z-", 1, 2, (0, 1)))),
    "j": (("b2",), (("g2y+", 2, -1, (1, 0)), ("g2y-", 2, 1, (1, 1)))),
}
GROUPS = {
    "own": 16, "ry": 4, "rz": 4, "by": 8, "az": 8, "a2": 4, "b2": 4, "below": 2, "above": 2, "beside": 4, "opposite": 4,
}
NAMES = list(GROUPS)


def group_of(name):
    way, step, link = name[0], name[1], name[-2]
    if way in "or":
        return {"o": "own", "r": "r" + link}[way]
    if way in "ab":
        return way + ("2" if step == "2" else link)
    if step == "2":
        return "opposite"
    return "beside" if way == "f" else {"1": "below", "3": "above"}[step]


def wrap(value, n):
    return lax.rem(value + n, n)


class Place:
    def __init__(self):
        self.rep, self.z, self.y, self.tp = (lax.axis_index(a) for a in AXES)
        self.whole_z = self.rep * 4 + self.z
        self.x, self.core = self.tp // 2, lax.rem(self.tp, 2)
        self.other = 1 - self.core

    def device(self, x=0, y=0, z=0, flip=False):
        z_there = wrap(self.whole_z + z, 8)
        core = self.other if flip else self.core
        return (z_there // 4, lax.rem(z_there, 4), wrap(self.y + y, 4), wrap(self.x + x, 4) * 2 + core)

    def shard(self, z=0, y=0):
        return wrap(self.z + z, 4) * 4 + wrap(self.y + y, 4)

    def slot(self, x=0, flip=False):
        return wrap(self.x + x, 4) * 2 + (self.other if flip else self.core)


class WeightGather:
    def __init__(self, place, index, own_ref, held, local_sem, send_sem, recv_sems):
        self.p, self.i, self.own, self.held = place, index, own_ref, held
        self.local = pltpu.make_async_copy(own_ref, held.at[place.shard()], local_sem.at[index])
        self.send_sem, self.recv_sems = send_sem.at[index], recv_sems

    def go(self, kind, z, y, part):
        where = {"y+": dict(y=1), "y-": dict(y=-1), "z+": dict(z=1), "z-": dict(z=-1)}[kind[-2:]]
        view = self.held.at[(self.p.shard(z, y), *part)]
        copy = pltpu.make_async_remote_copy(
            src_ref=view,
            dst_ref=view,
            send_sem=self.send_sem,
            recv_sem=self.recv_sems.at[self.i, NAMES.index(group_of(kind))],
            device_id=self.p.device(**where),
            device_id_type=MESH,
        )
        copy.start()

    def step(self, name):
        if name == "S":
            self.local.wait()
        waits, sends = STEPS[name]
        self.arrived(*waits)
        for message in sends:
            self.go(*message)

    def arrived(self, *groups):
        for name in groups:
            quarters = GROUPS[name]
            view = self.held.at[pl.ds(0, quarters // 4)] if quarters >= 4 else self.held.at[0, 0]
            pltpu.make_async_copy(view, view, self.recv_sems.at[self.i, NAMES.index(name)]).wait()

    def drain(self):
        view = self.held.at[pl.ds(0, 15)]
        pltpu.make_async_copy(view, view, self.send_sem).wait()


class TokenGather:
    def __init__(self, place, index, held, start, rows, send_sems, recv_sems):
        self.p, self.held, self.start, self.rows = place, held, start, rows
        self.send_sem, self.recv_sems = send_sems.at[index], recv_sems.at[index]
        self.sent = {}

    def go(self, name, sem, slot, device, start=0, rows=None):
        view = self.held.at[slot, pl.ds(self.start + start, rows or self.rows)]
        copy = pltpu.make_async_remote_copy(
            src_ref=view,
            dst_ref=view,
            send_sem=self.send_sem,
            recv_sem=self.recv_sems.at[sem],
            device_id=device,
            device_id_type=MESH,
        )
        copy.start()
        self.sent[name] = copy

    def slots_of(self, slots, sem):
        view = self.held.at[pl.ds(0, slots), pl.ds(self.start, self.rows)]
        pltpu.make_async_copy(view, view, sem).wait()

    def begin(self):
        p = self.p
        self.go("o+", 0, p.slot(), p.device(x=1))
        self.go("o-", 0, p.slot(), p.device(x=-1))
        self.go("p0", 2, p.slot(), p.device(flip=True))

    def near(self):
        p, half = self.p, self.rows // 2
        self.slots_of(2, self.recv_sems.at[0])
        self.go("f+", 1, p.slot(x=-1), p.device(x=1), 0, half)
        self.go("f-", 1, p.slot(x=1), p.device(x=-1), half, half)
        self.go("p1", 2, p.slot(x=-1), p.device(flip=True))
        self.go("p3", 2, p.slot(x=1), p.device(flip=True))

    def far(self):
        p = self.p
        self.slots_of(1, self.recv_sems.at[1])
        self.go("p2", 2, p.slot(x=2), p.device(flip=True))

    def finish(self):
        self.slots_of(4, self.recv_sems.at[2])

    def drain(self):
        self.slots_of(7, self.send_sem)


class TokenSum:
    def __init__(self, place, index, part, terms, from_core, chip, near, last, send_sems, recv_sems):
        self.p, self.part, self.rows = place, part, pl.ds(part * PART, PART)
        self.terms, self.from_core, self.chip, self.near, self.last = terms, from_core, chip, near, last
        self.send_sem, self.recv_sems = send_sems.at[index], recv_sems.at[index]
        self.sent = {}

    def go(self, name, sem, src, dst, device):
        copy = pltpu.make_async_remote_copy(
            src_ref=src,
            dst_ref=dst,
            send_sem=self.send_sem,
            recv_sem=self.recv_sems.at[sem],
            device_id=device,
            device_id_type=MESH,
        )
        copy.start()
        self.sent[name] = copy

    def half(self, h):
        return pl.ds(self.part * PART + h * HALF, HALF)

    def begin(self):
        p = self.p
        self.go("d", 0, self.terms.at[:, p.other, self.rows], self.from_core.at[:, self.rows], p.device(flip=True))

    def chip_sum(self, x):
        p = self.p
        there = wrap(p.x + x, 4)
        return self.terms[there, p.core, self.rows].astype(F32) + self.from_core[there, self.rows].astype(F32)

    def cores(self):
        p, chip = self.p, self.chip
        self.sent["d"].wait_recv()
        right, left, far = wrap(p.x + 1, 4), wrap(p.x - 1, 4), wrap(p.x + 2, 4)
        chip[far, self.rows] = self.chip_sum(2).astype(BF16)
        self.go("h+", 1, chip.at[far, self.half(0)], self.near.at[0, self.half(0)], p.device(x=1))
        self.go("h-", 1, chip.at[far, self.half(1)], self.near.at[1, self.half(1)], p.device(x=-1))
        chip[right, self.rows] = self.chip_sum(1).astype(BF16)
        self.go("e+", 2, chip.at[right, self.half(1)], self.last.at[0, self.half(1)], p.device(x=1))
        chip[left, self.rows] = self.chip_sum(-1).astype(BF16)
        self.go("e-", 2, chip.at[left, self.half(0)], self.last.at[1, self.half(0)], p.device(x=-1))

    def ring(self):
        p = self.p
        both = self.near.at[0, self.rows]
        pltpu.make_async_copy(both, both, self.recv_sems.at[1]).wait()
        for x, side in ((1, 0), (-1, 1)):
            rows = self.half(side)
            total = self.chip[wrap(p.x + x, 4), rows].astype(F32) + self.near[side, rows].astype(F32)
            self.near[side, rows] = total.astype(BF16)
            self.go("e2", 2, self.near.at[side, rows], self.last.at[side, rows], p.device(x=x))

    def finish(self, base):
        both = self.last.at[:, self.rows]
        pltpu.make_async_copy(both, both, self.recv_sems.at[2]).wait()
        total = self.chip_sum(0) + (self.last[0, self.rows].astype(F32) + self.last[1, self.rows].astype(F32))
        return (base.astype(F32) + total).astype(BF16)

    def drain(self):
        view = self.terms.at[:, 0, self.rows]
        part = self.chip.at[pl.ds(0, 3), self.rows]
        pltpu.make_async_copy(view, view, self.send_sem).wait()
        pltpu.make_async_copy(part, part, self.send_sem).wait()


class ColumnSum:
    def __init__(self, place, index, part, terms, from_core, chip, near, last, send_sems, recv_sems):
        self.p, self.start, self.rows = place, part * TALL, pl.ds(part * TALL, TALL)
        self.terms, self.from_core, self.chip, self.near, self.last = terms, from_core, chip, near, last
        self.send_sem, self.recv_sems = send_sems.at[index], recv_sems.at[index]

    def go(self, sem, src, dst, device):
        pltpu.make_async_remote_copy(
            src_ref=src,
            dst_ref=dst,
            send_sem=self.send_sem,
            recv_sem=self.recv_sems.at[sem],
            device_id=device,
            device_id_type=MESH,
        ).start()

    def arrived(self, view, sem):
        pltpu.make_async_copy(view, view, self.recv_sems.at[sem]).wait()

    def half(self, h):
        return pl.ds(self.start + h * (TALL // 2), TALL // 2)

    def chip_sum(self, there, rows):
        return self.terms[there, self.p.core, rows].astype(F32) + self.from_core[there, rows].astype(F32)

    def begin(self, k, core=None):
        there = wrap(self.p.z + k, 4)

        def send():
            terms = self.terms.at[there, self.p.other, self.rows]
            self.go(k, terms, self.from_core.at[there, self.rows], self.p.device(flip=True))

        if core is None:
            send()
        else:
            pl.when(core != self.p.core)(send)

    def away(self, k, core):
        there = wrap(self.p.z + k, 4)
        away = wrap(there - self.p.x, 4)
        return there, away if core is None else jnp.where(core == self.p.core, away, 4)

    def cores(self, k, core=None):
        p, chip = self.p, self.chip
        there, away = self.away(k, core)
        arrived = functools.partial(self.arrived, self.from_core.at[0, self.rows], k)
        if core is None:
            arrived()
        else:
            pl.when(core == p.core)(arrived)

        def add(rows):
            chip[there, rows] = self.chip_sum(there, rows).astype(BF16)

        @pl.when(away == 2)
        def _():
            add(self.rows)
            self.go(4, chip.at[there, self.half(0)], self.near.at[0, self.half(0)], p.device(x=1))
            self.go(5, chip.at[there, self.half(1)], self.near.at[1, self.half(1)], p.device(x=-1))

        for distance, x, side in ((1, 1, 0), (3, -1, 1)):

            @pl.when(away == distance)
            def _(x=x, side=side):
                rows = self.half(1 - side)
                add(rows)
                self.go(6, chip.at[there, rows], self.last.at[side, rows], p.device(x=x))
                add(self.half(side))

    def ring(self, k, core=None):
        p = self.p
        there, away = self.away(k, core)
        for distance, x, side in ((1, 1, 0), (3, -1, 1)):

            @pl.when(away == distance)
            def _(x=x, side=side):
                rows = self.half(side)
                view = self.near.at[side, rows]
                self.arrived(view, 4 + side)
                total = self.chip[there, rows].astype(F32) + self.near[side, rows].astype(F32)
                self.near[side, rows] = total.astype(BF16)
                self.go(6, view, self.last.at[side, rows], p.device(x=x))

    def finish(self, base):
        self.arrived(self.last.at[:, self.rows], 6)
        total = self.chip_sum(self.p.x, self.rows)
        total = total + (self.last[0, self.rows].astype(F32) + self.last[1, self.rows].astype(F32))
        return (base.astype(F32) + total).astype(BF16)

    def drain(self):
        view = self.chip.at[:, self.rows]
        part = self.chip.at[pl.ds(0, 3), self.rows]
        pltpu.make_async_copy(view, view, self.send_sem).wait()
        pltpu.make_async_copy(part, part, self.send_sem).wait()


def norm_rows(held, rows, gain_ref, normed):
    total = jnp.zeros((PART, 1), F32)
    for k in range(GROUP):
        piece = held[k, rows].astype(F32)
        total = total + jnp.sum(piece * piece, axis=-1, keepdims=True)
    inverse = lax.rsqrt(total * (1.0 / (GROUP * WIDTH)) + EPSILON)
    for k in range(GROUP):
        columns = slice(k * WIDTH, (k + 1) * WIDTH)
        piece = held[k, rows].astype(F32) * inverse * gain_ref[:, columns]
        normed[rows, columns] = piece.astype(BF16)


def block_diagonal(matrix_ref, out_ref, offset):
    blocks, size, _ = matrix_ref.shape
    row = lax.broadcasted_iota(jnp.int32, (size, blocks * size), 0)
    column = lax.broadcasted_iota(jnp.int32, (size, blocks * size), 1)
    for b in range(blocks):
        select = (column == row + b * size).astype(F32).astype(BF16)
        spread = jnp.dot(matrix_ref[b], select, preferred_element_type=F32)
        out_ref[b * size : (b + 1) * size, offset : offset + blocks * size] = spread.astype(BF16)


def shifted(values, by, row, fill):
    return jnp.where(row >= by, pltpu.roll(values, by, 0), fill)


def mixer_rows(values, offsets, taps, maps, rate):
    channels = values.shape[1]
    row = lax.broadcasted_iota(jnp.int32, values.shape, 0)
    wide = values.astype(F32)
    reach = taps.shape[0]
    total = taps[0:1] * shifted(wide, reach - 1, row, 0.0)
    for k in range(1, reach):
        by = reach - 1 - k
        total = total + taps[k : k + 1] * (shifted(wide, by, row, 0.0) if by else wide)
    conved = total.astype(BF16)
    both = jax.nn.sigmoid(jnp.dot(conved, maps, preferred_element_type=F32))
    decay = rate * both[:, :channels] + offsets
    factor = jnp.exp(decay)
    twice = 2.0 * decay
    small = -twice * (1.0 + twice * (0.5 + twice * (1.0 / 6.0 + twice * (1.0 / 24.0))))
    lost = jnp.where(twice > -0.03, small, 1.0 - factor * factor)
    state = jnp.sqrt(lost) * both[:, channels:] * conved.astype(F32)
    by = 1
    while by < SEQ_LEN:
        state = factor * shifted(state, by, row, 0.0) + state
        if 2 * by < SEQ_LEN:
            factor = factor * shifted(factor, by, row, 1.0)
        by *= 2
    return state


def gated(state, gates):
    gate = gates.astype(F32)
    gelu = 0.5 * gate * (1.0 + lax.erf(gate * (0.5**0.5)))
    return (state * gelu).astype(BF16)


ORDER = (
    "0S 1S 2S GS", "X 0a 1a 0b", "1b 2a 2b GA0", "0e 0f GB0 GA1", "1e 1f 0g 2e", "1g 1h 2f 0h",
    "0i GF0 0j N1", "GB1 1j 1i 2h", "3S N0 2g GF1", "2i N2 2j N3", "0F 4S 1F 5S", "I1 I0 M0 M3",
    "3a 2F P0 P3", "M2 3b M1 6S", "4a P2 K0 P1", "K2 K1 K3 5a", "3e 4b 5b 6a", "R0 R1 R2 7S",
    "3h R3 8S L0", "5f 5g L1 5e", "5h 4f L3 4h", "6b 3f L2 4g", "4e 3i 5j 7a", "A0 7b 3g A1",
    "5i 3j 4j A3", "A2 4i 8a B0", "B1 6g Q0 7e", "Q1 3F 5F B3", "6f 8b 7g B2", "6e 4F U0 8e",
    "7h Q2 Q3 6h", "8h 8g 7f U1", "8f V0 8i 6i", "6j 7i V1 V2", "7j k01 8j V3", "k00 k10 k11 k21",
    "V4 k30 k20 r10", "k40 k41 k31 r21", "r00 r30 r01 r20", "r11 r40 r31 r41", "l0 l1",
)


def kernel(
    stream_ref, gain1_hbm, gain2_hbm, input_ref, gate_ref, taps_hbm, decay_hbm, inmap_hbm, param_hbm, offset_hbm,
    output_ref, up_ref, down_ref,
    out_hbm,
    w_input, w_gate, w_output, w_up0, w_up1, w_up2, w_down0, w_down1, w_down2,
    held1, held2, normed, values, gates, offsets, state, activity, maps,
    terms1, core1, chip1, near1, last1, terms2, core2, chip2, near2, last2,
    gain1, gain2, taps_ref, decay_ref, inmap_ref, param_ref, rate_ref, out_ref,
    local_sem, out_sem, wsend, wrecv, tsend, trecv, csend, crecv,
):
    w_up, w_down = (w_up0, w_up1, w_up2), (w_down0, w_down1, w_down2)
    p = Place()
    barrier = pltpu.get_barrier_semaphore()
    greeted = [dict(x=1), dict(x=-1), dict(y=1), dict(y=-1), dict(z=1), dict(z=-1), dict(flip=True)]
    for where in greeted:
        pl.semaphore_signal(barrier, inc=1, device_id=p.device(**where), device_id_type=MESH)
    blocks = range(len(w_up))
    weights = [
        WeightGather(p, i, own, held, local_sem, wsend, wrecv)
        for i, (own, held) in enumerate(
            (
                (input_ref, w_input),
                (gate_ref, w_gate),
                (output_ref, w_output),
                *((up_ref.at[:, :, :, n * WIDTH : (n + 1) * WIDTH], w_up[n]) for n in blocks),
                *((down_ref.at[n], w_down[n]) for n in blocks),
            )
        )
    ]
    own_stream = pltpu.make_async_copy(stream_ref, held1.at[p.tp], local_sem.at[9])
    small = [
        pltpu.make_async_copy(source, target, local_sem.at[10 + k])
        for k, (source, target) in enumerate(
            (
                (decay_hbm, decay_ref),
                (inmap_hbm, inmap_ref),
                (param_hbm, param_ref),
                (gain1_hbm, gain1),
                (gain2_hbm, gain2),
                (taps_hbm, taps_ref),
                (offset_hbm, offsets),
            )
        )
    ]
    for copy in (weights[0].local, own_stream, *(w.local for w in weights[1:]), *small):
        copy.start()
    pl.semaphore_wait(barrier, len(greeted))

    gather1 = [TokenGather(p, c, held1, c * TALL, TALL, tsend, trecv) for c in range(2)]
    gather2 = [TokenGather(p, 2 + c, held2, c * PART, PART, tsend, trecv) for c in range(PARTS)]
    sum1 = [
        TokenSum(p, 2 + PARTS + c, c, terms1, core1, chip1, near1, last1, tsend, trecv) for c in range(PARTS)
    ]
    sum2 = [ColumnSum(p, c, c, terms2, core2, chip2, near2, last2, csend, crecv) for c in range(2)]
    writes = [
        pltpu.make_async_copy(out_ref.at[pl.ds(c * TALL, TALL)], out_hbm.at[pl.ds(c * TALL, TALL)], out_sem.at[c])
        for c in range(2)
    ]

    def rows_of(c):
        return pl.ds(c * PART, PART)

    def prepare():
        for copy in small:
            copy.wait()
        block_diagonal(decay_ref, maps, 0)
        block_diagonal(inmap_ref, maps, WIDTH)
        parameter = -param_ref[...]
        softplus = jnp.maximum(parameter, 0.0) + jnp.log1p(jnp.exp(-jnp.abs(parameter)))
        rate_ref[...] = -DECAY_MULTIPLIER * softplus

    def begin():
        own_stream.wait()
        for gather in gather1:
            gather.begin()

    def columns_of(held, j, depth):
        pair = held[2 * j : 2 * j + 2].reshape(2, depth, 128)
        return jnp.concatenate([pair[0], pair[1]], axis=1)

    def inward(m):
        rows = pl.ds(m * TALL, TALL)
        columns = normed[rows, :]
        for held, target in ((w_input, values), (w_gate, gates)):
            full = held[...].reshape(GROUP * WIDTH, WIDTH)
            target[rows, :] = jnp.dot(columns, full, preferred_element_type=F32).astype(BF16)

    def mix(c):
        rows = rows_of(c)
        taps = taps_ref[...].astype(F32)
        state[rows, :] = mixer_rows(values[rows, :], offsets[rows, :], taps, maps[...], rate_ref[...])

    def project(c):
        rows = rows_of(c)
        mixed = gated(state[rows, :], gates[rows, :])
        for j in range(GROUP):
            product = jnp.dot(mixed, columns_of(w_output, j, WIDTH), preferred_element_type=F32)
            terms1[j // 2, j % 2, rows] = product.astype(BF16)
        sum1[c].begin()

    def last_core(turn):
        near = p.y // 2
        return {3: near, 4: 1 - near}.get(turn)

    def lower(turn):
        z, core = TURNS[turn], last_core(turn)
        there = wrap(p.z + z, 4)
        for w in weights[-len(blocks) :]:
            w.arrived(*(() if turn == 0 else (NAMES[turn - 5],)))
        for c in range(2):
            rows = pl.ds(c * TALL, TALL)
            for k in (0, 1) if core is None else (core,):
                product = 0.0
                for n in blocks:
                    pair = w_down[n][pl.ds(there * 4 + 2 * k, 2)].reshape(2, WIDTH, 128)
                    columns = jnp.concatenate([pair[0], pair[1]], axis=1)
                    some = activity[rows, n * WIDTH : (n + 1) * WIDTH]
                    product = product + jnp.dot(some, columns, preferred_element_type=F32)
                terms2[there, k, rows] = product.astype(BF16)
            sum2[c].begin(z % 4, core)

    def middle_of(c):
        rows = rows_of(c)
        held2[p.tp, rows] = sum1[c].finish(held1[p.tp, rows])
        gather2[c].begin()

    def raise_rows(c):
        gather2[c].finish()
        norm_rows(held2, rows_of(c), gain2, normed)

    def lift(c):
        rows = pl.ds(c * TALL, TALL)
        columns = normed[rows, :]
        for n in blocks:
            full = w_up[n][...].reshape(GROUP * WIDTH, WIDTH)
            raised = jnp.maximum(jnp.dot(columns, full, preferred_element_type=F32), 0.0)
            activity[rows, n * WIDTH : (n + 1) * WIDTH] = (raised * raised).astype(BF16)

    def last_of(c):
        rows = pl.ds(c * TALL, TALL)
        out_ref[rows, :] = sum2[c].finish(held2[p.tp, rows])
        writes[c].start()

    actions = {
        "X": prepare,
        "GS": begin,
    }
    for i, w in enumerate(weights):
        for name in STEPS:
            actions[f"{i}{name}"] = functools.partial(w.step, name)
        if i < 3 + len(blocks):
            actions[f"{i}F"] = functools.partial(w.arrived, *NAMES[-4:])
    for c in range(PARTS):
        actions[f"N{c}"] = functools.partial(norm_rows, held1, rows_of(c), gain1, normed)
        actions[f"M{c}"] = functools.partial(mix, c)
        actions[f"P{c}"] = functools.partial(project, c)
        actions[f"K{c}"] = sum1[c].cores
        actions[f"L{c}"] = functools.partial(middle_of, c)
        actions[f"B{c}"] = gather2[c].far
        actions[f"Q{c}"] = functools.partial(raise_rows, c)
        actions[f"R{c}"] = sum1[c].ring
        actions[f"A{c}"] = gather2[c].near
    for turn, z in enumerate(TURNS):
        actions[f"V{turn}"] = functools.partial(lower, turn)
        for c in range(2):
            actions[f"k{turn}{c}"] = functools.partial(sum2[c].cores, z % 4, last_core(turn))
            actions[f"r{turn}{c}"] = functools.partial(sum2[c].ring, z % 4, last_core(turn))
    for c in range(2):
        actions[f"GA{c}"] = gather1[c].near
        actions[f"GB{c}"] = gather1[c].far
        actions[f"GF{c}"] = gather1[c].finish
        actions[f"I{c}"] = functools.partial(inward, c)
        actions[f"U{c}"] = functools.partial(lift, c)
        actions[f"l{c}"] = functools.partial(last_of, c)
    order = " ".join(ORDER).split()
    assert sorted(order) == sorted(actions)
    for name in order:
        actions[name]()

    for w in weights:
        w.drain()
    for event in (*gather1, *gather2, *sum1, *sum2):
        event.drain()
    for write in writes:
        write.wait()


def quarters(weight):
    rows, columns = weight.shape
    return weight.reshape(2, 2, rows // 4, columns)


def shards(
    stream,
    recurrent_norm_gain,
    feedforward_norm_gain,
    recurrent_input_weight,
    output_gate_weight,
    causal_filter_weight,
    decay_gate_matrix,
    input_gate_matrix,
    channel_decay_param,
    token_decay_offset,
    recurrent_output_weight,
    up_projection_weight,
    down_projection_weight,
):
    mixer = [quarters(w) for w in (recurrent_input_weight, output_gate_weight, recurrent_output_weight)]
    up, hidden = quarters(up_projection_weight), up_projection_weight.shape[1]
    blocks = hidden // WIDTH
    down = down_projection_weight.reshape(blocks, 2, 2, WIDTH // 4, -1)
    far = pl.BlockSpec(memory_space=pltpu.HBM)
    sums = [
        pltpu.VMEM((4, 2, ROWS, WIDTH), BF16),
        pltpu.VMEM((4, ROWS, WIDTH), BF16),
        pltpu.VMEM((4, ROWS, WIDTH), BF16),
        pltpu.VMEM((2, ROWS, WIDTH), BF16),
        pltpu.VMEM((2, ROWS, WIDTH), BF16),
    ]
    events = 2 + 2 * PARTS
    return pl.pallas_call(
        kernel,
        out_shape=jax.ShapeDtypeStruct(stream.shape, stream.dtype),
        in_specs=[far] * 13,
        out_specs=far,
        scratch_shapes=[
            *[pltpu.VMEM((16, *w.shape), BF16) for w in mixer],
            *[pltpu.VMEM((16, *up.shape[:-1], WIDTH), BF16)] * blocks,
            *[pltpu.VMEM((16, *down.shape[1:]), BF16)] * blocks,
            pltpu.VMEM((GROUP, ROWS, WIDTH), BF16),
            pltpu.VMEM((GROUP, ROWS, WIDTH), BF16),
            pltpu.VMEM((ROWS, GROUP * WIDTH), BF16),
            pltpu.VMEM((ROWS, WIDTH), BF16),
            pltpu.VMEM((ROWS, WIDTH), BF16),
            pltpu.VMEM((ROWS, WIDTH), F32),
            pltpu.VMEM((ROWS, WIDTH), F32),
            pltpu.VMEM((ROWS, hidden), BF16),
            pltpu.VMEM((WIDTH, 2 * WIDTH), BF16),
            *sums,
            *sums,
            pltpu.VMEM((1, GROUP * WIDTH), F32),
            pltpu.VMEM((1, GROUP * WIDTH), F32),
            pltpu.VMEM(causal_filter_weight.shape, BF16),
            pltpu.VMEM(decay_gate_matrix.shape, BF16),
            pltpu.VMEM(input_gate_matrix.shape, BF16),
            pltpu.VMEM((1, WIDTH), F32),
            pltpu.VMEM((1, WIDTH), F32),
            pltpu.VMEM((ROWS, WIDTH), BF16),
            pltpu.SemaphoreType.DMA((17,)),
            pltpu.SemaphoreType.DMA((2,)),
            pltpu.SemaphoreType.DMA((3 + 2 * blocks,)),
            pltpu.SemaphoreType.DMA((3 + 2 * blocks, len(GROUPS))),
            pltpu.SemaphoreType.DMA((events,)),
            pltpu.SemaphoreType.DMA((events, 3)),
            pltpu.SemaphoreType.DMA((2,)),
            pltpu.SemaphoreType.DMA((2, 7)),
        ],
        compiler_params=pltpu.CompilerParams(
            collective_id=0, has_side_effects=True, vmem_limit_bytes=VMEM_LIMIT
        ),
    )(
        stream,
        recurrent_norm_gain.reshape(1, -1),
        feedforward_norm_gain.reshape(1, -1),
        mixer[0],
        mixer[1],
        causal_filter_weight,
        decay_gate_matrix,
        input_gate_matrix,
        channel_decay_param.reshape(1, -1),
        token_decay_offset,
        mixer[2],
        up,
        down,
    )


def solution(mesh):
    split = Mesh(
        mesh.devices.reshape(mesh.shape["rep"], 4, 4, mesh.shape["tp"]),
        AXES,
    )
    placed = (
        P(REP_FS, "tp"),
        P(),
        P(),
        P(FS, "tp"),
        P(FS, "tp"),
        P(None, "tp"),
        P("tp", None, None),
        P("tp", None, None),
        P("tp"),
        P(REP_FS, "tp"),
        P("tp", FS),
        P(FS, "tp"),
        P("tp", FS),
    )
    return jax.shard_map(
        shards, mesh=split, in_specs=placed, out_specs=P(REP_FS, "tp"), check_vma=False
    )
```

```python
import functools

import jax
import jax.numpy as jnp
from jax import lax
from jax.experimental import pallas as pl
from jax.experimental.pallas import tpu as pltpu
from jax.sharding import Mesh
from jax.sharding import PartitionSpec as P

MESH = pl.DeviceIdType.MESH
SEQ_LEN = 128
FS = ("fs_0", "fs_1")
REP_FS = ("rep", "fs_0", "fs_1")
AXES = ("rep", "fs_0", "fs_1", "tp")

EPSILON = 1e-06
DECAY_MULTIPLIER = 8.0
F32 = jnp.float32
BF16 = jnp.bfloat16

ROWS, WIDTH, PARTS, GROUP = 512, 256, 4, 8
PART = ROWS // PARTS
HALF = PART // 2
TALL = ROWS // 2
VMEM_LIMIT = 40 * 1024 * 1024
TURNS = (0, -1, 1, 2, 2)

EVERY = slice(None)
STEPS = {
    "S": ((), (("oy+", 0, 0, ()), ("oy-", 0, 0, ()), ("oz+", 0, 0, ()), ("oz-", 0, 0, ()))),
    "a": (
        ("own",),
        (
            ("ry+", 0, -1, (EVERY, 0)), ("ry-", 0, 1, (EVERY, 1)),
            ("a1z+", 0, -1, (0,)), ("a1z-", 0, -1, (0,)), ("b1y+", -1, 0, (1,)), ("b1y-", -1, 0, (1,)),
            ("a3z+", 0, 1, (0,)), ("a3z-", 0, 1, (0,)), ("b3y+", 1, 0, (1,)), ("b3y-", 1, 0, (1,)),
        ),
    ),
    "b": ((), (("rz+", -1, 0, (EVERY, 0)), ("rz-", 1, 0, (EVERY, 1)))),
    "e": (("ry",), (("a2z+", 0, 2, (0,)), ("a2z-", 0, 2, (0,)))),
    "f": (("rz",), (("b2y+", 2, 0, (1,)), ("b2y-", 2, 0, (1,)))),
    "g": (
        ("by",),
        (("g1y+", -1, -1, (1, 0)), ("g1y-", -1, 1, (1, 1)), ("g3y+", 1, -1, (1, 0)), ("g3y-", 1, 1, (1, 1))),
    ),
    "h": (
        ("az",),
        (("f1z+", -1, -1, (0, 0)), ("f1z-", 1, -1, (0, 1)), ("f3z+", -1, 1, (0, 0)), ("f3z-", 1, 1, (0, 1))),
    ),
    "i": (("a2",), (("f2z+", -1, 2, (0, 0)), ("f2z-", 1, 2, (0, 1)))),
    "j": (("b2",), (("g2y+", 2, -1, (1, 0)), ("g2y-", 2, 1, (1, 1)))),
}
GROUPS = {
    "own": 16, "ry": 4, "rz": 4, "by": 8, "az": 8, "a2": 4, "b2": 4, "below": 2, "above": 2, "beside": 4, "opposite": 4,
}
NAMES = list(GROUPS)
TOGETHER = len(NAMES) - 3


def group_of(name):
    way, step, link = name[0], name[1], name[-2]
    if way in "or":
        return {"o": "own", "r": "r" + link}[way]
    if way in "ab":
        return way + ("2" if step == "2" else link)
    if step == "2":
        return "opposite"
    return "beside" if way == "f" else {"1": "below", "3": "above"}[step]


def wrap(value, n):
    return lax.rem(value + n, n)


class Place:
    def __init__(self):
        self.rep, self.z, self.y, self.tp = (lax.axis_index(a) for a in AXES)
        self.whole_z = self.rep * 4 + self.z
        self.x, self.core = self.tp // 2, lax.rem(self.tp, 2)
        self.other = 1 - self.core

    def device(self, x=0, y=0, z=0, flip=False):
        z_there = wrap(self.whole_z + z, 8)
        core = self.other if flip else self.core
        return (z_there // 4, lax.rem(z_there, 4), wrap(self.y + y, 4), wrap(self.x + x, 4) * 2 + core)

    def shard(self, z=0, y=0):
        return wrap(self.z + z, 4) * 4 + wrap(self.y + y, 4)

    def slot(self, x=0, flip=False):
        return wrap(self.x + x, 4) * 2 + (self.other if flip else self.core)


class WeightGather:
    def __init__(self, place, index, own_ref, held, local_sem, send_sem, recv_sems, apart):
        self.p, self.i, self.own, self.held = place, index, own_ref, held
        self.local = pltpu.make_async_copy(own_ref, held.at[place.shard()], local_sem.at[index])
        self.send_sem, self.recv_sems, self.apart = send_sem.at[index], recv_sems, apart

    def go(self, kind, z, y, part):
        where = {"y+": dict(y=1), "y-": dict(y=-1), "z+": dict(z=1), "z-": dict(z=-1)}[kind[-2:]]
        view = self.held.at[(self.p.shard(z, y), *part)]
        copy = pltpu.make_async_remote_copy(
            src_ref=view,
            dst_ref=view,
            send_sem=self.send_sem,
            recv_sem=self.semaphore(group_of(kind)),
            device_id=self.p.device(**where),
            device_id_type=MESH,
        )
        copy.start()

    def step(self, name):
        if name == "S":
            self.local.wait()
        waits, sends = STEPS[name]
        self.arrived(*waits)
        for message in sends:
            self.go(*message)

    def semaphore(self, name):
        k = NAMES.index(name)
        if self.apart < 0:
            return self.recv_sems.at[self.i * TOGETHER + min(k, TOGETHER - 1)]
        return self.recv_sems.at[self.i * TOGETHER + self.apart * (len(NAMES) - TOGETHER) + k]

    def finish(self):
        view = self.held.at[pl.ds(0, 3)]
        pltpu.make_async_copy(view, view, self.semaphore(NAMES[-1])).wait()

    def arrived(self, *groups):
        for name in groups:
            quarters = GROUPS[name]
            view = self.held.at[pl.ds(0, quarters // 4)] if quarters >= 4 else self.held.at[0, 0]
            pltpu.make_async_copy(view, view, self.semaphore(name)).wait()

    def drain(self):
        view = self.held.at[pl.ds(0, 15)]
        pltpu.make_async_copy(view, view, self.send_sem).wait()


class TokenGather:
    def __init__(self, place, index, held, start, rows, send_sems, recv_sems):
        self.p, self.held, self.start, self.rows = place, held, start, rows
        self.send_sem, self.recv_sems = send_sems.at[index], recv_sems.at[index]
        self.sent = {}

    def go(self, name, sem, slot, device, start=0, rows=None):
        view = self.held.at[slot, pl.ds(self.start + start, rows or self.rows)]
        copy = pltpu.make_async_remote_copy(
            src_ref=view,
            dst_ref=view,
            send_sem=self.send_sem,
            recv_sem=self.recv_sems.at[sem],
            device_id=device,
            device_id_type=MESH,
        )
        copy.start()
        self.sent[name] = copy

    def slots_of(self, slots, sem):
        view = self.held.at[pl.ds(0, slots), pl.ds(self.start, self.rows)]
        pltpu.make_async_copy(view, view, sem).wait()

    def begin(self):
        p = self.p
        self.go("o+", 0, p.slot(), p.device(x=1))
        self.go("o-", 0, p.slot(), p.device(x=-1))
        self.go("p0", 2, p.slot(), p.device(flip=True))

    def near(self):
        p, half = self.p, self.rows // 2
        self.slots_of(2, self.recv_sems.at[0])
        self.go("f+", 1, p.slot(x=-1), p.device(x=1), 0, half)
        self.go("f-", 1, p.slot(x=1), p.device(x=-1), half, half)
        self.go("p1", 2, p.slot(x=-1), p.device(flip=True))
        self.go("p3", 2, p.slot(x=1), p.device(flip=True))

    def far(self):
        p = self.p
        self.slots_of(1, self.recv_sems.at[1])
        self.go("p2", 2, p.slot(x=2), p.device(flip=True))

    def finish(self):
        self.slots_of(4, self.recv_sems.at[2])

    def drain(self):
        self.slots_of(7, self.send_sem)


class TokenSum:
    def __init__(self, place, index, part, terms, from_core, chip, near, last, send_sems, recv_sems):
        self.p, self.part, self.rows = place, part, pl.ds(part * PART, PART)
        self.terms, self.from_core, self.chip, self.near, self.last = terms, from_core, chip, near, last
        self.send_sem, self.recv_sems = send_sems.at[index], recv_sems.at[index]
        self.sent = {}

    def go(self, name, sem, src, dst, device):
        copy = pltpu.make_async_remote_copy(
            src_ref=src,
            dst_ref=dst,
            send_sem=self.send_sem,
            recv_sem=self.recv_sems.at[sem],
            device_id=device,
            device_id_type=MESH,
        )
        copy.start()
        self.sent[name] = copy

    def half(self, h):
        return pl.ds(self.part * PART + h * HALF, HALF)

    def begin(self):
        p = self.p
        self.go("d", 0, self.terms.at[:, p.other, self.rows], self.from_core.at[:, self.rows], p.device(flip=True))

    def chip_sum(self, x):
        p = self.p
        there = wrap(p.x + x, 4)
        return self.terms[there, p.core, self.rows].astype(F32) + self.from_core[there, self.rows].astype(F32)

    def cores(self):
        p, chip = self.p, self.chip
        self.sent["d"].wait_recv()
        right, left, far = wrap(p.x + 1, 4), wrap(p.x - 1, 4), wrap(p.x + 2, 4)
        chip[far, self.rows] = self.chip_sum(2).astype(BF16)
        self.go("h+", 1, chip.at[far, self.half(0)], self.near.at[0, self.half(0)], p.device(x=1))
        self.go("h-", 1, chip.at[far, self.half(1)], self.near.at[1, self.half(1)], p.device(x=-1))
        chip[right, self.rows] = self.chip_sum(1).astype(BF16)
        self.go("e+", 2, chip.at[right, self.half(1)], self.last.at[0, self.half(1)], p.device(x=1))
        chip[left, self.rows] = self.chip_sum(-1).astype(BF16)
        self.go("e-", 2, chip.at[left, self.half(0)], self.last.at[1, self.half(0)], p.device(x=-1))

    def ring(self):
        p = self.p
        both = self.near.at[0, self.rows]
        pltpu.make_async_copy(both, both, self.recv_sems.at[1]).wait()
        for x, side in ((1, 0), (-1, 1)):
            rows = self.half(side)
            total = self.chip[wrap(p.x + x, 4), rows].astype(F32) + self.near[side, rows].astype(F32)
            self.near[side, rows] = total.astype(BF16)
            self.go("e2", 2, self.near.at[side, rows], self.last.at[side, rows], p.device(x=x))

    def finish(self, base):
        both = self.last.at[:, self.rows]
        pltpu.make_async_copy(both, both, self.recv_sems.at[2]).wait()
        total = self.chip_sum(0) + (self.last[0, self.rows].astype(F32) + self.last[1, self.rows].astype(F32))
        return (base.astype(F32) + total).astype(BF16)

    def drain(self):
        view = self.terms.at[:, 0, self.rows]
        part = self.chip.at[pl.ds(0, 3), self.rows]
        pltpu.make_async_copy(view, view, self.send_sem).wait()
        pltpu.make_async_copy(part, part, self.send_sem).wait()


class ColumnSum:
    def __init__(self, place, index, part, terms, from_core, chip, near, last, send_sems, recv_sems):
        self.p, self.start, self.rows = place, part * TALL, pl.ds(part * TALL, TALL)
        self.terms, self.from_core, self.chip, self.near, self.last = terms, from_core, chip, near, last
        self.send_sem, self.recv_sems = send_sems.at[index], recv_sems.at[index]

    def go(self, sem, src, dst, device):
        pltpu.make_async_remote_copy(
            src_ref=src,
            dst_ref=dst,
            send_sem=self.send_sem,
            recv_sem=self.recv_sems.at[sem],
            device_id=device,
            device_id_type=MESH,
        ).start()

    def arrived(self, view, sem):
        pltpu.make_async_copy(view, view, self.recv_sems.at[sem]).wait()

    def half(self, h):
        return pl.ds(self.start + h * (TALL // 2), TALL // 2)

    def chip_sum(self, there, rows):
        return self.terms[there, self.p.core, rows].astype(F32) + self.from_core[there, rows].astype(F32)

    def begin(self, k, core=None):
        there = wrap(self.p.z + k, 4)

        def send():
            terms = self.terms.at[there, self.p.other, self.rows]
            self.go(k, terms, self.from_core.at[there, self.rows], self.p.device(flip=True))

        if core is None:
            send()
        else:
            pl.when(core != self.p.core)(send)

    def away(self, k, core):
        there = wrap(self.p.z + k, 4)
        away = wrap(there - self.p.x, 4)
        return there, away if core is None else jnp.where(core == self.p.core, away, 4)

    def cores(self, k, core=None):
        p, chip = self.p, self.chip
        there, away = self.away(k, core)
        arrived = functools.partial(self.arrived, self.from_core.at[0, self.rows], k)
        if core is None:
            arrived()
        else:
            pl.when(core == p.core)(arrived)

        def add(rows):
            chip[there, rows] = self.chip_sum(there, rows).astype(BF16)

        @pl.when(away == 2)
        def _():
            add(self.rows)
            self.go(4, chip.at[there, self.half(0)], self.near.at[0, self.half(0)], p.device(x=1))
            self.go(5, chip.at[there, self.half(1)], self.near.at[1, self.half(1)], p.device(x=-1))

        for distance, x, side in ((1, 1, 0), (3, -1, 1)):

            @pl.when(away == distance)
            def _(x=x, side=side):
                rows = self.half(1 - side)
                add(rows)
                self.go(6, chip.at[there, rows], self.last.at[side, rows], p.device(x=x))
                add(self.half(side))

    def ring(self, k, core=None):
        p = self.p
        there, away = self.away(k, core)
        for distance, x, side in ((1, 1, 0), (3, -1, 1)):

            @pl.when(away == distance)
            def _(x=x, side=side):
                rows = self.half(side)
                view = self.near.at[side, rows]
                self.arrived(view, 4 + side)
                total = self.chip[there, rows].astype(F32) + self.near[side, rows].astype(F32)
                self.near[side, rows] = total.astype(BF16)
                self.go(6, view, self.last.at[side, rows], p.device(x=x))

    def finish(self, base):
        self.arrived(self.last.at[:, self.rows], 6)
        total = self.chip_sum(self.p.x, self.rows)
        total = total + (self.last[0, self.rows].astype(F32) + self.last[1, self.rows].astype(F32))
        return (base.astype(F32) + total).astype(BF16)

    def drain(self):
        view = self.chip.at[:, self.rows]
        part = self.chip.at[pl.ds(0, 3), self.rows]
        pltpu.make_async_copy(view, view, self.send_sem).wait()
        pltpu.make_async_copy(part, part, self.send_sem).wait()


def norm_rows(held, rows, gain_ref, normed):
    total = jnp.zeros((PART, 1), F32)
    for k in range(GROUP):
        piece = held[k, rows].astype(F32)
        total = total + jnp.sum(piece * piece, axis=-1, keepdims=True)
    inverse = lax.rsqrt(total * (1.0 / (GROUP * WIDTH)) + EPSILON)
    for k in range(GROUP):
        columns = slice(k * WIDTH, (k + 1) * WIDTH)
        piece = held[k, rows].astype(F32) * inverse * gain_ref[:, columns]
        normed[rows, columns] = piece.astype(BF16)


def block_diagonal(matrix_ref, out_ref, offset):
    blocks, size, _ = matrix_ref.shape
    row = lax.broadcasted_iota(jnp.int32, (size, blocks * size), 0)
    column = lax.broadcasted_iota(jnp.int32, (size, blocks * size), 1)
    for b in range(blocks):
        select = (column == row + b * size).astype(F32).astype(BF16)
        spread = jnp.dot(matrix_ref[b], select, preferred_element_type=F32)
        out_ref[b * size : (b + 1) * size, offset : offset + blocks * size] = spread.astype(BF16)


def shifted(values, by, row, fill):
    return jnp.where(row >= by, pltpu.roll(values, by, 0), fill)


def mixer_rows(values, offsets, taps, maps, rate):
    channels = values.shape[1]
    row = lax.broadcasted_iota(jnp.int32, values.shape, 0)
    wide = values.astype(F32)
    reach = taps.shape[0]
    total = taps[0:1] * shifted(wide, reach - 1, row, 0.0)
    for k in range(1, reach):
        by = reach - 1 - k
        total = total + taps[k : k + 1] * (shifted(wide, by, row, 0.0) if by else wide)
    conved = total.astype(BF16)
    both = jax.nn.sigmoid(jnp.dot(conved, maps, preferred_element_type=F32))
    decay = rate * both[:, :channels] + offsets
    factor = jnp.exp(decay)
    twice = 2.0 * decay
    small = -twice * (1.0 + twice * (0.5 + twice * (1.0 / 6.0 + twice * (1.0 / 24.0))))
    lost = jnp.where(twice > -0.03, small, 1.0 - factor * factor)
    state = jnp.sqrt(lost) * both[:, channels:] * conved.astype(F32)
    by = 1
    while by < SEQ_LEN:
        state = factor * shifted(state, by, row, 0.0) + state
        if 2 * by < SEQ_LEN:
            factor = factor * shifted(factor, by, row, 1.0)
        by *= 2
    return state


def gated(state, gates):
    gate = gates.astype(F32)
    gelu = 0.5 * gate * (1.0 + lax.erf(gate * (0.5**0.5)))
    return (state * gelu).astype(BF16)


ORDER = (
    "0S 1S 2S GS", "X 0a 1a 0b", "1b 2a 2b GA0", "0e 0f GB0 GA1", "1e 1f 0g 2e", "1g 1h 2f 0h",
    "0i GF0 0j N1", "GB1 1j 1i 2h", "3S N0 2g GF1", "2i N2 2j N3", "0F 4S 1F 5S", "I1 I0 M0 M3",
    "3a 2F P0 P3", "M2 3b M1 6S", "4a P2 K0 P1", "K2 K1 K3 5a", "3e 4b 5b 6a", "R0 R1 R2 7S",
    "3h R3 8S L0", "5f 5g L1 5e", "5h 4f L3 4h", "6b 3f L2 4g", "4e 3i 5j 7a", "A0 7b 3g A1",
    "5i 3j 4j A3", "A2 4i 8a B0", "B1 6g Q0 7e", "Q1 3F 5F B3", "6f 8b 7g B2", "6e 4F U0 8e",
    "7h Q2 Q3 6h", "8h 8g 7f U1", "8f V0 8i 6i", "6j 7i V1 V2", "7j k01 8j V3", "k00 k10 k11 k21",
    "V4 k30 k20 r10", "k40 k41 k31 r21", "r00 r30 r01 r20", "r11 r40 r31 r41", "l0 l1",
)


def kernel(
    stream_ref, gain1_hbm, gain2_hbm, input_ref, gate_ref, taps_hbm, decay_hbm, inmap_hbm, param_hbm, offset_hbm,
    output_ref, up_ref, down_ref,
    out_ref,
    w_input, w_gate, w_output, w_up0, w_up1, w_up2, w_down0, w_down1, w_down2,
    held1, held2, normed, values, gates, offsets, state, activity, maps,
    terms1, core1, chip1, near1, last1, terms2, core2, chip2, near2, last2,
    gain1, gain2, taps_ref, decay_ref, inmap_ref, param_ref, rate_ref,
    local_sem, wsend, wrecv, tsend, trecv, csend, crecv,
):
    w_up, w_down = (w_up0, w_up1, w_up2), (w_down0, w_down1, w_down2)
    p = Place()
    barrier = pltpu.get_barrier_semaphore()
    greeted = [dict(x=1), dict(x=-1), dict(y=1), dict(y=-1), dict(z=1), dict(z=-1), dict(flip=True)]
    for where in greeted:
        pl.semaphore_signal(barrier, inc=1, device_id=p.device(**where), device_id_type=MESH)
    blocks = range(len(w_up))
    weights = [
        WeightGather(p, i, own, held, local_sem, wsend, wrecv, i - 3 - len(blocks))
        for i, (own, held) in enumerate(
            (
                (input_ref, w_input),
                (gate_ref, w_gate),
                (output_ref, w_output),
                *((up_ref.at[:, :, :, n * WIDTH : (n + 1) * WIDTH], w_up[n]) for n in blocks),
                *((down_ref.at[n], w_down[n]) for n in blocks),
            )
        )
    ]
    own_stream = pltpu.make_async_copy(stream_ref, held1.at[p.tp], local_sem.at[9])
    small = [
        pltpu.make_async_copy(source, target, local_sem.at[10 + k])
        for k, (source, target) in enumerate(
            (
                (decay_hbm, decay_ref),
                (inmap_hbm, inmap_ref),
                (param_hbm, param_ref),
                (gain1_hbm, gain1),
                (gain2_hbm, gain2),
                (taps_hbm, taps_ref),
                (offset_hbm, offsets),
            )
        )
    ]
    for copy in (weights[0].local, own_stream, *(w.local for w in weights[1:]), *small):
        copy.start()
    pl.semaphore_wait(barrier, len(greeted))

    gather1 = [TokenGather(p, c, held1, c * TALL, TALL, tsend, trecv) for c in range(2)]
    gather2 = [TokenGather(p, 2 + c, held2, c * PART, PART, tsend, trecv) for c in range(PARTS)]
    sum1 = [
        TokenSum(p, 2 + PARTS + c, c, terms1, core1, chip1, near1, last1, tsend, trecv) for c in range(PARTS)
    ]
    sum2 = [ColumnSum(p, c, c, terms2, core2, chip2, near2, last2, csend, crecv) for c in range(2)]
    def rows_of(c):
        return pl.ds(c * PART, PART)

    def prepare():
        for copy in small:
            copy.wait()
        block_diagonal(decay_ref, maps, 0)
        block_diagonal(inmap_ref, maps, WIDTH)
        parameter = -param_ref[...]
        softplus = jnp.maximum(parameter, 0.0) + jnp.log1p(jnp.exp(-jnp.abs(parameter)))
        rate_ref[...] = -DECAY_MULTIPLIER * softplus

    def begin():
        own_stream.wait()
        for gather in gather1:
            gather.begin()

    def columns_of(held, j, depth):
        pair = held[2 * j : 2 * j + 2].reshape(2, depth, 128)
        return jnp.concatenate([pair[0], pair[1]], axis=1)

    def inward(m):
        rows = pl.ds(m * TALL, TALL)
        columns = normed[rows, :]
        for held, target in ((w_input, values), (w_gate, gates)):
            full = held[...].reshape(GROUP * WIDTH, WIDTH)
            target[rows, :] = jnp.dot(columns, full, preferred_element_type=F32).astype(BF16)

    def mix(c):
        rows = rows_of(c)
        taps = taps_ref[...].astype(F32)
        state[rows, :] = mixer_rows(values[rows, :], offsets[rows, :], taps, maps[...], rate_ref[...])

    def project(c):
        rows = rows_of(c)
        mixed = gated(state[rows, :], gates[rows, :])
        for j in range(GROUP):
            product = jnp.dot(mixed, columns_of(w_output, j, WIDTH), preferred_element_type=F32)
            terms1[j // 2, j % 2, rows] = product.astype(BF16)
        sum1[c].begin()

    def last_core(turn):
        near = p.y // 2
        return {3: near, 4: 1 - near}.get(turn)

    def lower(turn):
        z, core = TURNS[turn], last_core(turn)
        there = wrap(p.z + z, 4)
        for w in weights[-len(blocks) :]:
            w.arrived(*(() if turn == 0 else (NAMES[turn - 5],)))
        for c in range(2):
            rows = pl.ds(c * TALL, TALL)
            for k in (0, 1) if core is None else (core,):
                product = 0.0
                for n in blocks:
                    pair = w_down[n][pl.ds(there * 4 + 2 * k, 2)].reshape(2, WIDTH, 128)
                    columns = jnp.concatenate([pair[0], pair[1]], axis=1)
                    some = activity[rows, n * WIDTH : (n + 1) * WIDTH]
                    product = product + jnp.dot(some, columns, preferred_element_type=F32)
                terms2[there, k, rows] = product.astype(BF16)
            sum2[c].begin(z % 4, core)

    def middle_of(c):
        rows = rows_of(c)
        held2[p.tp, rows] = sum1[c].finish(held1[p.tp, rows])
        gather2[c].begin()

    def raise_rows(c):
        gather2[c].finish()
        norm_rows(held2, rows_of(c), gain2, normed)

    def lift(c):
        rows = pl.ds(c * TALL, TALL)
        columns = normed[rows, :]
        for n in blocks:
            full = w_up[n][...].reshape(GROUP * WIDTH, WIDTH)
            raised = jnp.maximum(jnp.dot(columns, full, preferred_element_type=F32), 0.0)
            activity[rows, n * WIDTH : (n + 1) * WIDTH] = (raised * raised).astype(BF16)

    def last_of(c):
        rows = pl.ds(c * TALL, TALL)
        out_ref[rows, :] = sum2[c].finish(held2[p.tp, rows])

    actions = {
        "X": prepare,
        "GS": begin,
    }
    for i, w in enumerate(weights):
        for name in STEPS:
            actions[f"{i}{name}"] = functools.partial(w.step, name)
        if i < 3 + len(blocks):
            actions[f"{i}F"] = w.finish
    for c in range(PARTS):
        actions[f"N{c}"] = functools.partial(norm_rows, held1, rows_of(c), gain1, normed)
        actions[f"M{c}"] = functools.partial(mix, c)
        actions[f"P{c}"] = functools.partial(project, c)
        actions[f"K{c}"] = sum1[c].cores
        actions[f"L{c}"] = functools.partial(middle_of, c)
        actions[f"B{c}"] = gather2[c].far
        actions[f"Q{c}"] = functools.partial(raise_rows, c)
        actions[f"R{c}"] = sum1[c].ring
        actions[f"A{c}"] = gather2[c].near
    for turn, z in enumerate(TURNS):
        actions[f"V{turn}"] = functools.partial(lower, turn)
        for c in range(2):
            actions[f"k{turn}{c}"] = functools.partial(sum2[c].cores, z % 4, last_core(turn))
            actions[f"r{turn}{c}"] = functools.partial(sum2[c].ring, z % 4, last_core(turn))
    for c in range(2):
        actions[f"GA{c}"] = gather1[c].near
        actions[f"GB{c}"] = gather1[c].far
        actions[f"GF{c}"] = gather1[c].finish
        actions[f"I{c}"] = functools.partial(inward, c)
        actions[f"U{c}"] = functools.partial(lift, c)
        actions[f"l{c}"] = functools.partial(last_of, c)
    order = " ".join(ORDER).split()
    assert sorted(order) == sorted(actions)
    for name in order:
        actions[name]()

    for w in weights:
        w.drain()
    for event in (*gather1, *gather2, *sum1, *sum2):
        event.drain()


def quarters(weight):
    rows, columns = weight.shape
    return weight.reshape(2, 2, rows // 4, columns)


def shards(
    stream,
    recurrent_norm_gain,
    feedforward_norm_gain,
    recurrent_input_weight,
    output_gate_weight,
    causal_filter_weight,
    decay_gate_matrix,
    input_gate_matrix,
    channel_decay_param,
    token_decay_offset,
    recurrent_output_weight,
    up_projection_weight,
    down_projection_weight,
):
    mixer = [quarters(w) for w in (recurrent_input_weight, output_gate_weight, recurrent_output_weight)]
    up, hidden = quarters(up_projection_weight), up_projection_weight.shape[1]
    blocks = hidden // WIDTH
    down = down_projection_weight.reshape(blocks, 2, 2, WIDTH // 4, -1)
    arguments = (
        stream,
        recurrent_norm_gain.reshape(1, -1),
        feedforward_norm_gain.reshape(1, -1),
        mixer[0],
        mixer[1],
        causal_filter_weight,
        decay_gate_matrix,
        input_gate_matrix,
        channel_decay_param.reshape(1, -1),
        token_decay_offset,
        mixer[2],
        up,
        down,
    )
    far = pl.BlockSpec(memory_space=pltpu.HBM)
    sums = [
        pltpu.VMEM((4, 2, ROWS, WIDTH), BF16),
        pltpu.VMEM((4, ROWS, WIDTH), BF16),
        pltpu.VMEM((4, ROWS, WIDTH), BF16),
        pltpu.VMEM((2, ROWS, WIDTH), BF16),
        pltpu.VMEM((2, ROWS, WIDTH), BF16),
    ]
    events = 2 + 2 * PARTS
    return pl.pallas_call(
        kernel,
        out_shape=jax.ShapeDtypeStruct(stream.shape, stream.dtype),
        in_specs=[far] * 13,
        out_specs=pl.BlockSpec(memory_space=pltpu.VMEM),
        scratch_shapes=[
            *[pltpu.VMEM((16, *w.shape), BF16) for w in mixer],
            *[pltpu.VMEM((16, *up.shape[:-1], WIDTH), BF16)] * blocks,
            *[pltpu.VMEM((16, *down.shape[1:]), BF16)] * blocks,
            pltpu.VMEM((GROUP, ROWS, WIDTH), BF16),
            pltpu.VMEM((GROUP, ROWS, WIDTH), BF16),
            pltpu.VMEM((ROWS, GROUP * WIDTH), BF16),
            pltpu.VMEM((ROWS, WIDTH), BF16),
            pltpu.VMEM((ROWS, WIDTH), BF16),
            pltpu.VMEM((ROWS, WIDTH), F32),
            pltpu.VMEM((ROWS, WIDTH), F32),
            pltpu.VMEM((ROWS, hidden), BF16),
            pltpu.VMEM((WIDTH, 2 * WIDTH), BF16),
            *sums,
            *sums,
            pltpu.VMEM((1, GROUP * WIDTH), F32),
            pltpu.VMEM((1, GROUP * WIDTH), F32),
            pltpu.VMEM(causal_filter_weight.shape, BF16),
            pltpu.VMEM(decay_gate_matrix.shape, BF16),
            pltpu.VMEM(input_gate_matrix.shape, BF16),
            pltpu.VMEM((1, WIDTH), F32),
            pltpu.VMEM((1, WIDTH), F32),
            pltpu.SemaphoreType.DMA((17,)),
            pltpu.SemaphoreType.DMA((3 + 2 * blocks,)),
            pltpu.SemaphoreType.DMA(((3 + 2 * blocks) * TOGETHER + blocks * (len(NAMES) - TOGETHER),)),
            pltpu.SemaphoreType.DMA((events,)),
            pltpu.SemaphoreType.DMA((events, 3)),
            pltpu.SemaphoreType.DMA((2,)),
            pltpu.SemaphoreType.DMA((2, 7)),
        ],
        compiler_params=pltpu.CompilerParams(
            collective_id=0, has_side_effects=True, vmem_limit_bytes=VMEM_LIMIT
        ),
    )(*(pltpu.with_memory_space_constraint(value, pltpu.HBM) for value in arguments))


def solution(mesh):
    split = Mesh(
        mesh.devices.reshape(mesh.shape["rep"], 4, 4, mesh.shape["tp"]),
        AXES,
    )
    placed = (
        P(REP_FS, "tp"),
        P(),
        P(),
        P(FS, "tp"),
        P(FS, "tp"),
        P(None, "tp"),
        P("tp", None, None),
        P("tp", None, None),
        P("tp"),
        P(REP_FS, "tp"),
        P("tp", FS),
        P(FS, "tp"),
        P("tp", FS),
    )
    return jax.shard_map(
        shards, mesh=split, in_specs=placed, out_specs=P(REP_FS, "tp"), check_vma=False
    )
```

```python
import functools

import jax
import jax.numpy as jnp
from jax import lax
from jax.experimental import pallas as pl
from jax.experimental.pallas import tpu as pltpu
from jax.sharding import Mesh
from jax.sharding import PartitionSpec as P

MESH = pl.DeviceIdType.MESH
SEQ_LEN = 128
FS = ("fs_0", "fs_1")
REP_FS = ("rep", "fs_0", "fs_1")
AXES = ("rep", "fs_0", "fs_1", "tp")

EPSILON = 1e-06
DECAY_MULTIPLIER = 8.0
F32 = jnp.float32
BF16 = jnp.bfloat16

ROWS, WIDTH, PARTS, GROUP = 512, 256, 4, 8
PART = ROWS // PARTS
HALF = PART // 2
TALL = ROWS // 2
VMEM_LIMIT = 40 * 1024 * 1024
TURNS = (0, -1, 1, 2, 2)

EVERY = slice(None)
STEPS = {
    "S": ((), (("oy+", 0, 0, ()), ("oy-", 0, 0, ()), ("oz+", 0, 0, ()), ("oz-", 0, 0, ()))),
    "a": (
        ("own",),
        (
            ("ry+", 0, -1, (EVERY, 0)), ("ry-", 0, 1, (EVERY, 1)),
            ("a1z+", 0, -1, (0,)), ("a1z-", 0, -1, (0,)), ("b1y+", -1, 0, (1,)), ("b1y-", -1, 0, (1,)),
            ("a3z+", 0, 1, (0,)), ("a3z-", 0, 1, (0,)), ("b3y+", 1, 0, (1,)), ("b3y-", 1, 0, (1,)),
        ),
    ),
    "b": ((), (("rz+", -1, 0, (EVERY, 0)), ("rz-", 1, 0, (EVERY, 1)))),
    "e": (("ry",), (("a2z+", 0, 2, (0,)), ("a2z-", 0, 2, (0,)))),
    "f": (("rz",), (("b2y+", 2, 0, (1,)), ("b2y-", 2, 0, (1,)))),
    "g": (
        ("by",),
        (("g1y+", -1, -1, (1, 0)), ("g1y-", -1, 1, (1, 1)), ("g3y+", 1, -1, (1, 0)), ("g3y-", 1, 1, (1, 1))),
    ),
    "h": (
        ("az",),
        (("f1z+", -1, -1, (0, 0)), ("f1z-", 1, -1, (0, 1)), ("f3z+", -1, 1, (0, 0)), ("f3z-", 1, 1, (0, 1))),
    ),
    "i": (("a2",), (("f2z+", -1, 2, (0, 0)), ("f2z-", 1, 2, (0, 1)))),
    "j": (("b2",), (("g2y+", 2, -1, (1, 0)), ("g2y-", 2, 1, (1, 1)))),
}
GROUPS = {
    "own": 16, "ry": 4, "rz": 4, "by": 8, "az": 8, "a2": 4, "b2": 4, "below": 2, "above": 2, "beside": 4, "opposite": 4,
}
NAMES = list(GROUPS)
TOGETHER = len(NAMES) - 3


def group_of(name):
    way, step, link = name[0], name[1], name[-2]
    if way in "or":
        return {"o": "own", "r": "r" + link}[way]
    if way in "ab":
        return way + ("2" if step == "2" else link)
    if step == "2":
        return "opposite"
    return "beside" if way == "f" else {"1": "below", "3": "above"}[step]


def wrap(value, n):
    return lax.rem(value + n, n)


class Place:
    def __init__(self):
        self.rep, self.z, self.y, self.tp = (lax.axis_index(a) for a in AXES)
        self.whole_z = self.rep * 4 + self.z
        self.x, self.core = self.tp // 2, lax.rem(self.tp, 2)
        self.other = 1 - self.core

    def device(self, x=0, y=0, z=0, flip=False):
        z_there = wrap(self.whole_z + z, 8)
        core = self.other if flip else self.core
        return (z_there // 4, lax.rem(z_there, 4), wrap(self.y + y, 4), wrap(self.x + x, 4) * 2 + core)

    def shard(self, z=0, y=0):
        return wrap(self.z + z, 4) * 4 + wrap(self.y + y, 4)

    def slot(self, x=0, flip=False):
        return wrap(self.x + x, 4) * 2 + (self.other if flip else self.core)


class WeightGather:
    def __init__(self, place, index, own_ref, held, local_sem, send_sem, recv_sems, apart):
        self.p, self.i, self.own, self.held = place, index, own_ref, held
        self.local = pltpu.make_async_copy(own_ref, held.at[place.shard()], local_sem.at[index])
        self.send_sem, self.recv_sems, self.apart = send_sem.at[index], recv_sems, apart

    def go(self, kind, z, y, part):
        where = {"y+": dict(y=1), "y-": dict(y=-1), "z+": dict(z=1), "z-": dict(z=-1)}[kind[-2:]]
        view = self.held.at[(self.p.shard(z, y), *part)]
        copy = pltpu.make_async_remote_copy(
            src_ref=view,
            dst_ref=view,
            send_sem=self.send_sem,
            recv_sem=self.semaphore(group_of(kind)),
            device_id=self.p.device(**where),
            device_id_type=MESH,
        )
        copy.start()

    def step(self, name):
        if name == "S":
            self.local.wait()
        waits, sends = STEPS[name]
        self.arrived(*waits)
        for message in sends:
            self.go(*message)

    def semaphore(self, name):
        k = NAMES.index(name)
        if self.apart < 0:
            return self.recv_sems.at[self.i * TOGETHER + min(k, TOGETHER - 1)]
        return self.recv_sems.at[self.i * TOGETHER + self.apart * (len(NAMES) - TOGETHER) + k]

    def finish(self):
        view = self.held.at[pl.ds(0, 3)]
        pltpu.make_async_copy(view, view, self.semaphore(NAMES[-1])).wait()

    def arrived(self, *groups):
        for name in groups:
            quarters = GROUPS[name]
            view = self.held.at[pl.ds(0, quarters // 4)] if quarters >= 4 else self.held.at[0, 0]
            pltpu.make_async_copy(view, view, self.semaphore(name)).wait()

    def drain(self):
        view = self.held.at[pl.ds(0, 15)]
        pltpu.make_async_copy(view, view, self.send_sem).wait()


class TokenGather:
    def __init__(self, place, index, held, start, rows, send_sems, recv_sems):
        self.p, self.held, self.start, self.rows = place, held, start, rows
        self.send_sem, self.recv_sems = send_sems.at[index], recv_sems.at[index]
        self.sent = {}

    def go(self, name, sem, slot, device, start=0, rows=None):
        view = self.held.at[slot, pl.ds(self.start + start, rows or self.rows)]
        copy = pltpu.make_async_remote_copy(
            src_ref=view,
            dst_ref=view,
            send_sem=self.send_sem,
            recv_sem=self.recv_sems.at[sem],
            device_id=device,
            device_id_type=MESH,
        )
        copy.start()
        self.sent[name] = copy

    def slots_of(self, slots, sem):
        view = self.held.at[pl.ds(0, slots), pl.ds(self.start, self.rows)]
        pltpu.make_async_copy(view, view, sem).wait()

    def begin(self):
        p = self.p
        self.go("o+", 0, p.slot(), p.device(x=1))
        self.go("o-", 0, p.slot(), p.device(x=-1))
        self.go("p0", 2, p.slot(), p.device(flip=True))

    def near(self):
        p, half = self.p, self.rows // 2
        self.slots_of(2, self.recv_sems.at[0])
        self.go("f+", 1, p.slot(x=-1), p.device(x=1), 0, half)
        self.go("f-", 1, p.slot(x=1), p.device(x=-1), half, half)
        self.go("p1", 2, p.slot(x=-1), p.device(flip=True))
        self.go("p3", 2, p.slot(x=1), p.device(flip=True))

    def far(self):
        p = self.p
        self.slots_of(1, self.recv_sems.at[1])
        self.go("p2", 2, p.slot(x=2), p.device(flip=True))

    def finish(self):
        self.slots_of(4, self.recv_sems.at[2])

    def drain(self):
        self.slots_of(7, self.send_sem)


class TokenSum:
    def __init__(self, place, index, part, terms, from_core, chip, near, last, send_sems, recv_sems):
        self.p, self.part, self.rows = place, part, pl.ds(part * PART, PART)
        self.terms, self.from_core, self.chip, self.near, self.last = terms, from_core, chip, near, last
        self.send_sem, self.recv_sems = send_sems.at[index], recv_sems.at[index]
        self.sent = {}

    def go(self, name, sem, src, dst, device):
        copy = pltpu.make_async_remote_copy(
            src_ref=src,
            dst_ref=dst,
            send_sem=self.send_sem,
            recv_sem=self.recv_sems.at[sem],
            device_id=device,
            device_id_type=MESH,
        )
        copy.start()
        self.sent[name] = copy

    def half(self, h):
        return pl.ds(self.part * PART + h * HALF, HALF)

    def begin(self):
        p = self.p
        self.go("d", 0, self.terms.at[:, p.other, self.rows], self.from_core.at[:, self.rows], p.device(flip=True))

    def chip_sum(self, x):
        p = self.p
        there = wrap(p.x + x, 4)
        return self.terms[there, p.core, self.rows].astype(F32) + self.from_core[there, self.rows].astype(F32)

    def cores(self):
        p, chip = self.p, self.chip
        self.sent["d"].wait_recv()
        right, left, far = wrap(p.x + 1, 4), wrap(p.x - 1, 4), wrap(p.x + 2, 4)
        chip[far, self.rows] = self.chip_sum(2).astype(BF16)
        self.go("h+", 1, chip.at[far, self.half(0)], self.near.at[0, self.half(0)], p.device(x=1))
        self.go("h-", 1, chip.at[far, self.half(1)], self.near.at[1, self.half(1)], p.device(x=-1))
        chip[right, self.rows] = self.chip_sum(1).astype(BF16)
        self.go("e+", 2, chip.at[right, self.half(1)], self.last.at[0, self.half(1)], p.device(x=1))
        chip[left, self.rows] = self.chip_sum(-1).astype(BF16)
        self.go("e-", 2, chip.at[left, self.half(0)], self.last.at[1, self.half(0)], p.device(x=-1))

    def ring(self):
        p = self.p
        both = self.near.at[0, self.rows]
        pltpu.make_async_copy(both, both, self.recv_sems.at[1]).wait()
        for x, side in ((1, 0), (-1, 1)):
            rows = self.half(side)
            total = self.chip[wrap(p.x + x, 4), rows].astype(F32) + self.near[side, rows].astype(F32)
            self.near[side, rows] = total.astype(BF16)
            self.go("e2", 2, self.near.at[side, rows], self.last.at[side, rows], p.device(x=x))

    def finish(self, base):
        both = self.last.at[:, self.rows]
        pltpu.make_async_copy(both, both, self.recv_sems.at[2]).wait()
        total = self.chip_sum(0) + (self.last[0, self.rows].astype(F32) + self.last[1, self.rows].astype(F32))
        return (base.astype(F32) + total).astype(BF16)

    def drain(self):
        view = self.terms.at[:, 0, self.rows]
        part = self.chip.at[pl.ds(0, 3), self.rows]
        pltpu.make_async_copy(view, view, self.send_sem).wait()
        pltpu.make_async_copy(part, part, self.send_sem).wait()


class ColumnSum:
    def __init__(self, place, index, part, terms, from_core, chip, near, last, send_sems, recv_sems):
        self.p, self.start, self.rows = place, part * TALL, pl.ds(part * TALL, TALL)
        self.terms, self.from_core, self.chip, self.near, self.last = terms, from_core, chip, near, last
        self.send_sem, self.recv_sems = send_sems.at[index], recv_sems.at[index]

    def go(self, sem, src, dst, device):
        pltpu.make_async_remote_copy(
            src_ref=src,
            dst_ref=dst,
            send_sem=self.send_sem,
            recv_sem=self.recv_sems.at[sem],
            device_id=device,
            device_id_type=MESH,
        ).start()

    def arrived(self, view, sem):
        pltpu.make_async_copy(view, view, self.recv_sems.at[sem]).wait()

    def half(self, h):
        return pl.ds(self.start + h * (TALL // 2), TALL // 2)

    def chip_sum(self, there, rows):
        return self.terms[there, self.p.core, rows].astype(F32) + self.from_core[there, rows].astype(F32)

    def begin(self, k, core=None):
        there = wrap(self.p.z + k, 4)

        def send():
            terms = self.terms.at[there, self.p.other, self.rows]
            self.go(k, terms, self.from_core.at[there, self.rows], self.p.device(flip=True))

        if core is None:
            send()
        else:
            pl.when(core != self.p.core)(send)

    def away(self, k, core):
        there = wrap(self.p.z + k, 4)
        away = wrap(there - self.p.x, 4)
        return there, away if core is None else jnp.where(core == self.p.core, away, 4)

    def cores(self, k, core=None):
        p, chip = self.p, self.chip
        there, away = self.away(k, core)
        arrived = functools.partial(self.arrived, self.from_core.at[0, self.rows], k)
        if core is None:
            arrived()
        else:
            pl.when(core == p.core)(arrived)

        def add(rows):
            chip[there, rows] = self.chip_sum(there, rows).astype(BF16)

        @pl.when(away == 2)
        def _():
            add(self.rows)
            self.go(4, chip.at[there, self.half(0)], self.near.at[0, self.half(0)], p.device(x=1))
            self.go(5, chip.at[there, self.half(1)], self.near.at[1, self.half(1)], p.device(x=-1))

        for distance, x, side in ((1, 1, 0), (3, -1, 1)):

            @pl.when(away == distance)
            def _(x=x, side=side):
                rows = self.half(1 - side)
                add(rows)
                self.go(6, chip.at[there, rows], self.last.at[side, rows], p.device(x=x))
                add(self.half(side))

    def ring(self, k, core=None):
        p = self.p
        there, away = self.away(k, core)
        for distance, x, side in ((1, 1, 0), (3, -1, 1)):

            @pl.when(away == distance)
            def _(x=x, side=side):
                rows = self.half(side)
                view = self.near.at[side, rows]
                self.arrived(view, 4 + side)
                total = self.chip[there, rows].astype(F32) + self.near[side, rows].astype(F32)
                self.near[side, rows] = total.astype(BF16)
                self.go(6, view, self.last.at[side, rows], p.device(x=x))

    def finish(self, base):
        self.arrived(self.last.at[:, self.rows], 6)
        total = self.chip_sum(self.p.x, self.rows)
        total = total + (self.last[0, self.rows].astype(F32) + self.last[1, self.rows].astype(F32))
        return (base.astype(F32) + total).astype(BF16)

    def drain(self):
        view = self.chip.at[:, self.rows]
        part = self.chip.at[pl.ds(0, 3), self.rows]
        pltpu.make_async_copy(view, view, self.send_sem).wait()
        pltpu.make_async_copy(part, part, self.send_sem).wait()


def norm_rows(held, rows, gain_ref, normed):
    total = jnp.zeros((PART, 1), F32)
    for k in range(GROUP):
        piece = held[k, rows].astype(F32)
        total = total + jnp.sum(piece * piece, axis=-1, keepdims=True)
    inverse = lax.rsqrt(total * (1.0 / (GROUP * WIDTH)) + EPSILON)
    for k in range(GROUP):
        columns = slice(k * WIDTH, (k + 1) * WIDTH)
        piece = held[k, rows].astype(F32) * inverse * gain_ref[:, columns]
        normed[rows, columns] = piece.astype(BF16)


def block_diagonal(matrix_ref, out_ref, offset):
    blocks, size, _ = matrix_ref.shape
    row = lax.broadcasted_iota(jnp.int32, (size, blocks * size), 0)
    column = lax.broadcasted_iota(jnp.int32, (size, blocks * size), 1)
    for b in range(blocks):
        select = (column == row + b * size).astype(F32).astype(BF16)
        spread = jnp.dot(matrix_ref[b], select, preferred_element_type=F32)
        out_ref[b * size : (b + 1) * size, offset : offset + blocks * size] = spread.astype(BF16)


def shifted(values, by, row, fill):
    return jnp.where(row >= by, pltpu.roll(values, by, 0), fill)


def mixer_rows(values, offsets, taps, maps, rate):
    channels = values.shape[1]
    row = lax.broadcasted_iota(jnp.int32, values.shape, 0)
    wide = values.astype(F32)
    reach = taps.shape[0]
    total = taps[0:1] * shifted(wide, reach - 1, row, 0.0)
    for k in range(1, reach):
        by = reach - 1 - k
        total = total + taps[k : k + 1] * (shifted(wide, by, row, 0.0) if by else wide)
    conved = total.astype(BF16)
    both = jax.nn.sigmoid(jnp.dot(conved, maps, preferred_element_type=F32))
    decay = rate * both[:, :channels] + offsets
    factor = jnp.exp(decay)
    twice = 2.0 * decay
    small = -twice * (1.0 + twice * (0.5 + twice * (1.0 / 6.0 + twice * (1.0 / 24.0))))
    lost = jnp.where(twice > -0.03, small, 1.0 - factor * factor)
    state = jnp.sqrt(lost) * both[:, channels:] * conved.astype(F32)
    by = 1
    while by < SEQ_LEN:
        state = factor * shifted(state, by, row, 0.0) + state
        if 2 * by < SEQ_LEN:
            factor = factor * shifted(factor, by, row, 1.0)
        by *= 2
    return state


def gated(state, gates):
    gate = gates.astype(F32)
    gelu = 0.5 * gate * (1.0 + lax.erf(gate * (0.5**0.5)))
    return (state * gelu).astype(BF16)


ORDER = (
    "0S GS 1S 2S", "0a GA0 0b 1a", "1b GA1 2a 2b", "0f X 1e 0e", "GB0 1f 0g 0h", "1h GB1 1g 2e",
    "2h 2f 2g 1j", "GF1 1i GF0 0i", "0j 3S N0 N3", "2i 2j N1 4S", "5S 7S N2 0F", "1F I1 I0 M0",
    "2F P0 M2 P2", "8S M1 P1 6S", "M3 K0 P3 3a", "K2 K1 4a 4b", "5a R0 K3 R1", "3b 3e R2 5b",
    "7a R3 L0 6a", "5e L1 4g 4f", "6b L2 7b 5f", "4e L3 8a A0", "3f 5i 6h A1", "8b 3h A2 3g",
    "5h 5j 4h 4j", "4i A3 3i 6e", "7e 7h 5g 8e", "7f 3j B1 B0", "B2 8h 6g B3", "8g 6f Q0 7g",
    "Q2 5F 8f Q1", "4F Q3 3F U0", "U1 7j 6j 6i", "V0 8i 7i V1", "8j V2 V3 k00", "k01 k10 k20 V4",
    "k11 k30 k31 k21", "k40 k41 r10 r00", "r20 r30 r11 r01", "r40 r21 r31 r41", "l0 l1",
)


def kernel(
    stream_ref, gain1_hbm, gain2_hbm, input_ref, gate_ref, taps_hbm, decay_hbm, inmap_hbm, param_hbm, offset_hbm,
    output_ref, up_ref, down_ref,
    out_ref,
    w_input, w_gate, w_output, w_up0, w_up1, w_up2, w_down0, w_down1, w_down2,
    held1, held2, normed, values, gates, offsets, state, activity, maps,
    terms1, core1, chip1, near1, last1, terms2, core2, chip2, near2, last2,
    gain1, gain2, taps_ref, decay_ref, inmap_ref, param_ref, rate_ref,
    local_sem, wsend, wrecv, tsend, trecv, csend, crecv,
):
    w_up, w_down = (w_up0, w_up1, w_up2), (w_down0, w_down1, w_down2)
    p = Place()
    barrier = pltpu.get_barrier_semaphore()
    greeted = [dict(x=1), dict(x=-1), dict(y=1), dict(y=-1), dict(z=1), dict(z=-1), dict(flip=True)]
    for where in greeted:
        pl.semaphore_signal(barrier, inc=1, device_id=p.device(**where), device_id_type=MESH)
    blocks = range(len(w_up))
    weights = [
        WeightGather(p, i, own, held, local_sem, wsend, wrecv, i - 3 - len(blocks))
        for i, (own, held) in enumerate(
            (
                (input_ref, w_input),
                (gate_ref, w_gate),
                (output_ref, w_output),
                *((up_ref.at[:, :, :, n * WIDTH : (n + 1) * WIDTH], w_up[n]) for n in blocks),
                *((down_ref.at[n], w_down[n]) for n in blocks),
            )
        )
    ]
    own_stream = pltpu.make_async_copy(stream_ref, held1.at[p.tp], local_sem.at[9])
    small = [
        pltpu.make_async_copy(source, target, local_sem.at[10 + k])
        for k, (source, target) in enumerate(
            (
                (decay_hbm, decay_ref),
                (inmap_hbm, inmap_ref),
                (param_hbm, param_ref),
                (gain1_hbm, gain1),
                (gain2_hbm, gain2),
                (taps_hbm, taps_ref),
                (offset_hbm, offsets),
            )
        )
    ]
    for copy in (weights[0].local, own_stream, *(w.local for w in weights[1:]), *small):
        copy.start()
    pl.semaphore_wait(barrier, len(greeted))

    gather1 = [TokenGather(p, c, held1, c * TALL, TALL, tsend, trecv) for c in range(2)]
    gather2 = [TokenGather(p, 2 + c, held2, c * PART, PART, tsend, trecv) for c in range(PARTS)]
    sum1 = [
        TokenSum(p, 2 + PARTS + c, c, terms1, core1, chip1, near1, last1, tsend, trecv) for c in range(PARTS)
    ]
    sum2 = [ColumnSum(p, c, c, terms2, core2, chip2, near2, last2, csend, crecv) for c in range(2)]
    def rows_of(c):
        return pl.ds(c * PART, PART)

    def prepare():
        for copy in small:
            copy.wait()
        block_diagonal(decay_ref, maps, 0)
        block_diagonal(inmap_ref, maps, WIDTH)
        parameter = -param_ref[...]
        softplus = jnp.maximum(parameter, 0.0) + jnp.log1p(jnp.exp(-jnp.abs(parameter)))
        rate_ref[...] = -DECAY_MULTIPLIER * softplus

    def begin():
        own_stream.wait()
        for gather in gather1:
            gather.begin()

    def columns_of(held, j, depth):
        pair = held[2 * j : 2 * j + 2].reshape(2, depth, 128)
        return jnp.concatenate([pair[0], pair[1]], axis=1)

    def inward(m):
        rows = pl.ds(m * TALL, TALL)
        columns = normed[rows, :]
        for held, target in ((w_input, values), (w_gate, gates)):
            full = held[...].reshape(GROUP * WIDTH, WIDTH)
            target[rows, :] = jnp.dot(columns, full, preferred_element_type=F32).astype(BF16)

    def mix(c):
        rows = rows_of(c)
        taps = taps_ref[...].astype(F32)
        state[rows, :] = mixer_rows(values[rows, :], offsets[rows, :], taps, maps[...], rate_ref[...])

    def project(c):
        rows = rows_of(c)
        mixed = gated(state[rows, :], gates[rows, :])
        for j in range(GROUP):
            product = jnp.dot(mixed, columns_of(w_output, j, WIDTH), preferred_element_type=F32)
            terms1[j // 2, j % 2, rows] = product.astype(BF16)
        sum1[c].begin()

    def last_core(turn):
        near = p.y // 2
        return {3: near, 4: 1 - near}.get(turn)

    def lower(turn):
        z, core = TURNS[turn], last_core(turn)
        there = wrap(p.z + z, 4)
        for w in weights[-len(blocks) :]:
            w.arrived(*(() if turn == 0 else (NAMES[turn - 5],)))
        for c in range(2):
            rows = pl.ds(c * TALL, TALL)
            for k in (0, 1) if core is None else (core,):
                product = 0.0
                for n in blocks:
                    pair = w_down[n][pl.ds(there * 4 + 2 * k, 2)].reshape(2, WIDTH, 128)
                    columns = jnp.concatenate([pair[0], pair[1]], axis=1)
                    some = activity[rows, n * WIDTH : (n + 1) * WIDTH]
                    product = product + jnp.dot(some, columns, preferred_element_type=F32)
                terms2[there, k, rows] = product.astype(BF16)
            sum2[c].begin(z % 4, core)

    def middle_of(c):
        rows = rows_of(c)
        held2[p.tp, rows] = sum1[c].finish(held1[p.tp, rows])
        gather2[c].begin()

    def raise_rows(c):
        gather2[c].finish()
        norm_rows(held2, rows_of(c), gain2, normed)

    def lift(c):
        rows = pl.ds(c * TALL, TALL)
        columns = normed[rows, :]
        for n in blocks:
            full = w_up[n][...].reshape(GROUP * WIDTH, WIDTH)
            raised = jnp.maximum(jnp.dot(columns, full, preferred_element_type=F32), 0.0)
            activity[rows, n * WIDTH : (n + 1) * WIDTH] = (raised * raised).astype(BF16)

    def last_of(c):
        rows = pl.ds(c * TALL, TALL)
        out_ref[rows, :] = sum2[c].finish(held2[p.tp, rows])

    actions = {
        "X": prepare,
        "GS": begin,
    }
    for i, w in enumerate(weights):
        for name in STEPS:
            actions[f"{i}{name}"] = functools.partial(w.step, name)
        if i < 3 + len(blocks):
            actions[f"{i}F"] = w.finish
    for c in range(PARTS):
        actions[f"N{c}"] = functools.partial(norm_rows, held1, rows_of(c), gain1, normed)
        actions[f"M{c}"] = functools.partial(mix, c)
        actions[f"P{c}"] = functools.partial(project, c)
        actions[f"K{c}"] = sum1[c].cores
        actions[f"L{c}"] = functools.partial(middle_of, c)
        actions[f"B{c}"] = gather2[c].far
        actions[f"Q{c}"] = functools.partial(raise_rows, c)
        actions[f"R{c}"] = sum1[c].ring
        actions[f"A{c}"] = gather2[c].near
    for turn, z in enumerate(TURNS):
        actions[f"V{turn}"] = functools.partial(lower, turn)
        for c in range(2):
            actions[f"k{turn}{c}"] = functools.partial(sum2[c].cores, z % 4, last_core(turn))
            actions[f"r{turn}{c}"] = functools.partial(sum2[c].ring, z % 4, last_core(turn))
    for c in range(2):
        actions[f"GA{c}"] = gather1[c].near
        actions[f"GB{c}"] = gather1[c].far
        actions[f"GF{c}"] = gather1[c].finish
        actions[f"I{c}"] = functools.partial(inward, c)
        actions[f"U{c}"] = functools.partial(lift, c)
        actions[f"l{c}"] = functools.partial(last_of, c)
    order = " ".join(ORDER).split()
    assert sorted(order) == sorted(actions)
    for name in order:
        actions[name]()

    for w in weights:
        w.drain()
    for event in (*gather1, *gather2, *sum1, *sum2):
        event.drain()


def quarters(weight):
    rows, columns = weight.shape
    return weight.reshape(2, 2, rows // 4, columns)


def shards(
    stream,
    recurrent_norm_gain,
    feedforward_norm_gain,
    recurrent_input_weight,
    output_gate_weight,
    causal_filter_weight,
    decay_gate_matrix,
    input_gate_matrix,
    channel_decay_param,
    token_decay_offset,
    recurrent_output_weight,
    up_projection_weight,
    down_projection_weight,
):
    mixer = [quarters(w) for w in (recurrent_input_weight, output_gate_weight, recurrent_output_weight)]
    up, hidden = quarters(up_projection_weight), up_projection_weight.shape[1]
    blocks = hidden // WIDTH
    down = down_projection_weight.reshape(blocks, 2, 2, WIDTH // 4, -1)
    arguments = (
        stream,
        recurrent_norm_gain.reshape(1, -1),
        feedforward_norm_gain.reshape(1, -1),
        mixer[0],
        mixer[1],
        causal_filter_weight,
        decay_gate_matrix,
        input_gate_matrix,
        channel_decay_param.reshape(1, -1),
        token_decay_offset,
        mixer[2],
        up,
        down,
    )
    far = pl.BlockSpec(memory_space=pltpu.HBM)
    sums = [
        pltpu.VMEM((4, 2, ROWS, WIDTH), BF16),
        pltpu.VMEM((4, ROWS, WIDTH), BF16),
        pltpu.VMEM((4, ROWS, WIDTH), BF16),
        pltpu.VMEM((2, ROWS, WIDTH), BF16),
        pltpu.VMEM((2, ROWS, WIDTH), BF16),
    ]
    events = 2 + 2 * PARTS
    return pl.pallas_call(
        kernel,
        out_shape=jax.ShapeDtypeStruct(stream.shape, stream.dtype),
        in_specs=[far] * 13,
        out_specs=pl.BlockSpec(memory_space=pltpu.VMEM),
        scratch_shapes=[
            *[pltpu.VMEM((16, *w.shape), BF16) for w in mixer],
            *[pltpu.VMEM((16, *up.shape[:-1], WIDTH), BF16)] * blocks,
            *[pltpu.VMEM((16, *down.shape[1:]), BF16)] * blocks,
            pltpu.VMEM((GROUP, ROWS, WIDTH), BF16),
            pltpu.VMEM((GROUP, ROWS, WIDTH), BF16),
            pltpu.VMEM((ROWS, GROUP * WIDTH), BF16),
            pltpu.VMEM((ROWS, WIDTH), BF16),
            pltpu.VMEM((ROWS, WIDTH), BF16),
            pltpu.VMEM((ROWS, WIDTH), F32),
            pltpu.VMEM((ROWS, WIDTH), F32),
            pltpu.VMEM((ROWS, hidden), BF16),
            pltpu.VMEM((WIDTH, 2 * WIDTH), BF16),
            *sums,
            *sums,
            pltpu.VMEM((1, GROUP * WIDTH), F32),
            pltpu.VMEM((1, GROUP * WIDTH), F32),
            pltpu.VMEM(causal_filter_weight.shape, BF16),
            pltpu.VMEM(decay_gate_matrix.shape, BF16),
            pltpu.VMEM(input_gate_matrix.shape, BF16),
            pltpu.VMEM((1, WIDTH), F32),
            pltpu.VMEM((1, WIDTH), F32),
            pltpu.SemaphoreType.DMA((17,)),
            pltpu.SemaphoreType.DMA((3 + 2 * blocks,)),
            pltpu.SemaphoreType.DMA(((3 + 2 * blocks) * TOGETHER + blocks * (len(NAMES) - TOGETHER),)),
            pltpu.SemaphoreType.DMA((events,)),
            pltpu.SemaphoreType.DMA((events, 3)),
            pltpu.SemaphoreType.DMA((2,)),
            pltpu.SemaphoreType.DMA((2, 7)),
        ],
        compiler_params=pltpu.CompilerParams(
            collective_id=0, has_side_effects=True, vmem_limit_bytes=VMEM_LIMIT
        ),
    )(*(pltpu.with_memory_space_constraint(value, pltpu.HBM) for value in arguments))


def solution(mesh):
    split = Mesh(
        mesh.devices.reshape(mesh.shape["rep"], 4, 4, mesh.shape["tp"]),
        AXES,
    )
    placed = (
        P(REP_FS, "tp"),
        P(),
        P(),
        P(FS, "tp"),
        P(FS, "tp"),
        P(None, "tp"),
        P("tp", None, None),
        P("tp", None, None),
        P("tp"),
        P(REP_FS, "tp"),
        P("tp", FS),
        P(FS, "tp"),
        P("tp", FS),
    )
    return jax.shard_map(
        shards, mesh=split, in_specs=placed, out_specs=P(REP_FS, "tp"), check_vma=False
    )
```

```python
import functools

import jax
import jax.numpy as jnp
from jax import lax
from jax.experimental import pallas as pl
from jax.experimental.pallas import tpu as pltpu
from jax.sharding import Mesh
from jax.sharding import PartitionSpec as P

MESH = pl.DeviceIdType.MESH
SEQ_LEN = 128
FS = ("fs_0", "fs_1")
REP_FS = ("rep", "fs_0", "fs_1")
AXES = ("rep", "fs_0", "fs_1", "tp")

EPSILON = 1e-06
DECAY_MULTIPLIER = 8.0
F32 = jnp.float32
BF16 = jnp.bfloat16

ROWS, WIDTH, PARTS, GROUP = 512, 256, 4, 8
PART = ROWS // PARTS
HALF = PART // 2
TALL = ROWS // 2
VMEM_LIMIT = 40 * 1024 * 1024
TURNS = (0, -1, 1, 2, 2)

EVERY = slice(None)
STEPS = {
    "S": ((), (("oy+", 0, 0, ()), ("oy-", 0, 0, ()), ("oz+", 0, 0, ()), ("oz-", 0, 0, ()))),
    "a": (
        ("own",),
        (
            ("ry+", 0, -1, (EVERY, 0)), ("ry-", 0, 1, (EVERY, 1)),
            ("a1z+", 0, -1, (0,)), ("a1z-", 0, -1, (0,)), ("b1y+", -1, 0, (1,)), ("b1y-", -1, 0, (1,)),
            ("a3z+", 0, 1, (0,)), ("a3z-", 0, 1, (0,)), ("b3y+", 1, 0, (1,)), ("b3y-", 1, 0, (1,)),
        ),
    ),
    "b": ((), (("rz+", -1, 0, (EVERY, 0)), ("rz-", 1, 0, (EVERY, 1)))),
    "e": (("ry",), (("a2z+", 0, 2, (0,)), ("a2z-", 0, 2, (0,)))),
    "f": (("rz",), (("b2y+", 2, 0, (1,)), ("b2y-", 2, 0, (1,)))),
    "g": (
        ("by",),
        (("g1y+", -1, -1, (1, 0)), ("g1y-", -1, 1, (1, 1)), ("g3y+", 1, -1, (1, 0)), ("g3y-", 1, 1, (1, 1))),
    ),
    "h": (
        ("az",),
        (("f1z+", -1, -1, (0, 0)), ("f1z-", 1, -1, (0, 1)), ("f3z+", -1, 1, (0, 0)), ("f3z-", 1, 1, (0, 1))),
    ),
    "i": (("a2",), (("f2z+", -1, 2, (0, 0)), ("f2z-", 1, 2, (0, 1)))),
    "j": (("b2",), (("g2y+", 2, -1, (1, 0)), ("g2y-", 2, 1, (1, 1)))),
}
GROUPS = {
    "own": 16, "ry": 4, "rz": 4, "by": 8, "az": 8, "a2": 4, "b2": 4, "below": 2, "above": 2, "beside": 4, "opposite": 4,
}
NAMES = list(GROUPS)
TOGETHER = len(NAMES) - 3


def group_of(name):
    way, step, link = name[0], name[1], name[-2]
    if way in "or":
        return {"o": "own", "r": "r" + link}[way]
    if way in "ab":
        return way + ("2" if step == "2" else link)
    if step == "2":
        return "opposite"
    return "beside" if way == "f" else {"1": "below", "3": "above"}[step]


def wrap(value, n):
    return lax.rem(value + n, n)


class Place:
    def __init__(self):
        self.rep, self.z, self.y, self.tp = (lax.axis_index(a) for a in AXES)
        self.whole_z = self.rep * 4 + self.z
        self.x, self.core = self.tp // 2, lax.rem(self.tp, 2)
        self.other = 1 - self.core

    def device(self, x=0, y=0, z=0, flip=False):
        z_there = wrap(self.whole_z + z, 8)
        core = self.other if flip else self.core
        return (z_there // 4, lax.rem(z_there, 4), wrap(self.y + y, 4), wrap(self.x + x, 4) * 2 + core)

    def shard(self, z=0, y=0):
        return wrap(self.z + z, 4) * 4 + wrap(self.y + y, 4)

    def slot(self, x=0, flip=False):
        return wrap(self.x + x, 4) * 2 + (self.other if flip else self.core)


class WeightGather:
    def __init__(self, place, index, own_ref, held, local_sem, send_sem, recv_sems, apart):
        self.p, self.i, self.own, self.held = place, index, own_ref, held
        self.local = pltpu.make_async_copy(own_ref, held.at[place.shard()], local_sem.at[index])
        self.send_sem, self.recv_sems, self.apart = send_sem.at[index], recv_sems, apart

    def go(self, kind, z, y, part):
        where = {"y+": dict(y=1), "y-": dict(y=-1), "z+": dict(z=1), "z-": dict(z=-1)}[kind[-2:]]
        view = self.held.at[(self.p.shard(z, y), *part)]
        copy = pltpu.make_async_remote_copy(
            src_ref=view,
            dst_ref=view,
            send_sem=self.send_sem,
            recv_sem=self.semaphore(group_of(kind)),
            device_id=self.p.device(**where),
            device_id_type=MESH,
        )
        copy.start()

    def step(self, name):
        if name == "S":
            self.local.wait()
        waits, sends = STEPS[name]
        self.arrived(*waits)
        for message in sends:
            self.go(*message)

    def semaphore(self, name):
        k = NAMES.index(name)
        if self.apart < 0:
            return self.recv_sems.at[self.i * TOGETHER + min(k, TOGETHER - 1)]
        return self.recv_sems.at[self.i * TOGETHER + self.apart * (len(NAMES) - TOGETHER) + k]

    def finish(self):
        view = self.held.at[pl.ds(0, 3)]
        pltpu.make_async_copy(view, view, self.semaphore(NAMES[-1])).wait()

    def arrived(self, *groups):
        for name in groups:
            quarters = GROUPS[name]
            view = self.held.at[pl.ds(0, quarters // 4)] if quarters >= 4 else self.held.at[0, 0]
            pltpu.make_async_copy(view, view, self.semaphore(name)).wait()

    def drain(self):
        view = self.held.at[pl.ds(0, 15)]
        pltpu.make_async_copy(view, view, self.send_sem).wait()


class TokenGather:
    def __init__(self, place, index, held, start, rows, send_sems, recv_sems):
        self.p, self.held, self.start, self.rows = place, held, start, rows
        self.send_sem, self.recv_sems = send_sems.at[index], recv_sems.at[index]
        self.sent = {}

    def go(self, name, sem, slot, device, start=0, rows=None):
        view = self.held.at[slot, pl.ds(self.start + start, rows or self.rows)]
        copy = pltpu.make_async_remote_copy(
            src_ref=view,
            dst_ref=view,
            send_sem=self.send_sem,
            recv_sem=self.recv_sems.at[sem],
            device_id=device,
            device_id_type=MESH,
        )
        copy.start()
        self.sent[name] = copy

    def slots_of(self, slots, sem):
        view = self.held.at[pl.ds(0, slots), pl.ds(self.start, self.rows)]
        pltpu.make_async_copy(view, view, sem).wait()

    def begin(self):
        p = self.p
        self.go("o+", 0, p.slot(), p.device(x=1))
        self.go("o-", 0, p.slot(), p.device(x=-1))
        self.go("p0", 2, p.slot(), p.device(flip=True))

    def near(self):
        p, half = self.p, self.rows // 2
        self.slots_of(2, self.recv_sems.at[0])
        self.go("f+", 1, p.slot(x=-1), p.device(x=1), 0, half)
        self.go("f-", 1, p.slot(x=1), p.device(x=-1), half, half)
        self.go("p1", 2, p.slot(x=-1), p.device(flip=True))
        self.go("p3", 2, p.slot(x=1), p.device(flip=True))

    def far(self):
        p = self.p
        self.slots_of(1, self.recv_sems.at[1])
        self.go("p2", 2, p.slot(x=2), p.device(flip=True))

    def finish(self):
        self.slots_of(4, self.recv_sems.at[2])

    def drain(self):
        self.slots_of(7, self.send_sem)


class TokenSum:
    def __init__(self, place, index, part, terms, from_core, chip, near, last, send_sems, recv_sems):
        self.p, self.part, self.rows = place, part, pl.ds(part * PART, PART)
        self.terms, self.from_core, self.chip, self.near, self.last = terms, from_core, chip, near, last
        self.send_sem, self.recv_sems = send_sems.at[index], recv_sems.at[index]
        self.sent = {}

    def go(self, name, sem, src, dst, device):
        copy = pltpu.make_async_remote_copy(
            src_ref=src,
            dst_ref=dst,
            send_sem=self.send_sem,
            recv_sem=self.recv_sems.at[sem],
            device_id=device,
            device_id_type=MESH,
        )
        copy.start()
        self.sent[name] = copy

    def half(self, h):
        return pl.ds(self.part * PART + h * HALF, HALF)

    def begin(self):
        p = self.p
        self.go("d", 0, self.terms.at[:, p.other, self.rows], self.from_core.at[:, self.rows], p.device(flip=True))

    def chip_sum(self, x):
        p = self.p
        there = wrap(p.x + x, 4)
        return self.terms[there, p.core, self.rows].astype(F32) + self.from_core[there, self.rows].astype(F32)

    def cores(self):
        p, chip = self.p, self.chip
        self.sent["d"].wait_recv()
        right, left, far = wrap(p.x + 1, 4), wrap(p.x - 1, 4), wrap(p.x + 2, 4)
        chip[far, self.rows] = self.chip_sum(2).astype(BF16)
        self.go("h+", 1, chip.at[far, self.half(0)], self.near.at[0, self.half(0)], p.device(x=1))
        self.go("h-", 1, chip.at[far, self.half(1)], self.near.at[1, self.half(1)], p.device(x=-1))
        chip[right, self.rows] = self.chip_sum(1).astype(BF16)
        self.go("e+", 2, chip.at[right, self.half(1)], self.last.at[0, self.half(1)], p.device(x=1))
        chip[left, self.rows] = self.chip_sum(-1).astype(BF16)
        self.go("e-", 2, chip.at[left, self.half(0)], self.last.at[1, self.half(0)], p.device(x=-1))

    def ring(self):
        p = self.p
        both = self.near.at[0, self.rows]
        pltpu.make_async_copy(both, both, self.recv_sems.at[1]).wait()
        for x, side in ((1, 0), (-1, 1)):
            rows = self.half(side)
            total = self.chip[wrap(p.x + x, 4), rows].astype(F32) + self.near[side, rows].astype(F32)
            self.near[side, rows] = total.astype(BF16)
            self.go("e2", 2, self.near.at[side, rows], self.last.at[side, rows], p.device(x=x))

    def finish(self, base):
        both = self.last.at[:, self.rows]
        pltpu.make_async_copy(both, both, self.recv_sems.at[2]).wait()
        total = self.chip_sum(0) + (self.last[0, self.rows].astype(F32) + self.last[1, self.rows].astype(F32))
        return (base.astype(F32) + total).astype(BF16)

    def drain(self):
        view = self.terms.at[:, 0, self.rows]
        part = self.chip.at[pl.ds(0, 3), self.rows]
        pltpu.make_async_copy(view, view, self.send_sem).wait()
        pltpu.make_async_copy(part, part, self.send_sem).wait()


class ColumnSum:
    def __init__(self, place, index, part, terms, from_core, chip, near, last, send_sems, recv_sems):
        self.p, self.start, self.rows = place, part * TALL, pl.ds(part * TALL, TALL)
        self.terms, self.from_core, self.chip, self.near, self.last = terms, from_core, chip, near, last
        self.send_sem, self.recv_sems = send_sems.at[index], recv_sems.at[index]

    def go(self, sem, src, dst, device):
        pltpu.make_async_remote_copy(
            src_ref=src,
            dst_ref=dst,
            send_sem=self.send_sem,
            recv_sem=self.recv_sems.at[sem],
            device_id=device,
            device_id_type=MESH,
        ).start()

    def arrived(self, view, sem):
        pltpu.make_async_copy(view, view, self.recv_sems.at[sem]).wait()

    def half(self, h):
        return pl.ds(self.start + h * (TALL // 2), TALL // 2)

    def chip_sum(self, there, rows):
        return self.terms[there, self.p.core, rows].astype(F32) + self.from_core[there, rows].astype(F32)

    def begin(self, k, core=None):
        there = wrap(self.p.z + k, 4)

        def send():
            terms = self.terms.at[there, self.p.other, self.rows]
            self.go(k, terms, self.from_core.at[there, self.rows], self.p.device(flip=True))

        if core is None:
            send()
        else:
            pl.when(core != self.p.core)(send)

    def away(self, k, core):
        there = wrap(self.p.z + k, 4)
        away = wrap(there - self.p.x, 4)
        return there, away if core is None else jnp.where(core == self.p.core, away, 4)

    def cores(self, k, core=None):
        p, chip = self.p, self.chip
        there, away = self.away(k, core)
        arrived = functools.partial(self.arrived, self.from_core.at[0, self.rows], k)
        if core is None:
            arrived()
        else:
            pl.when(core == p.core)(arrived)

        def add(rows):
            chip[there, rows] = self.chip_sum(there, rows).astype(BF16)

        @pl.when(away == 2)
        def _():
            add(self.rows)
            self.go(4, chip.at[there, self.half(0)], self.near.at[0, self.half(0)], p.device(x=1))
            self.go(5, chip.at[there, self.half(1)], self.near.at[1, self.half(1)], p.device(x=-1))

        for distance, x, side in ((1, 1, 0), (3, -1, 1)):

            @pl.when(away == distance)
            def _(x=x, side=side):
                rows = self.half(1 - side)
                add(rows)
                self.go(6, chip.at[there, rows], self.last.at[side, rows], p.device(x=x))
                add(self.half(side))

    def ring(self, k, core=None):
        p = self.p
        there, away = self.away(k, core)
        for distance, x, side in ((1, 1, 0), (3, -1, 1)):

            @pl.when(away == distance)
            def _(x=x, side=side):
                rows = self.half(side)
                view = self.near.at[side, rows]
                self.arrived(view, 4 + side)
                total = self.chip[there, rows].astype(F32) + self.near[side, rows].astype(F32)
                self.near[side, rows] = total.astype(BF16)
                self.go(6, view, self.last.at[side, rows], p.device(x=x))

    def finish(self, base):
        self.arrived(self.last.at[:, self.rows], 6)
        total = self.chip_sum(self.p.x, self.rows)
        total = total + (self.last[0, self.rows].astype(F32) + self.last[1, self.rows].astype(F32))
        return (base.astype(F32) + total).astype(BF16)

    def drain(self):
        view = self.chip.at[:, self.rows]
        part = self.chip.at[pl.ds(0, 3), self.rows]
        pltpu.make_async_copy(view, view, self.send_sem).wait()
        pltpu.make_async_copy(part, part, self.send_sem).wait()


def norm_rows(held, rows, gain_ref, normed):
    total = jnp.zeros((PART, 1), F32)
    for k in range(GROUP):
        piece = held[k, rows].astype(F32)
        total = total + jnp.sum(piece * piece, axis=-1, keepdims=True)
    inverse = lax.rsqrt(total * (1.0 / (GROUP * WIDTH)) + EPSILON)
    for k in range(GROUP):
        columns = slice(k * WIDTH, (k + 1) * WIDTH)
        piece = held[k, rows].astype(F32) * inverse * gain_ref[:, columns]
        normed[rows, columns] = piece.astype(BF16)


def block_diagonal(matrix_ref, out_ref, offset):
    blocks, size, _ = matrix_ref.shape
    row = lax.broadcasted_iota(jnp.int32, (size, blocks * size), 0)
    column = lax.broadcasted_iota(jnp.int32, (size, blocks * size), 1)
    for b in range(blocks):
        select = (column == row + b * size).astype(F32).astype(BF16)
        spread = jnp.dot(matrix_ref[b], select, preferred_element_type=F32)
        out_ref[b * size : (b + 1) * size, offset : offset + blocks * size] = spread.astype(BF16)


def shifted(values, by, row, fill):
    return jnp.where(row >= by, pltpu.roll(values, by, 0), fill)


def mixer_rows(values, offsets, taps, maps, rate):
    channels = values.shape[1]
    row = lax.broadcasted_iota(jnp.int32, values.shape, 0)
    wide = values.astype(F32)
    reach = taps.shape[0]
    total = taps[0:1] * shifted(wide, reach - 1, row, 0.0)
    for k in range(1, reach):
        by = reach - 1 - k
        total = total + taps[k : k + 1] * (shifted(wide, by, row, 0.0) if by else wide)
    conved = total.astype(BF16)
    both = jax.nn.sigmoid(jnp.dot(conved, maps, preferred_element_type=F32))
    decay = rate * both[:, :channels] + offsets
    factor = jnp.exp(decay)
    twice = 2.0 * decay
    small = -twice * (1.0 + twice * (0.5 + twice * (1.0 / 6.0 + twice * (1.0 / 24.0))))
    lost = jnp.where(twice > -0.03, small, 1.0 - factor * factor)
    state = jnp.sqrt(lost) * both[:, channels:] * conved.astype(F32)
    by = 1
    while by < SEQ_LEN:
        state = factor * shifted(state, by, row, 0.0) + state
        if 2 * by < SEQ_LEN:
            factor = factor * shifted(factor, by, row, 1.0)
        by *= 2
    return state


def gated(state, gates):
    gate = gates.astype(F32)
    gelu = 0.5 * gate * (1.0 + lax.erf(gate * (0.5**0.5)))
    return (state * gelu).astype(BF16)


ORDER = (
    "0S GS 1S 2S", "0a 0b 1a GA0", "1b 2a GA1 0f", "2b 1e 0e 1h", "1f X GB0 0g", "1g 2e 0h 2f",
    "2g 1i 2h GF0", "GB1 1j 0j 0i", "3S N1 GF1 2i", "N3 2j 4S 5S", "N2 N0 1F 0F", "I1 7S I0 M0",
    "2F 3a P0 M2", "6S P2 M1 4a", "M3 3b K0 P1", "P3 5a K2 K1", "R0 4b 8S K3", "5b 4e 7a R1",
    "R2 7b L0 4f", "5e 6a 6b 3f", "R3 L1 5f 8a", "3e L2 8b 5h", "L3 5g 4h 7f", "5i A0 6e 3g",
    "4j A1 4i A2", "3j 4g 3h 5j", "A3 6f 8f 3i", "B0 7e 8h B1", "B2 6h 8e Q0", "6g 8g 7g 7h",
    "6i B3 Q1 7j", "Q2 5F 4F 3F", "U0 Q3 U1 V0", "8j 8i 7i 6j", "V1 V2 V3 k00", "k10 k20 k31 V4",
    "k21 k11 k01 k30", "k40 r00 k41 r20", "r10 r01 r30 r11", "r21 r40 r31 r41", "l0 l1",
)


def kernel(
    stream_ref, gain1_hbm, gain2_hbm, input_ref, gate_ref, taps_hbm, decay_hbm, inmap_hbm, param_hbm, offset_hbm,
    output_ref, up_ref, down_ref,
    out_ref,
    w_input, w_gate, w_output, w_up0, w_up1, w_up2, w_down0, w_down1, w_down2,
    held1, held2, normed, values, gates, offsets, state, activity, maps,
    terms1, core1, chip1, near1, last1, terms2, core2, chip2, near2, last2,
    gain1, gain2, taps_ref, decay_ref, inmap_ref, param_ref, rate_ref,
    local_sem, wsend, wrecv, tsend, trecv, csend, crecv,
):
    w_up, w_down = (w_up0, w_up1, w_up2), (w_down0, w_down1, w_down2)
    p = Place()
    barrier = pltpu.get_barrier_semaphore()
    greeted = [dict(x=1), dict(x=-1), dict(y=1), dict(y=-1), dict(z=1), dict(z=-1), dict(flip=True)]
    for where in greeted:
        pl.semaphore_signal(barrier, inc=1, device_id=p.device(**where), device_id_type=MESH)
    blocks = range(len(w_up))
    weights = [
        WeightGather(p, i, own, held, local_sem, wsend, wrecv, i - 3 - len(blocks))
        for i, (own, held) in enumerate(
            (
                (input_ref, w_input),
                (gate_ref, w_gate),
                (output_ref, w_output),
                *((up_ref.at[:, :, :, n * WIDTH : (n + 1) * WIDTH], w_up[n]) for n in blocks),
                *((down_ref.at[n], w_down[n]) for n in blocks),
            )
        )
    ]
    own_stream = pltpu.make_async_copy(stream_ref, held1.at[p.tp], local_sem.at[9])
    small = [
        pltpu.make_async_copy(source, target, local_sem.at[10 + k])
        for k, (source, target) in enumerate(
            (
                (decay_hbm, decay_ref),
                (inmap_hbm, inmap_ref),
                (param_hbm, param_ref),
                (gain1_hbm, gain1),
                (gain2_hbm, gain2),
                (taps_hbm, taps_ref),
                (offset_hbm, offsets),
            )
        )
    ]
    for copy in (weights[0].local, own_stream, *(w.local for w in weights[1:]), *small):
        copy.start()
    pl.semaphore_wait(barrier, len(greeted))

    gather1 = [TokenGather(p, c, held1, c * TALL, TALL, tsend, trecv) for c in range(2)]
    gather2 = [TokenGather(p, 2 + c, held2, c * PART, PART, tsend, trecv) for c in range(PARTS)]
    sum1 = [
        TokenSum(p, 2 + PARTS + c, c, terms1, core1, chip1, near1, last1, tsend, trecv) for c in range(PARTS)
    ]
    sum2 = [ColumnSum(p, c, c, terms2, core2, chip2, near2, last2, csend, crecv) for c in range(2)]
    def rows_of(c):
        return pl.ds(c * PART, PART)

    def prepare():
        for copy in small:
            copy.wait()
        block_diagonal(decay_ref, maps, 0)
        block_diagonal(inmap_ref, maps, WIDTH)
        parameter = -param_ref[...]
        softplus = jnp.maximum(parameter, 0.0) + jnp.log1p(jnp.exp(-jnp.abs(parameter)))
        rate_ref[...] = -DECAY_MULTIPLIER * softplus

    def begin():
        own_stream.wait()
        for gather in gather1:
            gather.begin()

    def columns_of(held, j, depth):
        pair = held[2 * j : 2 * j + 2].reshape(2, depth, 128)
        return jnp.concatenate([pair[0], pair[1]], axis=1)

    def inward(m):
        rows = pl.ds(m * TALL, TALL)
        columns = normed[rows, :]
        for held, target in ((w_input, values), (w_gate, gates)):
            full = held[...].reshape(GROUP * WIDTH, WIDTH)
            target[rows, :] = jnp.dot(columns, full, preferred_element_type=F32).astype(BF16)

    def mix(c):
        rows = rows_of(c)
        taps = taps_ref[...].astype(F32)
        state[rows, :] = mixer_rows(values[rows, :], offsets[rows, :], taps, maps[...], rate_ref[...])

    def project(c):
        rows = rows_of(c)
        mixed = gated(state[rows, :], gates[rows, :])
        for j in range(GROUP):
            product = jnp.dot(mixed, columns_of(w_output, j, WIDTH), preferred_element_type=F32)
            terms1[j // 2, j % 2, rows] = product.astype(BF16)
        sum1[c].begin()

    def last_core(turn):
        near = p.y // 2
        return {3: near, 4: 1 - near}.get(turn)

    def lower(turn):
        z, core = TURNS[turn], last_core(turn)
        there = wrap(p.z + z, 4)
        for w in weights[-len(blocks) :]:
            w.arrived(*(() if turn == 0 else (NAMES[turn - 5],)))
        for c in range(2):
            rows = pl.ds(c * TALL, TALL)
            for k in (0, 1) if core is None else (core,):
                product = 0.0
                for n in blocks:
                    pair = w_down[n][pl.ds(there * 4 + 2 * k, 2)].reshape(2, WIDTH, 128)
                    columns = jnp.concatenate([pair[0], pair[1]], axis=1)
                    some = activity[rows, n * WIDTH : (n + 1) * WIDTH]
                    product = product + jnp.dot(some, columns, preferred_element_type=F32)
                terms2[there, k, rows] = product.astype(BF16)
            sum2[c].begin(z % 4, core)

    def middle_of(c):
        rows = rows_of(c)
        held2[p.tp, rows] = sum1[c].finish(held1[p.tp, rows])
        gather2[c].begin()

    def raise_rows(c):
        gather2[c].finish()
        norm_rows(held2, rows_of(c), gain2, normed)

    def lift(c):
        rows = pl.ds(c * TALL, TALL)
        columns = normed[rows, :]
        for n in blocks:
            full = w_up[n][...].reshape(GROUP * WIDTH, WIDTH)
            raised = jnp.maximum(jnp.dot(columns, full, preferred_element_type=F32), 0.0)
            activity[rows, n * WIDTH : (n + 1) * WIDTH] = (raised * raised).astype(BF16)

    def last_of(c):
        rows = pl.ds(c * TALL, TALL)
        out_ref[rows, :] = sum2[c].finish(held2[p.tp, rows])

    actions = {
        "X": prepare,
        "GS": begin,
    }
    for i, w in enumerate(weights):
        for name in STEPS:
            actions[f"{i}{name}"] = functools.partial(w.step, name)
        if i < 3 + len(blocks):
            actions[f"{i}F"] = w.finish
    for c in range(PARTS):
        actions[f"N{c}"] = functools.partial(norm_rows, held1, rows_of(c), gain1, normed)
        actions[f"M{c}"] = functools.partial(mix, c)
        actions[f"P{c}"] = functools.partial(project, c)
        actions[f"K{c}"] = sum1[c].cores
        actions[f"L{c}"] = functools.partial(middle_of, c)
        actions[f"B{c}"] = gather2[c].far
        actions[f"Q{c}"] = functools.partial(raise_rows, c)
        actions[f"R{c}"] = sum1[c].ring
        actions[f"A{c}"] = gather2[c].near
    for turn, z in enumerate(TURNS):
        actions[f"V{turn}"] = functools.partial(lower, turn)
        for c in range(2):
            actions[f"k{turn}{c}"] = functools.partial(sum2[c].cores, z % 4, last_core(turn))
            actions[f"r{turn}{c}"] = functools.partial(sum2[c].ring, z % 4, last_core(turn))
    for c in range(2):
        actions[f"GA{c}"] = gather1[c].near
        actions[f"GB{c}"] = gather1[c].far
        actions[f"GF{c}"] = gather1[c].finish
        actions[f"I{c}"] = functools.partial(inward, c)
        actions[f"U{c}"] = functools.partial(lift, c)
        actions[f"l{c}"] = functools.partial(last_of, c)
    order = " ".join(ORDER).split()
    assert sorted(order) == sorted(actions)
    for name in order:
        actions[name]()

    for w in weights:
        w.drain()
    for event in (*gather1, *gather2, *sum1, *sum2):
        event.drain()


def quarters(weight):
    rows, columns = weight.shape
    return weight.reshape(2, 2, rows // 4, columns)


def shards(
    stream,
    recurrent_norm_gain,
    feedforward_norm_gain,
    recurrent_input_weight,
    output_gate_weight,
    causal_filter_weight,
    decay_gate_matrix,
    input_gate_matrix,
    channel_decay_param,
    token_decay_offset,
    recurrent_output_weight,
    up_projection_weight,
    down_projection_weight,
):
    mixer = [quarters(w) for w in (recurrent_input_weight, output_gate_weight, recurrent_output_weight)]
    up, hidden = quarters(up_projection_weight), up_projection_weight.shape[1]
    blocks = hidden // WIDTH
    down = down_projection_weight.reshape(blocks, 2, 2, WIDTH // 4, -1)
    arguments = (
        stream,
        recurrent_norm_gain.reshape(1, -1),
        feedforward_norm_gain.reshape(1, -1),
        mixer[0],
        mixer[1],
        causal_filter_weight,
        decay_gate_matrix,
        input_gate_matrix,
        channel_decay_param.reshape(1, -1),
        token_decay_offset,
        mixer[2],
        up,
        down,
    )
    far = pl.BlockSpec(memory_space=pltpu.HBM)
    sums = [
        pltpu.VMEM((4, 2, ROWS, WIDTH), BF16),
        pltpu.VMEM((4, ROWS, WIDTH), BF16),
        pltpu.VMEM((4, ROWS, WIDTH), BF16),
        pltpu.VMEM((2, ROWS, WIDTH), BF16),
        pltpu.VMEM((2, ROWS, WIDTH), BF16),
    ]
    events = 2 + 2 * PARTS
    return pl.pallas_call(
        kernel,
        out_shape=jax.ShapeDtypeStruct(stream.shape, stream.dtype),
        in_specs=[far] * 13,
        out_specs=pl.BlockSpec(memory_space=pltpu.VMEM),
        scratch_shapes=[
            *[pltpu.VMEM((16, *w.shape), BF16) for w in mixer],
            *[pltpu.VMEM((16, *up.shape[:-1], WIDTH), BF16)] * blocks,
            *[pltpu.VMEM((16, *down.shape[1:]), BF16)] * blocks,
            pltpu.VMEM((GROUP, ROWS, WIDTH), BF16),
            pltpu.VMEM((GROUP, ROWS, WIDTH), BF16),
            pltpu.VMEM((ROWS, GROUP * WIDTH), BF16),
            pltpu.VMEM((ROWS, WIDTH), BF16),
            pltpu.VMEM((ROWS, WIDTH), BF16),
            pltpu.VMEM((ROWS, WIDTH), F32),
            pltpu.VMEM((ROWS, WIDTH), F32),
            pltpu.VMEM((ROWS, hidden), BF16),
            pltpu.VMEM((WIDTH, 2 * WIDTH), BF16),
            *sums,
            *sums,
            pltpu.VMEM((1, GROUP * WIDTH), F32),
            pltpu.VMEM((1, GROUP * WIDTH), F32),
            pltpu.VMEM(causal_filter_weight.shape, BF16),
            pltpu.VMEM(decay_gate_matrix.shape, BF16),
            pltpu.VMEM(input_gate_matrix.shape, BF16),
            pltpu.VMEM((1, WIDTH), F32),
            pltpu.VMEM((1, WIDTH), F32),
            pltpu.SemaphoreType.DMA((17,)),
            pltpu.SemaphoreType.DMA((3 + 2 * blocks,)),
            pltpu.SemaphoreType.DMA(((3 + 2 * blocks) * TOGETHER + blocks * (len(NAMES) - TOGETHER),)),
            pltpu.SemaphoreType.DMA((events,)),
            pltpu.SemaphoreType.DMA((events, 3)),
            pltpu.SemaphoreType.DMA((2,)),
            pltpu.SemaphoreType.DMA((2, 7)),
        ],
        compiler_params=pltpu.CompilerParams(
            collective_id=0, has_side_effects=True, vmem_limit_bytes=VMEM_LIMIT
        ),
    )(*(pltpu.with_memory_space_constraint(value, pltpu.HBM) for value in arguments))


def solution(mesh):
    split = Mesh(
        mesh.devices.reshape(mesh.shape["rep"], 4, 4, mesh.shape["tp"]),
        AXES,
    )
    placed = (
        P(REP_FS, "tp"),
        P(),
        P(),
        P(FS, "tp"),
        P(FS, "tp"),
        P(None, "tp"),
        P("tp", None, None),
        P("tp", None, None),
        P("tp"),
        P(REP_FS, "tp"),
        P("tp", FS),
        P(FS, "tp"),
        P("tp", FS),
    )
    return jax.shard_map(
        shards, mesh=split, in_specs=placed, out_specs=P(REP_FS, "tp"), check_vma=False
    )
```

```python
import functools

import jax
import jax.numpy as jnp
from jax import lax
from jax.experimental import pallas as pl
from jax.experimental.pallas import tpu as pltpu
from jax.sharding import Mesh
from jax.sharding import PartitionSpec as P

MESH = pl.DeviceIdType.MESH
SEQ_LEN = 128
FS = ("fs_0", "fs_1")
REP_FS = ("rep", "fs_0", "fs_1")
AXES = ("rep", "fs_0", "fs_1", "tp")

EPSILON = 1e-06
DECAY_MULTIPLIER = 8.0
F32 = jnp.float32
BF16 = jnp.bfloat16

ROWS, WIDTH, PARTS, GROUP = 512, 256, 4, 8
PART = ROWS // PARTS
HALF = PART // 2
TALL = ROWS // 2
VMEM_LIMIT = 40 * 1024 * 1024
TURNS = (0, -1, 1, 2, 2)

EVERY = slice(None)
STEPS = {
    "S": ((), (("oy+", 0, 0, ()), ("oy-", 0, 0, ()), ("oz+", 0, 0, ()), ("oz-", 0, 0, ()))),
    "a": (
        ("own",),
        (
            ("ry+", 0, -1, (EVERY, 0)), ("ry-", 0, 1, (EVERY, 1)),
            ("a1z+", 0, -1, (0,)), ("a1z-", 0, -1, (0,)), ("b1y+", -1, 0, (1,)), ("b1y-", -1, 0, (1,)),
            ("a3z+", 0, 1, (0,)), ("a3z-", 0, 1, (0,)), ("b3y+", 1, 0, (1,)), ("b3y-", 1, 0, (1,)),
        ),
    ),
    "b": ((), (("rz+", -1, 0, (EVERY, 0)), ("rz-", 1, 0, (EVERY, 1)))),
    "e": (("ry",), (("a2z+", 0, 2, (0,)), ("a2z-", 0, 2, (0,)))),
    "f": (("rz",), (("b2y+", 2, 0, (1,)), ("b2y-", 2, 0, (1,)))),
    "g": (
        ("by",),
        (("g1y+", -1, -1, (1, 0)), ("g1y-", -1, 1, (1, 1)), ("g3y+", 1, -1, (1, 0)), ("g3y-", 1, 1, (1, 1))),
    ),
    "h": (
        ("az",),
        (("f1z+", -1, -1, (0, 0)), ("f1z-", 1, -1, (0, 1)), ("f3z+", -1, 1, (0, 0)), ("f3z-", 1, 1, (0, 1))),
    ),
    "i": (("a2",), (("f2z+", -1, 2, (0, 0)), ("f2z-", 1, 2, (0, 1)))),
    "j": (("b2",), (("g2y+", 2, -1, (1, 0)), ("g2y-", 2, 1, (1, 1)))),
}
GROUPS = {
    "own": 16, "ry": 4, "rz": 4, "by": 8, "az": 8, "a2": 4, "b2": 4, "below": 2, "above": 2, "beside": 4, "opposite": 4,
}
NAMES = list(GROUPS)
TOGETHER = len(NAMES) - 3


def group_of(name):
    way, step, link = name[0], name[1], name[-2]
    if way in "or":
        return {"o": "own", "r": "r" + link}[way]
    if way in "ab":
        return way + ("2" if step == "2" else link)
    if step == "2":
        return "opposite"
    return "beside" if way == "f" else {"1": "below", "3": "above"}[step]


def wrap(value, n):
    return lax.rem(value + n, n)


class Place:
    def __init__(self):
        self.rep, self.z, self.y, self.tp = (lax.axis_index(a) for a in AXES)
        self.whole_z = self.rep * 4 + self.z
        self.x, self.core = self.tp // 2, lax.rem(self.tp, 2)
        self.other = 1 - self.core

    def device(self, x=0, y=0, z=0, flip=False):
        z_there = wrap(self.whole_z + z, 8)
        core = self.other if flip else self.core
        return (z_there // 4, lax.rem(z_there, 4), wrap(self.y + y, 4), wrap(self.x + x, 4) * 2 + core)

    def shard(self, z=0, y=0):
        return wrap(self.z + z, 4) * 4 + wrap(self.y + y, 4)

    def slot(self, x=0, flip=False):
        return wrap(self.x + x, 4) * 2 + (self.other if flip else self.core)


class WeightGather:
    def __init__(self, place, index, own_ref, held, local_sem, send_sem, recv_sems, apart):
        self.p, self.i, self.own, self.held = place, index, own_ref, held
        self.local = pltpu.make_async_copy(own_ref, held.at[place.shard()], local_sem.at[index])
        self.send_sem, self.recv_sems, self.apart = send_sem.at[index], recv_sems, apart

    def go(self, kind, z, y, part):
        where = {"y+": dict(y=1), "y-": dict(y=-1), "z+": dict(z=1), "z-": dict(z=-1)}[kind[-2:]]
        view = self.held.at[(self.p.shard(z, y), *part)]
        copy = pltpu.make_async_remote_copy(
            src_ref=view,
            dst_ref=view,
            send_sem=self.send_sem,
            recv_sem=self.semaphore(group_of(kind)),
            device_id=self.p.device(**where),
            device_id_type=MESH,
        )
        copy.start()

    def step(self, name):
        if name == "S":
            self.local.wait()
        waits, sends = STEPS[name]
        self.arrived(*waits)
        for message in sends:
            self.go(*message)

    def semaphore(self, name):
        k = NAMES.index(name)
        if self.apart < 0:
            return self.recv_sems.at[self.i * TOGETHER + min(k, TOGETHER - 1)]
        return self.recv_sems.at[self.i * TOGETHER + self.apart * (len(NAMES) - TOGETHER) + k]

    def finish(self):
        view = self.held.at[pl.ds(0, 3)]
        pltpu.make_async_copy(view, view, self.semaphore(NAMES[-1])).wait()

    def arrived(self, *groups):
        for name in groups:
            quarters = GROUPS[name]
            view = self.held.at[pl.ds(0, quarters // 4)] if quarters >= 4 else self.held.at[0, 0]
            pltpu.make_async_copy(view, view, self.semaphore(name)).wait()

    def drain(self):
        view = self.held.at[pl.ds(0, 15)]
        pltpu.make_async_copy(view, view, self.send_sem).wait()


class TokenGather:
    def __init__(self, place, index, held, start, rows, send_sems, recv_sems):
        self.p, self.held, self.start, self.rows = place, held, start, rows
        self.send_sem, self.recv_sems = send_sems.at[index], recv_sems.at[index]
        self.sent = {}

    def go(self, name, sem, slot, device, start=0, rows=None):
        view = self.held.at[slot, pl.ds(self.start + start, rows or self.rows)]
        copy = pltpu.make_async_remote_copy(
            src_ref=view,
            dst_ref=view,
            send_sem=self.send_sem,
            recv_sem=self.recv_sems.at[sem],
            device_id=device,
            device_id_type=MESH,
        )
        copy.start()
        self.sent[name] = copy

    def slots_of(self, slots, sem):
        view = self.held.at[pl.ds(0, slots), pl.ds(self.start, self.rows)]
        pltpu.make_async_copy(view, view, sem).wait()

    def begin(self):
        p = self.p
        self.go("o+", 0, p.slot(), p.device(x=1))
        self.go("o-", 0, p.slot(), p.device(x=-1))
        self.go("p0", 2, p.slot(), p.device(flip=True))

    def near(self):
        p, half = self.p, self.rows // 2
        self.slots_of(2, self.recv_sems.at[0])
        self.go("f+", 1, p.slot(x=-1), p.device(x=1), 0, half)
        self.go("f-", 1, p.slot(x=1), p.device(x=-1), half, half)
        self.go("p1", 2, p.slot(x=-1), p.device(flip=True))
        self.go("p3", 2, p.slot(x=1), p.device(flip=True))

    def far(self):
        p = self.p
        self.slots_of(1, self.recv_sems.at[1])
        self.go("p2", 2, p.slot(x=2), p.device(flip=True))

    def finish(self):
        self.slots_of(4, self.recv_sems.at[2])

    def drain(self):
        self.slots_of(7, self.send_sem)


class TokenSum:
    def __init__(self, place, index, part, terms, from_core, chip, near, last, send_sems, recv_sems):
        self.p, self.part, self.rows = place, part, pl.ds(part * PART, PART)
        self.terms, self.from_core, self.chip, self.near, self.last = terms, from_core, chip, near, last
        self.send_sem, self.recv_sems = send_sems.at[index], recv_sems.at[index]
        self.sent = {}

    def go(self, name, sem, src, dst, device):
        copy = pltpu.make_async_remote_copy(
            src_ref=src,
            dst_ref=dst,
            send_sem=self.send_sem,
            recv_sem=self.recv_sems.at[sem],
            device_id=device,
            device_id_type=MESH,
        )
        copy.start()
        self.sent[name] = copy

    def half(self, h):
        return pl.ds(self.part * PART + h * HALF, HALF)

    def begin(self):
        p = self.p
        self.go("d", 0, self.terms.at[:, p.other, self.rows], self.from_core.at[:, self.rows], p.device(flip=True))

    def chip_sum(self, x):
        p = self.p
        there = wrap(p.x + x, 4)
        return self.terms[there, p.core, self.rows].astype(F32) + self.from_core[there, self.rows].astype(F32)

    def cores(self):
        p, chip = self.p, self.chip
        self.sent["d"].wait_recv()
        right, left, far = wrap(p.x + 1, 4), wrap(p.x - 1, 4), wrap(p.x + 2, 4)
        chip[far, self.rows] = self.chip_sum(2).astype(BF16)
        self.go("h+", 1, chip.at[far, self.half(0)], self.near.at[0, self.half(0)], p.device(x=1))
        self.go("h-", 1, chip.at[far, self.half(1)], self.near.at[1, self.half(1)], p.device(x=-1))
        chip[right, self.rows] = self.chip_sum(1).astype(BF16)
        self.go("e+", 2, chip.at[right, self.half(1)], self.last.at[0, self.half(1)], p.device(x=1))
        chip[left, self.rows] = self.chip_sum(-1).astype(BF16)
        self.go("e-", 2, chip.at[left, self.half(0)], self.last.at[1, self.half(0)], p.device(x=-1))

    def ring(self):
        p = self.p
        both = self.near.at[0, self.rows]
        pltpu.make_async_copy(both, both, self.recv_sems.at[1]).wait()
        for x, side in ((1, 0), (-1, 1)):
            rows = self.half(side)
            total = self.chip[wrap(p.x + x, 4), rows].astype(F32) + self.near[side, rows].astype(F32)
            self.near[side, rows] = total.astype(BF16)
            self.go("e2", 2, self.near.at[side, rows], self.last.at[side, rows], p.device(x=x))

    def finish(self, base):
        both = self.last.at[:, self.rows]
        pltpu.make_async_copy(both, both, self.recv_sems.at[2]).wait()
        total = self.chip_sum(0) + (self.last[0, self.rows].astype(F32) + self.last[1, self.rows].astype(F32))
        return (base.astype(F32) + total).astype(BF16)

    def drain(self):
        view = self.terms.at[:, 0, self.rows]
        part = self.chip.at[pl.ds(0, 3), self.rows]
        pltpu.make_async_copy(view, view, self.send_sem).wait()
        pltpu.make_async_copy(part, part, self.send_sem).wait()


class ColumnSum:
    def __init__(self, place, index, part, terms, from_core, chip, near, last, send_sems, recv_sems):
        self.p, self.start, self.rows = place, part * TALL, pl.ds(part * TALL, TALL)
        self.terms, self.from_core, self.chip, self.near, self.last = terms, from_core, chip, near, last
        self.send_sem, self.recv_sems = send_sems.at[index], recv_sems.at[index]

    def go(self, sem, src, dst, device):
        pltpu.make_async_remote_copy(
            src_ref=src,
            dst_ref=dst,
            send_sem=self.send_sem,
            recv_sem=self.recv_sems.at[sem],
            device_id=device,
            device_id_type=MESH,
        ).start()

    def arrived(self, view, sem):
        pltpu.make_async_copy(view, view, self.recv_sems.at[sem]).wait()

    def half(self, h):
        return pl.ds(self.start + h * (TALL // 2), TALL // 2)

    def chip_sum(self, there, rows):
        return self.terms[there, self.p.core, rows].astype(F32) + self.from_core[there, rows].astype(F32)

    def begin(self, k, core=None):
        there = wrap(self.p.z + k, 4)

        def send():
            terms = self.terms.at[there, self.p.other, self.rows]
            self.go(k, terms, self.from_core.at[there, self.rows], self.p.device(flip=True))

        if core is None:
            send()
        else:
            pl.when(core != self.p.core)(send)

    def away(self, k, core):
        there = wrap(self.p.z + k, 4)
        away = wrap(there - self.p.x, 4)
        return there, away if core is None else jnp.where(core == self.p.core, away, 4)

    def cores(self, k, core=None):
        p, chip = self.p, self.chip
        there, away = self.away(k, core)
        arrived = functools.partial(self.arrived, self.from_core.at[0, self.rows], k)
        if core is None:
            arrived()
        else:
            pl.when(core == p.core)(arrived)

        def add(rows):
            chip[there, rows] = self.chip_sum(there, rows).astype(BF16)

        @pl.when(away == 2)
        def _():
            add(self.rows)
            self.go(4, chip.at[there, self.half(0)], self.near.at[0, self.half(0)], p.device(x=1))
            self.go(5, chip.at[there, self.half(1)], self.near.at[1, self.half(1)], p.device(x=-1))

        for distance, x, side in ((1, 1, 0), (3, -1, 1)):

            @pl.when(away == distance)
            def _(x=x, side=side):
                rows = self.half(1 - side)
                add(rows)
                self.go(6, chip.at[there, rows], self.last.at[side, rows], p.device(x=x))
                add(self.half(side))

    def ring(self, k, core=None):
        p = self.p
        there, away = self.away(k, core)
        for distance, x, side in ((1, 1, 0), (3, -1, 1)):

            @pl.when(away == distance)
            def _(x=x, side=side):
                rows = self.half(side)
                view = self.near.at[side, rows]
                self.arrived(view, 4 + side)
                total = self.chip[there, rows].astype(F32) + self.near[side, rows].astype(F32)
                self.near[side, rows] = total.astype(BF16)
                self.go(6, view, self.last.at[side, rows], p.device(x=x))

    def finish(self, base):
        self.arrived(self.last.at[:, self.rows], 6)
        total = self.chip_sum(self.p.x, self.rows)
        total = total + (self.last[0, self.rows].astype(F32) + self.last[1, self.rows].astype(F32))
        return (base.astype(F32) + total).astype(BF16)

    def drain(self):
        view = self.chip.at[:, self.rows]
        part = self.chip.at[pl.ds(0, 3), self.rows]
        pltpu.make_async_copy(view, view, self.send_sem).wait()
        pltpu.make_async_copy(part, part, self.send_sem).wait()


def norm_rows(held, rows, gain_ref, normed):
    total = jnp.zeros((PART, 1), F32)
    for k in range(GROUP):
        piece = held[k, rows].astype(F32)
        total = total + jnp.sum(piece * piece, axis=-1, keepdims=True)
    inverse = lax.rsqrt(total * (1.0 / (GROUP * WIDTH)) + EPSILON)
    for k in range(GROUP):
        columns = slice(k * WIDTH, (k + 1) * WIDTH)
        piece = held[k, rows].astype(F32) * inverse * gain_ref[:, columns]
        normed[rows, columns] = piece.astype(BF16)


def block_diagonal(matrix_ref, out_ref, offset):
    blocks, size, _ = matrix_ref.shape
    row = lax.broadcasted_iota(jnp.int32, (size, blocks * size), 0)
    column = lax.broadcasted_iota(jnp.int32, (size, blocks * size), 1)
    for b in range(blocks):
        select = (column == row + b * size).astype(F32).astype(BF16)
        spread = jnp.dot(matrix_ref[b], select, preferred_element_type=F32)
        out_ref[b * size : (b + 1) * size, offset : offset + blocks * size] = spread.astype(BF16)


def shifted(values, by, row, fill):
    return jnp.where(row >= by, pltpu.roll(values, by, 0), fill)


def mixer_rows(values, offsets, taps, maps, rate):
    channels = values.shape[1]
    row = lax.broadcasted_iota(jnp.int32, values.shape, 0)
    wide = values.astype(F32)
    reach = taps.shape[0]
    total = taps[0:1] * shifted(wide, reach - 1, row, 0.0)
    for k in range(1, reach):
        by = reach - 1 - k
        total = total + taps[k : k + 1] * (shifted(wide, by, row, 0.0) if by else wide)
    conved = total.astype(BF16)
    both = jax.nn.sigmoid(jnp.dot(conved, maps, preferred_element_type=F32))
    decay = rate * both[:, :channels] + offsets
    factor = jnp.exp(decay)
    twice = 2.0 * decay
    small = -twice * (1.0 + twice * (0.5 + twice * (1.0 / 6.0 + twice * (1.0 / 24.0))))
    lost = jnp.where(twice > -0.03, small, 1.0 - factor * factor)
    state = jnp.sqrt(lost) * both[:, channels:] * conved.astype(F32)
    by = 1
    while by < SEQ_LEN:
        state = factor * shifted(state, by, row, 0.0) + state
        if 2 * by < SEQ_LEN:
            factor = factor * shifted(factor, by, row, 1.0)
        by *= 2
    return state


def gated(state, gates):
    gate = gates.astype(F32)
    gelu = 0.5 * gate * (1.0 + lax.erf(gate * (0.5**0.5)))
    return (state * gelu).astype(BF16)


ORDER = (
    "0S GS 1S 2S", "0a X 0b GA0", "1a 1b 2a 0e", "2b GA1 1e 0f", "0h 0g 1f GB0", "2e GB1 1g 6S",
    "1h 0i 2f GF1", "GF0 0j N2 1i", "1j 2g 3S 2i", "2h N3 N0 2j", "4S N1 5S 1F", "7S 0F I1 I0",
    "M0 M2 2F P0", "M1 P1 3a M3", "P2 3b 4a K0", "K1 8S P3 K2", "5a R0 4b K3", "3f 5b 3e 7a",
    "4e R1 6a R2", "R3 L0 5e 8a", "5f L1 L2 6b", "4f L3 4g 5h", "3i 7b 4h 7g", "3g A1 3h 8b",
    "A0 4i A2 5g", "A3 4j 5i 5j", "7e 8e 3j 6e", "7h 8h 7f B0", "6f 6h B1 B2", "8f 8g 6g B3",
    "4F Q1 Q0 5F", "3F U0 Q3 Q2", "6i 7j 8i 6j", "U1 8j V0 7i", "V1 V2 V3 k00", "k10 V4 k01 k20",
    "k30 k11 k31 k21", "k40 k41 r10 r20", "r30 r00 r01 r11", "r21 r31 r40 r41", "l0 l1",
)


def kernel(
    stream_ref, gain1_hbm, gain2_hbm, input_ref, gate_ref, taps_hbm, decay_hbm, inmap_hbm, param_hbm, offset_hbm,
    output_ref, up_ref, down_ref,
    out_ref,
    w_input, w_gate, w_output, w_up0, w_up1, w_up2, w_down0, w_down1, w_down2,
    held1, held2, normed, values, gates, offsets, state, activity, maps,
    terms1, core1, chip1, near1, last1, terms2, core2, chip2, near2, last2,
    gain1, gain2, taps_ref, decay_ref, inmap_ref, param_ref, rate_ref,
    local_sem, wsend, wrecv, tsend, trecv, csend, crecv,
):
    w_up, w_down = (w_up0, w_up1, w_up2), (w_down0, w_down1, w_down2)
    p = Place()
    barrier = pltpu.get_barrier_semaphore()
    greeted = [dict(x=1), dict(x=-1), dict(y=1), dict(y=-1), dict(z=1), dict(z=-1), dict(flip=True)]
    for where in greeted:
        pl.semaphore_signal(barrier, inc=1, device_id=p.device(**where), device_id_type=MESH)
    blocks = range(len(w_up))
    weights = [
        WeightGather(p, i, own, held, local_sem, wsend, wrecv, i - 3 - len(blocks))
        for i, (own, held) in enumerate(
            (
                (input_ref, w_input),
                (gate_ref, w_gate),
                (output_ref, w_output),
                *((up_ref.at[:, :, :, n * WIDTH : (n + 1) * WIDTH], w_up[n]) for n in blocks),
                *((down_ref.at[n], w_down[n]) for n in blocks),
            )
        )
    ]
    own_stream = pltpu.make_async_copy(stream_ref, held1.at[p.tp], local_sem.at[9])
    small = [
        pltpu.make_async_copy(source, target, local_sem.at[10 + k])
        for k, (source, target) in enumerate(
            (
                (decay_hbm, decay_ref),
                (inmap_hbm, inmap_ref),
                (param_hbm, param_ref),
                (gain1_hbm, gain1),
                (gain2_hbm, gain2),
                (taps_hbm, taps_ref),
                (offset_hbm, offsets),
            )
        )
    ]
    for copy in (weights[0].local, own_stream, *(w.local for w in weights[1:]), *small):
        copy.start()
    pl.semaphore_wait(barrier, len(greeted))

    gather1 = [TokenGather(p, c, held1, c * TALL, TALL, tsend, trecv) for c in range(2)]
    gather2 = [TokenGather(p, 2 + c, held2, c * PART, PART, tsend, trecv) for c in range(PARTS)]
    sum1 = [
        TokenSum(p, 2 + PARTS + c, c, terms1, core1, chip1, near1, last1, tsend, trecv) for c in range(PARTS)
    ]
    sum2 = [ColumnSum(p, c, c, terms2, core2, chip2, near2, last2, csend, crecv) for c in range(2)]
    def rows_of(c):
        return pl.ds(c * PART, PART)

    def prepare():
        for copy in small:
            copy.wait()
        block_diagonal(decay_ref, maps, 0)
        block_diagonal(inmap_ref, maps, WIDTH)
        parameter = -param_ref[...]
        softplus = jnp.maximum(parameter, 0.0) + jnp.log1p(jnp.exp(-jnp.abs(parameter)))
        rate_ref[...] = -DECAY_MULTIPLIER * softplus

    def begin():
        own_stream.wait()
        for gather in gather1:
            gather.begin()

    def columns_of(held, j, depth):
        pair = held[2 * j : 2 * j + 2].reshape(2, depth, 128)
        return jnp.concatenate([pair[0], pair[1]], axis=1)

    def inward(m):
        rows = pl.ds(m * TALL, TALL)
        columns = normed[rows, :]
        for held, target in ((w_input, values), (w_gate, gates)):
            full = held[...].reshape(GROUP * WIDTH, WIDTH)
            target[rows, :] = jnp.dot(columns, full, preferred_element_type=F32).astype(BF16)

    def mix(c):
        rows = rows_of(c)
        taps = taps_ref[...].astype(F32)
        state[rows, :] = mixer_rows(values[rows, :], offsets[rows, :], taps, maps[...], rate_ref[...])

    def project(c):
        rows = rows_of(c)
        mixed = gated(state[rows, :], gates[rows, :])
        for j in range(GROUP):
            product = jnp.dot(mixed, columns_of(w_output, j, WIDTH), preferred_element_type=F32)
            terms1[j // 2, j % 2, rows] = product.astype(BF16)
        sum1[c].begin()

    def last_core(turn):
        near = p.y // 2
        return {3: near, 4: 1 - near}.get(turn)

    def lower(turn):
        z, core = TURNS[turn], last_core(turn)
        there = wrap(p.z + z, 4)
        for w in weights[-len(blocks) :]:
            w.arrived(*(() if turn == 0 else (NAMES[turn - 5],)))
        for c in range(2):
            rows = pl.ds(c * TALL, TALL)
            for k in (0, 1) if core is None else (core,):
                product = 0.0
                for n in blocks:
                    pair = w_down[n][pl.ds(there * 4 + 2 * k, 2)].reshape(2, WIDTH, 128)
                    columns = jnp.concatenate([pair[0], pair[1]], axis=1)
                    some = activity[rows, n * WIDTH : (n + 1) * WIDTH]
                    product = product + jnp.dot(some, columns, preferred_element_type=F32)
                terms2[there, k, rows] = product.astype(BF16)
            sum2[c].begin(z % 4, core)

    def middle_of(c):
        rows = rows_of(c)
        held2[p.tp, rows] = sum1[c].finish(held1[p.tp, rows])
        gather2[c].begin()

    def raise_rows(c):
        gather2[c].finish()
        norm_rows(held2, rows_of(c), gain2, normed)

    def lift(c):
        rows = pl.ds(c * TALL, TALL)
        columns = normed[rows, :]
        for n in blocks:
            full = w_up[n][...].reshape(GROUP * WIDTH, WIDTH)
            raised = jnp.maximum(jnp.dot(columns, full, preferred_element_type=F32), 0.0)
            activity[rows, n * WIDTH : (n + 1) * WIDTH] = (raised * raised).astype(BF16)

    def last_of(c):
        rows = pl.ds(c * TALL, TALL)
        out_ref[rows, :] = sum2[c].finish(held2[p.tp, rows])

    actions = {
        "X": prepare,
        "GS": begin,
    }
    for i, w in enumerate(weights):
        for name in STEPS:
            actions[f"{i}{name}"] = functools.partial(w.step, name)
        if i < 3 + len(blocks):
            actions[f"{i}F"] = w.finish
    for c in range(PARTS):
        actions[f"N{c}"] = functools.partial(norm_rows, held1, rows_of(c), gain1, normed)
        actions[f"M{c}"] = functools.partial(mix, c)
        actions[f"P{c}"] = functools.partial(project, c)
        actions[f"K{c}"] = sum1[c].cores
        actions[f"L{c}"] = functools.partial(middle_of, c)
        actions[f"B{c}"] = gather2[c].far
        actions[f"Q{c}"] = functools.partial(raise_rows, c)
        actions[f"R{c}"] = sum1[c].ring
        actions[f"A{c}"] = gather2[c].near
    for turn, z in enumerate(TURNS):
        actions[f"V{turn}"] = functools.partial(lower, turn)
        for c in range(2):
            actions[f"k{turn}{c}"] = functools.partial(sum2[c].cores, z % 4, last_core(turn))
            actions[f"r{turn}{c}"] = functools.partial(sum2[c].ring, z % 4, last_core(turn))
    for c in range(2):
        actions[f"GA{c}"] = gather1[c].near
        actions[f"GB{c}"] = gather1[c].far
        actions[f"GF{c}"] = gather1[c].finish
        actions[f"I{c}"] = functools.partial(inward, c)
        actions[f"U{c}"] = functools.partial(lift, c)
        actions[f"l{c}"] = functools.partial(last_of, c)
    order = " ".join(ORDER).split()
    assert sorted(order) == sorted(actions)
    for name in order:
        actions[name]()

    for w in weights:
        w.drain()
    for event in (*gather1, *gather2, *sum1, *sum2):
        event.drain()


def quarters(weight):
    rows, columns = weight.shape
    return weight.reshape(2, 2, rows // 4, columns)


def shards(
    stream,
    recurrent_norm_gain,
    feedforward_norm_gain,
    recurrent_input_weight,
    output_gate_weight,
    causal_filter_weight,
    decay_gate_matrix,
    input_gate_matrix,
    channel_decay_param,
    token_decay_offset,
    recurrent_output_weight,
    up_projection_weight,
    down_projection_weight,
):
    mixer = [quarters(w) for w in (recurrent_input_weight, output_gate_weight, recurrent_output_weight)]
    up, hidden = quarters(up_projection_weight), up_projection_weight.shape[1]
    blocks = hidden // WIDTH
    down = down_projection_weight.reshape(blocks, 2, 2, WIDTH // 4, -1)
    arguments = (
        stream,
        recurrent_norm_gain.reshape(1, -1),
        feedforward_norm_gain.reshape(1, -1),
        mixer[0],
        mixer[1],
        causal_filter_weight,
        decay_gate_matrix,
        input_gate_matrix,
        channel_decay_param.reshape(1, -1),
        token_decay_offset,
        mixer[2],
        up,
        down,
    )
    far = pl.BlockSpec(memory_space=pltpu.HBM)
    sums = [
        pltpu.VMEM((4, 2, ROWS, WIDTH), BF16),
        pltpu.VMEM((4, ROWS, WIDTH), BF16),
        pltpu.VMEM((4, ROWS, WIDTH), BF16),
        pltpu.VMEM((2, ROWS, WIDTH), BF16),
        pltpu.VMEM((2, ROWS, WIDTH), BF16),
    ]
    events = 2 + 2 * PARTS
    return pl.pallas_call(
        kernel,
        out_shape=jax.ShapeDtypeStruct(stream.shape, stream.dtype),
        in_specs=[far] * 13,
        out_specs=pl.BlockSpec(memory_space=pltpu.VMEM),
        scratch_shapes=[
            *[pltpu.VMEM((16, *w.shape), BF16) for w in mixer],
            *[pltpu.VMEM((16, *up.shape[:-1], WIDTH), BF16)] * blocks,
            *[pltpu.VMEM((16, *down.shape[1:]), BF16)] * blocks,
            pltpu.VMEM((GROUP, ROWS, WIDTH), BF16),
            pltpu.VMEM((GROUP, ROWS, WIDTH), BF16),
            pltpu.VMEM((ROWS, GROUP * WIDTH), BF16),
            pltpu.VMEM((ROWS, WIDTH), BF16),
            pltpu.VMEM((ROWS, WIDTH), BF16),
            pltpu.VMEM((ROWS, WIDTH), F32),
            pltpu.VMEM((ROWS, WIDTH), F32),
            pltpu.VMEM((ROWS, hidden), BF16),
            pltpu.VMEM((WIDTH, 2 * WIDTH), BF16),
            *sums,
            *sums,
            pltpu.VMEM((1, GROUP * WIDTH), F32),
            pltpu.VMEM((1, GROUP * WIDTH), F32),
            pltpu.VMEM(causal_filter_weight.shape, BF16),
            pltpu.VMEM(decay_gate_matrix.shape, BF16),
            pltpu.VMEM(input_gate_matrix.shape, BF16),
            pltpu.VMEM((1, WIDTH), F32),
            pltpu.VMEM((1, WIDTH), F32),
            pltpu.SemaphoreType.DMA((17,)),
            pltpu.SemaphoreType.DMA((3 + 2 * blocks,)),
            pltpu.SemaphoreType.DMA(((3 + 2 * blocks) * TOGETHER + blocks * (len(NAMES) - TOGETHER),)),
            pltpu.SemaphoreType.DMA((events,)),
            pltpu.SemaphoreType.DMA((events, 3)),
            pltpu.SemaphoreType.DMA((2,)),
            pltpu.SemaphoreType.DMA((2, 7)),
        ],
        compiler_params=pltpu.CompilerParams(
            collective_id=0, has_side_effects=True, vmem_limit_bytes=VMEM_LIMIT
        ),
    )(*(pltpu.with_memory_space_constraint(value, pltpu.HBM) for value in arguments))


def solution(mesh):
    split = Mesh(
        mesh.devices.reshape(mesh.shape["rep"], 4, 4, mesh.shape["tp"]),
        AXES,
    )
    placed = (
        P(REP_FS, "tp"),
        P(),
        P(),
        P(FS, "tp"),
        P(FS, "tp"),
        P(None, "tp"),
        P("tp", None, None),
        P("tp", None, None),
        P("tp"),
        P(REP_FS, "tp"),
        P("tp", FS),
        P(FS, "tp"),
        P("tp", FS),
    )
    return jax.shard_map(
        shards, mesh=split, in_specs=placed, out_specs=P(REP_FS, "tp"), check_vma=False
    )
```
